256 devices in a mesh: sp: 16 (over y, x), tp: 16 (over z, core).
Axes of the slice: x: 4, y: 4, z: 8, core: 2. Of those that a mesh axis runs over, the one named last changes fastest.
Arguments:
- layer_in: bfloat16 [5120, 2048], P('sp', 'tp'), may hold values from -6 to 6
- out_cot: bfloat16 [5120, 2048], P('sp', 'tp'), may hold values from -6 to 6
- route_ids: int32 [5120, 2], P('sp'), may hold values from 0 to 15, all different within a row; in each aligned block of 320 rows (0 to 319, 320 to 639, ...) at most 80 rows name the same one
- route_probs: float32 [5120, 2], P('sp'), may hold values from 0.2 to 1
- group_prob: float32 [5120], P('sp'), may hold values from 0.3 to 1
- gate_weight: bfloat16 [16, 2048, 2048], P('sp', 'tp'), may hold values from -0.125 to 0.125
- up_weight: bfloat16 [16, 2048, 2048], P('sp', 'tp'), may hold values from -0.125 to 0.125
- down_weight: bfloat16 [16, 2048, 2048], P('sp', 'tp'), may hold values from -0.125 to 0.125
- out_weight: bfloat16 [2048, 2048], P(None, 'tp'), may hold values from -0.125 to 0.125
- query: bfloat16 [5120, 1024], P('sp', 'tp'), may hold values from -6 to 6
- key_in: bfloat16 [5120, 1024], P('sp', 'tp'), may hold values from -0.75 to 0.75
- value: bfloat16 [5120, 2048], P('sp', 'tp'), may hold values from -6 to 6
- decay_logit: bfloat16 [5120, 1024], P('sp', 'tp'), may hold values from -2.5 to 8.5, as said below
Outputs:
- gate_grad: float32 [16, 2048, 2048], P('sp', 'tp')
- up_grad: float32 [16, 2048, 2048], P('sp', 'tp')
- down_grad: float32 [16, 2048, 2048], P('sp', 'tp')
- proj_grad: float32 [2048, 2048], P('sp', 'tp')
- query_grad: float32 [5120, 1024], P('sp', 'tp')
- key_grad: float32 [5120, 1024], P('sp', 'tp')
- value_grad: float32 [5120, 2048], P('sp', 'tp')
- logit_grad: float32 [5120, 1024], P('sp', 'tp')
The draws below stay inside these ranges and needn't reach their ends.
Inputs may be any that keep to these rules, and one draw needn't show every extreme that they name: `route_ids`: each row names two different experts of 0 to 15; every expert is named by some row; within each aligned block of 320 rows (the rows of one device) no expert is named more than 80 times, and in some block one expert is named exactly 80 times. `decay_logit`: values lie between -2.5 and 8.5; even heads have pre-activations near 5, odd heads near 1.
All inputs are finite; a program needn't handle non-finite values.
Results may differ from the reference program's by a relative error of at most 0.019.
Values may be sent and summed in bfloat16 or wider, within the bound.
A program may use at most 128 MiB of HBM per device.

```python
import math
import jax
import jax.numpy as jnp
import numpy as np
from jax import lax

D = 2048
FFE = 2048
HEADS = 16
DK = 64
DV = 128
BLOCK = 64
TOK_DEV = 320
TOKENS = 5120
EXPERTS = 16
CAP = 80
N_SP = 16
N_TP = 16


def draw_decay_logit(key, part):
    shift_key, noise_key = jax.random.split(key, 2)
    channel_head = jnp.arange(HEADS * DK) // DK
    base_level = jnp.where(channel_head % 2 == 0, 5.0, 1.0)
    span_shift = jax.random.uniform(shift_key, (TOKENS // TOK_DEV, HEADS), minval=-0.8, maxval=0.8)
    row_span = jnp.arange(TOKENS) // TOK_DEV
    slow_part = span_shift[row_span][:, channel_head]
    noise_part = jnp.clip(0.6 * jax.random.normal(noise_key, (TOKENS, HEADS * DK)), -2.4, 2.4)
    return (base_level[None, :] + slow_part + noise_part).astype(jnp.float32).astype(jnp.bfloat16)


def raised(entries, rng, source, target, blocks, factor):
    owner, partner = [(jnp.arange(entries.shape[axis_at]) // (entries.shape[axis_at] // blocks)).reshape([-1 if axis == axis_at else 1 for axis in range(entries.ndim)]) for axis_at in (source, target)]
    chosen = jax.random.permutation(rng, blocks)[partner]
    strong = (owner == chosen) | (owner == (partner + blocks // 2) % blocks)
    return jnp.where(strong, factor * entries, entries)


def block_scale(rng, shape, cuts, least, largest):
    gain = 1.0
    for position, blocks in cuts:
        draws = jax.random.uniform(jax.random.fold_in(jax.random.fold_in(rng, 6), position), (blocks,), jnp.float32, least / len(cuts), largest / len(cuts))
        gain = gain * jnp.repeat(jnp.exp(draws), shape[position] // blocks).reshape((-1,) + (1,) * (len(shape) - 1 - position))
    return gain


def shared_out(stream_key, own, number, rows, count, top, most, slope):
    sequence = jax.random.permutation(stream_key, count)
    crowded, ordinary = load_shares(count, rows * top, most, slope, True), load_shares(count, rows * top, most, slope, False)
    places = jnp.arange(count)

    def named(sizes, turn):
        used = int((sizes > 0).sum())
        fixed = max(1, used // 4)
        passed = fixed + (places - fixed + turn * (used - fixed)) % max(1, count - fixed)
        return jnp.zeros((count,), jnp.int32).at[sequence[jnp.where(places < fixed, places, passed)]].set(jnp.asarray(sizes, jnp.int32))

    sizes = jnp.where(number % 4 == 0, named(crowded, number // 4), named(ordinary, number - number // 4 - 1))
    mixed = jax.random.permutation(jax.random.fold_in(own, 3), count)
    giver, receiver = mixed[0:count // 2 * 2:2], mixed[1:count // 2 * 2:2]
    room = jnp.minimum(sizes[giver] - 1, most - sizes[receiver]) // 2
    room = jnp.where((giver == sequence[0]) | (receiver == sequence[0]) | (sizes[receiver] == 0), 0, jnp.maximum(room, 0))
    passed = jax.random.randint(jax.random.fold_in(own, 4), (count // 2,), 0, 1 << 20) % (room + 1)
    sizes = sizes.at[giver].add(-passed).at[receiver].add(passed)
    items = jnp.searchsorted(jnp.cumsum(sizes), jnp.arange(rows * top), side="right").astype(jnp.int32)
    grid = items.reshape(top, rows).T
    grid = grid[jax.random.permutation(jax.random.fold_in(own, 1), rows)]
    turn = jax.random.randint(jax.random.fold_in(own, 2), (rows, 1), 0, top)
    return jnp.take_along_axis(grid, (jnp.arange(top)[None, :] + turn) % top, axis=1)


def load_shares(amount, total, reach, skew, full):
    weights = [(1 << 20) // math.isqrt(rank ** skew) + 1 for rank in range(1, amount + 1)]
    largest = reach if full else min(reach, max(-(-total // amount), total * weights[0] // sum(weights)))
    least = 1 if total - largest >= amount - 1 else 0
    given, surplus = [largest] + [least] * (amount - 1), total - largest - least * (amount - 1)
    while surplus > 0:
        candidates = [i for i in range(1, amount) if given[i] < largest] or [i for i in range(1, amount) if given[i] < reach]
        whole, budget = sum([weights[i] for i in candidates]), surplus
        for i in candidates:
            addition = min(reach - given[i], max(1, budget * weights[i] // whole), surplus)
            given[i] = given[i] + addition
            surplus = surplus - addition
    return np.array(given)


def normal_values(rng, dims, deviation, limit, cuts=(), held_as=jnp.bfloat16):
    level = block_scale(rng, dims, cuts, -0.22, 0.18) if cuts else 1.0
    entries = jax.random.normal(rng, dims, jnp.float32) * deviation * level
    return jnp.minimum(jnp.maximum(entries, -limit), limit).astype(held_as)


def noise_with(key, shape, scale, most, cuts, heavy, held_as=jnp.bfloat16):
    drawn = scale * jax.random.normal(key, shape, jnp.float32)
    if cuts:
        drawn = drawn * block_scale(key, shape, cuts, -0.22, 0.18)
    return jnp.clip(raised(drawn, jax.random.fold_in(key, 3), *heavy), -most, most).astype(held_as)


def setup_inputs(seed: int = 0) -> dict:
    streams_of = jax.random.split(jax.random.key(seed), 14)
    layer_in = normal_values(streams_of[0], (TOKENS, D), 1.0, 6.0, ((0, 16), (1, 16)))
    out_cot = noise_with(streams_of[1], (TOKENS, D), 1.0, 6.0, ((0, 16), (1, 16)), (0, 1, 16, 2.0))
    route_ids_keys = jax.random.split(jax.random.fold_in(streams_of[2], 1), TOKENS // TOK_DEV)
    route_ids_turns = jax.random.permutation(jax.random.fold_in(streams_of[2], 3), TOKENS // TOK_DEV)
    route_ids = jax.vmap(lambda own, number: shared_out(jax.random.fold_in(streams_of[2], 2), own, number, TOK_DEV, EXPERTS, 2, CAP, 1))(route_ids_keys, route_ids_turns).reshape((TOKENS, 2))
    route_probs = jnp.clip(0.2 + 0.8 * jax.random.uniform(streams_of[3], (TOKENS, 2), jnp.float32) ** block_scale(streams_of[3], (TOKENS, 2), ((0, 16),), -0.2, 0.2), 0.2, 1.0)
    group_prob = jnp.clip(0.3 + 0.7 * jax.random.uniform(streams_of[4], (TOKENS,), jnp.float32) ** block_scale(streams_of[4], (TOKENS,), ((0, 16),), -0.2, 0.2), 0.3, 1.0)
    gate_weight = normal_values(streams_of[5], (EXPERTS, FFE, D), D ** -0.5, 0.125, ((0, 16), (1, 16)))
    up_weight = normal_values(streams_of[6], (EXPERTS, FFE, D), D ** -0.5, 0.125, ((0, 16), (1, 16)))
    down_weight = normal_values(streams_of[7], (EXPERTS, FFE, D), FFE ** -0.5, 0.125, ((0, 16), (1, 16)))
    out_weight = normal_values(streams_of[8], (D, HEADS * DV), (HEADS * DV) ** -0.5, 0.125, ((1, 16),))
    query = normal_values(streams_of[9], (TOKENS, HEADS * DK), 1.0, 6.0, ((0, 16), (1, 16)))
    key_in = normal_values(streams_of[10], (TOKENS, HEADS * DK), 0.125, 0.75, ((0, 16), (1, 16)))
    value = normal_values(streams_of[11], (TOKENS, HEADS * DV), 1.0, 6.0, ((0, 16), (1, 16)))
    decay_logit = draw_decay_logit(jax.random.fold_in(streams_of[13], 71), 0)
    return dict(layer_in=layer_in, out_cot=out_cot, route_ids=route_ids, route_probs=route_probs, group_prob=group_prob, gate_weight=gate_weight, up_weight=up_weight, down_weight=down_weight, out_weight=out_weight, query=query, key_in=key_in, value=value, decay_logit=decay_logit)


decay_temp = 16.0
highest = lax.Precision.HIGHEST

def mixer_forward(scaled_query, keys_all, values_all, log_decay):
    length_all, head_count, key_dim = scaled_query.shape
    val_dim = values_all.shape[-1]
    blocks = length_all // BLOCK

    def split_blocks(tensor):
        return tensor.reshape(blocks, BLOCK, head_count, tensor.shape[-1]).transpose(2, 0, 1, 3)
    query_blk = split_blocks(scaled_query)
    key_blk = split_blocks(keys_all)
    value_blk = split_blocks(values_all)
    cumulative = jnp.cumsum(split_blocks(log_decay), axis=2)
    span_log = cumulative[:, :, -1:, :]
    query_decayed = query_blk * jnp.exp(cumulative)
    key_back = key_blk * jnp.exp(-cumulative)
    key_to_end = key_blk * jnp.exp(span_log - cumulative)
    causal = jnp.tril(jnp.ones((BLOCK, BLOCK), dtype=bool))
    scores = jnp.where(causal, jnp.einsum('hncd,hnsd->hncs', query_decayed, key_back, precision=highest), 0.0)
    within = jnp.einsum('hncs,hnsv->hncv', scores, value_blk, precision=highest)
    update = jnp.einsum('hncd,hncv->hndv', key_to_end, value_blk, precision=highest)
    block_decay = jnp.exp(span_log[:, :, 0, :])

    def advance(carry_state, inputs):
        decay_now, update_now = inputs
        return (carry_state * decay_now[..., None] + update_now, carry_state)
    start_state = jnp.zeros((head_count, key_dim, val_dim), jnp.float32)
    _, entering = lax.scan(advance, start_state, (jnp.moveaxis(block_decay, 1, 0), jnp.moveaxis(update, 1, 0)))
    entering = jnp.moveaxis(entering, 0, 1)
    carried = jnp.einsum('hncd,hndv->hncv', query_decayed, entering, precision=highest)
    return (within + carried).transpose(1, 2, 0, 3).reshape(length_all, head_count * val_dim)

def reference(layer_in, out_cot, route_ids, route_probs, group_prob, gate_weight, up_weight, down_weight, out_weight, query, key_in, value, decay_logit):
    length_all = layer_in.shape[0]
    width = layer_in.shape[1]
    route_weight = group_prob[:, None] * route_probs / lax.optimization_barrier(jnp.sum(route_probs, axis=1, keepdims=True))
    scaled_cot = (route_weight[:, :, None] * out_cot.astype(jnp.float32)[:, None, :]).astype(jnp.bfloat16)
    flat_ids = route_ids.reshape(-1)
    flat_cot = scaled_cot.reshape(-1, width)
    rows_max = N_SP * CAP
    hidden_dev = FFE // N_TP

    def one_expert(expert):
        order_rows = jnp.argsort((flat_ids != expert).astype(jnp.int32), stable=True)[:rows_max]
        valid_rows = flat_ids[order_rows] == expert
        token_rows = (order_rows // 2).astype(jnp.int32)
        inputs_x = layer_in[token_rows]
        cot_rows = jnp.where(valid_rows[:, None], flat_cot[order_rows], jnp.zeros((), jnp.bfloat16))
        gate_mat = gate_weight[expert]
        up_mat = up_weight[expert]
        down_mat = down_weight[expert]
        gate_pre = jnp.dot(inputs_x, gate_mat.T, preferred_element_type=jnp.float32)
        up_pre = jnp.dot(inputs_x, up_mat.T, preferred_element_type=jnp.float32)
        sigmoid_gate = jax.nn.sigmoid(gate_pre)
        active = gate_pre * sigmoid_gate
        hidden = (active * up_pre).astype(jnp.bfloat16)
        hidden_cot = jnp.dot(cot_rows, down_mat.T, preferred_element_type=jnp.float32)
        up_cot = (hidden_cot * active).astype(jnp.bfloat16)
        gate_cot = (hidden_cot * up_pre * sigmoid_gate * (1.0 + gate_pre * (1.0 - sigmoid_gate))).astype(jnp.bfloat16)
        down_g = jnp.dot(hidden.T, cot_rows, preferred_element_type=jnp.float32)
        gate_g = jnp.dot(gate_cot.T, inputs_x, preferred_element_type=jnp.float32)
        up_g = jnp.dot(up_cot.T, inputs_x, preferred_element_type=jnp.float32)
        gate_groups = gate_cot.astype(jnp.float32).reshape(rows_max, N_TP, hidden_dev)
        up_groups = up_cot.astype(jnp.float32).reshape(rows_max, N_TP, hidden_dev)
        gate_split = gate_mat.astype(jnp.float32).reshape(N_TP, hidden_dev, width)
        up_split = up_mat.astype(jnp.float32).reshape(N_TP, hidden_dev, width)
        partial_sum = jnp.einsum('rjf,jfd->rjd', gate_groups, gate_split, precision=highest)
        partial_sum = partial_sum + jnp.einsum('rjf,jfd->rjd', up_groups, up_split, precision=highest)
        rounded = lax.optimization_barrier(partial_sum.astype(jnp.bfloat16)).astype(jnp.float32)
        input_grad = lax.optimization_barrier(jnp.sum(rounded, axis=1))
        return (gate_g, up_g, down_g, input_grad, token_rows)
    gate_grad, up_grad, down_grad, input_grads, token_index = lax.map(one_expert, jnp.arange(EXPERTS, dtype=jnp.int32))
    routed_sum = jax.ops.segment_sum(input_grads.reshape(-1, width), token_index.reshape(-1), num_segments=length_all)
    mixed_cot = (out_cot.astype(jnp.float32) + routed_sum).astype(jnp.bfloat16)
    mixer_cot = jnp.dot(mixed_cot, out_weight, preferred_element_type=jnp.float32)

    def forward(query_f, key_f, value_f, logit_f):
        scaled = query_f.reshape(length_all, HEADS, DK) * DK ** (-0.5)
        log_decay = (jax.nn.log_sigmoid(logit_f) / decay_temp).reshape(length_all, HEADS, DK)
        return mixer_forward(scaled, key_f.reshape(length_all, HEADS, DK), value_f.reshape(length_all, HEADS, DV), log_decay)
    mixer_f32, pullback = jax.vjp(forward, query.astype(jnp.float32), key_in.astype(jnp.float32), value.astype(jnp.float32), decay_logit.astype(jnp.float32))
    query_grad, key_grad, value_grad, logit_grad = pullback(mixer_cot)
    mixer_out = mixer_f32.astype(jnp.bfloat16)
    proj_grad = jnp.dot(mixed_cot.T, mixer_out, preferred_element_type=jnp.float32)
    return (gate_grad, up_grad, down_grad, proj_grad, query_grad, key_grad, value_grad, logit_grad)
```

```python
import functools

import jax
import jax.numpy as jnp
from jax import lax
from jax.experimental import pallas as pl
from jax.experimental.pallas import tpu as pltpu
from jax.sharding import PartitionSpec as P

DK = 64
DV = 128
BLOCK = 64


decay_temp = 16.0
highest = lax.Precision.HIGHEST
f32, bf16 = jnp.float32, jnp.bfloat16
MESH = pl.DeviceIdType.MESH


def dot_nt(a, b):
    return lax.dot_general(a, b, (((1,), (1,)), ((), ())), preferred_element_type=f32)


def dot_nn(a, b):
    return lax.dot_general(a, b, (((1,), (0,)), ((), ())), preferred_element_type=f32)


def moe_kernel(
    sizes,
    layer_in,
    out_cot,
    ids,
    probs,
    group,
    gate,
    up,
    down,
    out_w,
    gate_g,
    up_g,
    down_g,
    full_cot,
    mixer_cot,
    send,
    sel_t,
    rows,
    pre,
    part_w,
    gu,
    gu_part,
    gu_t,
    hid_t,
    stage,
    inbox,
    ret_out,
    ret,
    a2a_s,
    a2a_r,
    back_s,
    back_r,
    ag_s,
    ag_r,
    agd_s,
    agd_r,
    rs_s,
    rs_r,
    tk_s,
    tk_r,
    tkd_s,
    tkd_r,
    misc_s,
    misc_r,
):
    n_sp, n_x, n_z, pieces = sizes
    n_y = n_sp // n_x
    half = n_z // 2
    toks, cols = layer_in.shape
    cap = 4 * toks // n_sp
    n_rows = n_sp * cap
    per = n_sp // pieces
    chunk = n_rows // pieces
    sp = lax.axis_index("sp")
    tp = lax.axis_index("tp")
    core = lax.rem(tp, 2)
    z = tp // 2
    z_up = lax.rem(z + 1, n_z)
    z_dn = lax.rem(z + n_z - 1, n_z)
    partner = (sp, 2 * z + 1 - core)
    above, below = (sp, 2 * z_up + core), (sp, 2 * z_dn + core)
    my_y, my_x = sp // n_x, lax.rem(sp, n_x)

    def there(r):
        ry, rx = r // n_x, lax.rem(r, n_x)
        return lax.rem(my_y + ry, n_y) * n_x + lax.rem(my_x + rx, n_x)

    def back_to(r):
        ry, rx = r // n_x, lax.rem(r, n_x)
        return lax.rem(my_y + n_y - ry, n_y) * n_x + lax.rem(my_x + n_x - rx, n_x)

    def zpos(d):
        return lax.rem(z + d + n_z, n_z)

    def remote(src, dst, s, r, dev):
        return pltpu.make_async_remote_copy(
            src_ref=src, dst_ref=dst, send_sem=s, recv_sem=r, device_id=dev, device_id_type=MESH
        )

    barrier = pltpu.get_barrier_semaphore()
    for r in range(1, n_sp):
        pl.semaphore_signal(barrier, inc=1, device_id=(there(r), tp), device_id_type=MESH)
    for dev in (partner, above, below):
        pl.semaphore_signal(barrier, inc=1, device_id=dev, device_id_type=MESH)

    experts = lax.broadcasted_iota(jnp.int32, (toks, 128), 1)
    id0, id1 = ids[:, 0:1], ids[:, 1:2]
    hit0, hit1 = experts == id0, experts == id1
    chosen = (jnp.where(hit0, 1.0, 0.0) + jnp.where(hit1, 1.0, 0.0)).astype(bf16)
    t_row = lax.broadcasted_iota(jnp.int32, (toks, toks), 0)
    t_col = lax.broadcasted_iota(jnp.int32, (toks, toks), 1)
    earlier = jnp.where(t_col < t_row, 1.0, 0.0).astype(bf16)
    count = dot_nn(earlier, chosen)
    pos0 = jnp.sum(jnp.where(hit0, count, 0.0), axis=1, keepdims=True)
    pos1 = jnp.sum(jnp.where(hit1, count, 0.0), axis=1, keepdims=True)

    def offset_of(expert):
        ey, ex = expert // n_x, lax.rem(expert, n_x)
        return lax.rem(ey + n_y - my_y, n_y) * n_x + lax.rem(ex + n_x - my_x, n_x)

    slot0 = offset_of(id0) * cap + pos0.astype(jnp.int32)
    slot1 = offset_of(id1) * cap + pos1.astype(jnp.int32)
    slots = lax.broadcasted_iota(jnp.int32, (toks, n_rows), 1)
    sel_t[...] = (
        jnp.where(slots == slot0, 1.0, 0.0) + jnp.where(slots == slot1, 1.0, 0.0)
    ).astype(bf16)
    diagonal = t_row == t_col

    def as_row(column):
        return jnp.sum(jnp.where(diagonal, column, 0.0), axis=0, keepdims=True)

    p0, p1 = as_row(probs[:, 0:1]), as_row(probs[:, 1:2])
    w0 = group[...] * p0 / (p0 + p1)
    w1 = group[...] * p1 / (p0 + p1)
    slot0_row, slot1_row = as_row(slot0.astype(f32)), as_row(slot1.astype(f32))
    both = jnp.concatenate([layer_in[...], out_cot[...]], axis=1)

    def select(p, carry):
        base = pl.multiple_of(p * chunk, chunk)
        here = (lax.broadcasted_iota(jnp.int32, (chunk, toks), 0) + p * chunk).astype(f32)
        m0, m1 = here == slot0_row, here == slot1_row
        pick = (jnp.where(m0, 1.0, 0.0) + jnp.where(m1, 1.0, 0.0)).astype(bf16)
        weight = jnp.sum(jnp.where(m0, w0, 0.0) + jnp.where(m1, w1, 0.0), axis=1, keepdims=True)
        picked = dot_nn(pick, both)
        send[0, pl.ds(base, chunk), :] = picked[:, :cols].astype(bf16)
        send[1, pl.ds(base, chunk), :] = (picked[:, cols:] * weight).astype(bf16)
        return carry

    lax.fori_loop(0, pieces, select, 0)
    pl.semaphore_wait(barrier, n_sp + 2)

    give_w = [
        remote(w, part_w.at[k], misc_s.at[k], misc_r.at[k], partner)
        for k, w in enumerate((gate, up))
    ]
    for copy in give_w:
        copy.start()

    def slot_rows(r):
        return pl.ds(pl.multiple_of(r * cap, cap), cap)

    def dispatch(r):
        return remote(
            send.at[:, slot_rows(r), :],
            rows.at[tp, :, slot_rows(r), :],
            a2a_s.at[r],
            a2a_r.at[r],
            (there(r), tp),
        )

    def start_dispatch(r, carry):
        dispatch(r).start()
        return carry

    lax.fori_loop(1, n_sp, start_dispatch, 0)
    rows[tp, :, slot_rows(0), :] = send[:, slot_rows(0), :]

    last = (half - 1) * pieces

    def ring(n_pieces, where, sems_s, sems_r, sems_ds, sems_dr, own_ready, compute):
        h_p = n_pieces // 2
        total = (half - 1) * n_pieces + h_p

        def along(block, p, d, k):
            ref = where(block, p)
            return remote(ref, ref, sems_s.at[d, k], sems_r.at[d, k], above if d == 0 else below)

        def across(block, p, k):
            ref = where(block, p)
            return remote(ref, ref, sems_ds.at[k], sems_dr.at[k], partner)

        def own(p, carry):
            own_ready(p)
            along(tp, p, 0, p).start()
            along(tp, p, 1, p).start()
            across(tp, p, p).start()
            return carry

        lax.fori_loop(0, n_pieces, own, 0)

        def own_compute(p, carry):
            across(tp, p, p).wait_recv()
            compute(z, p)
            return carry

        lax.fori_loop(0, n_pieces, own_compute, 0)

        def at(t):
            in_half = t >= (half - 1) * n_pieces
            p_up = lax.rem(t, n_pieces)
            p_dn = jnp.where(in_half, p_up + h_p, p_up)
            hop = t // n_pieces
            return hop, p_up, p_dn

        def step(t, carry):
            hop, p_up, p_dn = at(t)
            b_up, b_dn = zpos(-1 - hop), zpos(1 + hop)
            along(2 * b_up + core, p_up, 0, t).wait_recv()

            @pl.when((hop < half - 2) | ((hop == half - 2) & (p_up < h_p)))
            def _():
                along(2 * b_up + core, p_up, 0, t + n_pieces).start()

            across(2 * b_up + core, p_up, n_pieces + 2 * t).start()
            along(2 * b_dn + core, p_dn, 1, t).wait_recv()

            @pl.when(hop < half - 2)
            def _():
                along(2 * b_dn + core, p_dn, 1, t + n_pieces).start()

            @pl.when((hop == half - 2) & (p_dn >= h_p))
            def _():
                along(2 * b_dn + core, p_dn, 1, t + n_pieces - h_p).start()

            across(2 * b_dn + core, p_dn, n_pieces + 2 * t + 1).start()

            @pl.when(t > 0)
            def _():
                use(t - 1)

            return carry

        def use(t):
            hop, p_up, p_dn = at(t)
            b_up, b_dn = zpos(-1 - hop), zpos(1 + hop)
            across(2 * b_up + 1 - core, p_up, n_pieces + 2 * t).wait_recv()
            compute(b_up, p_up)
            across(2 * b_dn + 1 - core, p_dn, n_pieces + 2 * t + 1).wait_recv()
            compute(b_dn, p_dn)

        lax.fori_loop(0, total, step, 0)
        use(total - 1)

        def drain():
            def one(k, carry):
                along(tp, 0, 0, k).wait_send()
                along(tp, 0, 1, k).wait_send()
                return carry

            lax.fori_loop(0, total, one, 0)

            def other(k, carry):
                across(tp, 0, k).wait_send()
                return carry

            lax.fori_loop(0, n_pieces + 2 * total, other, 0)

        return drain

    def piece_rows(p):
        return pl.ds(pl.multiple_of(p * chunk, chunk), chunk)

    def rows_ready(p):
        for i in range(per):
            r = p * per + i

            @pl.when(r > 0)
            def _():
                dispatch(r).wait_recv()

    def feats(b):
        return pl.ds(pl.multiple_of(b * 2 * cols, 2 * cols), 2 * cols)

    pre[...] = jnp.zeros_like(pre)

    def expert_in(b, p):
        w_gu = jnp.concatenate([gate[:, feats(b)], up[:, feats(b)]], axis=0)
        at = piece_rows(p)
        x = jnp.concatenate([rows[2 * b, 0, at, :], rows[2 * b + 1, 0, at, :]], axis=1)
        c = jnp.concatenate([rows[2 * b, 1, at, :], rows[2 * b + 1, 1, at, :]], axis=1)
        pre[at, 0:256] += dot_nt(x, w_gu)
        pre[at, 256:384] += dot_nt(c, down[:, feats(b)])

    drain_rows = ring(
        pieces,
        lambda block, p: rows.at[block, :, piece_rows(p), :],
        ag_s,
        ag_r,
        agd_s,
        agd_r,
        rows_ready,
        expert_in,
    )

    def middle(p, carry):
        at = piece_rows(p)
        gate_pre, up_pre, hidden_cot = pre[at, 0:128], pre[at, 128:256], pre[at, 256:384]
        sig = jax.nn.sigmoid(gate_pre)
        active = gate_pre * sig
        hidden = active * up_pre
        up_cot = (hidden_cot * active).astype(bf16)
        gate_cot = (hidden_cot * up_pre * sig * (1.0 + gate_pre * (1.0 - sig))).astype(bf16)
        gu[at, 0:128] = gate_cot
        gu[at, 128:256] = up_cot
        pre[at, 0:128] = hidden
        return carry

    lax.fori_loop(0, pieces, middle, 0)
    give_gu = remote(gu, gu_part, misc_s.at[2], misc_r.at[2], partner)
    give_gu.start()
    gu_t[...] = gu[...].T
    hid_t[...] = pre[:, 0:128].astype(bf16).T
    for copy in give_w:
        copy.wait_recv()
    give_gu.wait_recv()

    h_p = pieces // 2
    rs_total = h_p + (half - 1) * pieces

    def partial(b, p):
        cols_at = pl.ds(pl.multiple_of((2 * b + core) * cols, cols), cols)
        mine = jnp.concatenate([gate[:, cols_at], up[:, cols_at]], axis=0)
        theirs = jnp.concatenate([part_w[0, :, cols_at], part_w[1, :, cols_at]], axis=0)
        at = piece_rows(p)
        return dot_nn(gu[at, :], mine) + dot_nn(gu_part[at, :], theirs)

    def hop_sum(d, k):
        return remote(
            stage.at[d, k],
            inbox.at[d, k],
            rs_s.at[d, k],
            rs_r.at[d, k],
            above if d == 0 else below,
        )

    def first(t, carry):
        for d in range(2):
            stage[d, t] = partial(zpos(half), t + d * h_p).astype(bf16)
            hop_sum(d, t).start()
        return carry

    lax.fori_loop(0, h_p, first, 0)

    def gradients(b):
        x = jnp.concatenate([rows[2 * b, 0], rows[2 * b + 1, 0]], axis=1)
        c = jnp.concatenate([rows[2 * b, 1], rows[2 * b + 1, 1]], axis=1)
        both_g = dot_nn(gu_t[...], x)
        gate_g[:, feats(b)] = both_g[0:128]
        up_g[:, feats(b)] = both_g[128:256]
        down_g[:, feats(b)] = dot_nn(hid_t[...], c)

    def later(u, carry):
        t = u + h_p
        hop, p = 1 + u // pieces, lax.rem(u, pieces)
        for d in range(2):
            dest = zpos(half - hop) if d == 0 else zpos(hop - half)
            value = partial(dest, p)
            mine_first = (p >= h_p) if d == 0 else (p < h_p)
            alone = (hop == 1) & mine_first
            k_in = jnp.where(hop == 1, p - d * h_p, t - pieces)

            @pl.when(alone)
            def _():
                stage[d, t] = value.astype(bf16)

            @pl.when(jnp.logical_not(alone))
            def _():
                hop_sum(d, k_in).wait_recv()
                stage[d, t] = (value + inbox[d, k_in].astype(f32)).astype(bf16)

            hop_sum(d, t).start()

        @pl.when(u < n_z)
        def _():
            gradients(u)

        return carry

    lax.fori_loop(0, rs_total - h_p, later, 0)

    def give_back(r):
        return remote(
            ret_out.at[slot_rows(r), :],
            ret.at[slot_rows(r), :],
            back_s.at[r],
            back_r.at[r],
            (back_to(r), tp),
        )

    def finish(p, carry):
        k_in = rs_total - pieces + p
        value = partial(z, p)
        for d in range(2):
            hop_sum(d, k_in).wait_recv()
            value = value + inbox[d, k_in].astype(f32)
        ret_out[piece_rows(p), :] = value.astype(bf16)
        for i in range(per):
            r = p * per + i

            @pl.when(r > 0)
            def _():
                give_back(r).start()

        return carry

    lax.fori_loop(0, pieces, finish, 0)
    for g in range(rs_total - h_p, n_z):
        gradients(g)
    ret[slot_rows(0), :] = ret_out[slot_rows(0), :]

    def take_back(r, carry):
        give_back(r).wait_recv()
        return carry

    lax.fori_loop(1, n_sp, take_back, 0)
    mixed = (out_cot[...].astype(f32) + dot_nn(sel_t[...], ret[...])).astype(bf16)
    full_cot[tp] = mixed

    tok_half = toks // 2
    mixer_cot[...] = jnp.zeros_like(mixer_cot)

    def project(b, p):
        at = pl.ds(pl.multiple_of(p * tok_half, tok_half), tok_half)
        c = jnp.concatenate([full_cot[2 * b, at, :], full_cot[2 * b + 1, at, :]], axis=1)
        mixer_cot[at, :] += dot_nn(c, out_w[feats(b), :])

    drain_toks = ring(
        2,
        lambda block, p: full_cot.at[block, pl.ds(pl.multiple_of(p * tok_half, tok_half), tok_half), :],
        tk_s,
        tk_r,
        tkd_s,
        tkd_r,
        lambda p: None,
        project,
    )

    def sent(r, carry):
        dispatch(r).wait_send()
        give_back(r).wait_send()
        return carry

    lax.fori_loop(1, n_sp, sent, 0)
    for copy in (*give_w, give_gu):
        copy.wait_send()

    def sums_sent(k, carry):
        for d in range(2):
            hop_sum(d, k).wait_send()
        return carry

    lax.fori_loop(0, rs_total, sums_sent, 0)
    drain_rows()
    drain_toks()


def moe(layer_in, out_cot, ids, probs, group, gate, up, down, out_w, n_sp, n_tp):
    toks, cols = layer_in.shape
    n_x = 4 if n_sp == 16 else n_sp
    n_z = n_tp // 2
    half = n_z // 2
    pieces = 4 if n_sp % 4 == 0 else 2
    width = gate.shape[1]
    n_rows = 4 * toks
    total = (half - 1) * pieces + pieces // 2
    tk_total = (half - 1) * 2 + 1
    chunk = n_rows // pieces
    dma = pltpu.SemaphoreType.DMA
    vmem = pl.BlockSpec(memory_space=pltpu.VMEM)
    return pl.pallas_call(
        functools.partial(moe_kernel, (n_sp, n_x, n_z, pieces)),
        out_shape=(
            jax.ShapeDtypeStruct((128, width), f32),
            jax.ShapeDtypeStruct((128, width), f32),
            jax.ShapeDtypeStruct((128, width), f32),
            jax.ShapeDtypeStruct((n_tp, toks, cols), bf16),
            jax.ShapeDtypeStruct((toks, 128), f32),
        ),
        in_specs=[vmem] * 9,
        out_specs=[vmem] * 5,
        scratch_shapes=[
            pltpu.VMEM((2, n_rows, cols), bf16),
            pltpu.VMEM((toks, n_rows), bf16),
            pltpu.VMEM((n_tp, 2, n_rows, cols), bf16),
            pltpu.VMEM((n_rows, 384), f32),
            pltpu.VMEM((2, 128, width), bf16),
            pltpu.VMEM((n_rows, 256), bf16),
            pltpu.VMEM((n_rows, 256), bf16),
            pltpu.VMEM((256, n_rows), bf16),
            pltpu.VMEM((128, n_rows), bf16),
            pltpu.VMEM((2, total, chunk, cols), bf16),
            pltpu.VMEM((2, total, chunk, cols), bf16),
            pltpu.VMEM((n_rows, cols), bf16),
            pltpu.VMEM((n_rows, cols), bf16),
            dma((n_sp,)),
            dma((n_sp,)),
            dma((n_sp,)),
            dma((n_sp,)),
            dma((2, total)),
            dma((2, total)),
            dma((pieces + 2 * total,)),
            dma((pieces + 2 * total,)),
            dma((2, total)),
            dma((2, total)),
            dma((2, tk_total)),
            dma((2, tk_total)),
            dma((2 + 2 * tk_total,)),
            dma((2 + 2 * tk_total,)),
            dma((3,)),
            dma((3,)),
        ],
        compiler_params=pltpu.CompilerParams(
            collective_id=0, has_side_effects=True, vmem_limit_bytes=60 * 1024 * 1024
        ),
    )(layer_in, out_cot, ids, probs, group, gate, up, down, out_w)


def sent_to_all(x, axis):
    copies = jnp.broadcast_to(x, (lax.axis_size(axis), *x.shape))
    return lax.all_to_all(copies, axis, split_axis=0, concat_axis=0, tiled=True)


def all_in_one(x, axis):
    leaves = jax.tree.leaves(x)
    turns = sorted(range(len(leaves)), key=lambda k: -leaves[k].size)
    width = (1, *leaves[turns[0]].shape)[-1]
    lines = [
        jnp.pad(leaves[k].reshape(-1), (0, -leaves[k].size % width)).reshape(-1, width)
        for k in turns
    ]
    both, at, found = (sent_to_all(jnp.concatenate(lines), axis), 0, {})
    for k, line in zip(turns, lines):
        section = both[:, at : at + len(line)].reshape(len(both), -1)
        found[k] = section[:, : leaves[k].size].reshape(-1, *leaves[k].shape)
        at += len(line)
    numbers = iter(range(len(leaves)))
    return jax.tree.map(lambda _: found[next(numbers)], x)


def folded_in_pairs(pieces, combine):
    while len(jax.tree.leaves(pieces)[0]) > 1:
        pieces = jax.vmap(combine)(
            *(jax.tree.map(lambda part: part[side::2], pieces) for side in (0, 1))
        )
    return jax.tree.map(lambda part: part[0], pieces)


def entering(x, axis, combine, identity, reverse):
    length, index = (lax.axis_size(axis), lax.axis_index(axis))
    passed = jnp.arange(length) > index if reverse else jnp.arange(length) < index

    def kept(part, zero, own):
        part = jnp.where(
            passed.reshape(-1, *(1 for _ in own.shape)),
            part.astype(own.dtype),
            jnp.asarray(zero, own.dtype),
        )
        return part[::-1] if reverse else part

    pieces = all_in_one(
        jax.tree.map(
            lambda part, kind: part.astype(kind),
            x,
            jax.tree.map(lambda a: jnp.bfloat16 if a.dtype == jnp.float32 else a.dtype, x),
        ),
        axis,
    )
    return folded_in_pairs(jax.tree.map(kept, pieces, identity, x), combine)


def in_blocks(x, dim, length):
    lengths = x.shape
    blocks = x.reshape(*lengths[:dim], length, lengths[dim] // length, *lengths[dim + 1 :])
    return jnp.moveaxis(blocks, dim, 0)


def summed_on_arrival(x, axis, dim):
    length = lax.axis_size(axis)
    blocks = lax.all_to_all(in_blocks(x, dim, length), axis, 0, 0, tiled=True)
    return jnp.sum(blocks.astype(jnp.float32), axis=0)


def combine_spans(earlier, later):
    return (earlier[0] * later[0], later[1] + later[0][..., None] * earlier[1])


def contract_rows(left_mat, right_mat):
    return lax.dot_general(
        left_mat, right_mat, (((0,), (0,)), ((), ())), preferred_element_type=jnp.float32
    )


def contract_cols(left_mat, right_mat):
    return lax.dot_general(
        left_mat, right_mat, (((1,), (1,)), ((), ())), preferred_element_type=jnp.float32
    )


def to_blocks(tensor, head_count):
    rows_here = tensor.shape[0]
    return (
        tensor.astype(jnp.float32)
        .reshape(rows_here // BLOCK, BLOCK, head_count, -1)
        .transpose(2, 0, 1, 3)
    )


def from_blocks(tensor):
    head_count, blocks, _, channels = tensor.shape
    return tensor.transpose(1, 2, 0, 3).reshape(blocks * BLOCK, head_count * channels)


def local(
    layer_in,
    out_cot,
    route_ids,
    route_probs,
    group_prob,
    gate_weight,
    up_weight,
    down_weight,
    out_weight,
    query,
    key_in,
    value,
    decay_logit,
):
    tok_rows = layer_in.shape[0]
    head_dev = query.shape[1] // DK
    scaled_query = to_blocks(query, head_dev) * DK ** (-0.5)
    key_blk = to_blocks(key_in, head_dev)
    value_blk = to_blocks(value, head_dev)
    logit_blk = to_blocks(decay_logit, head_dev)
    cumulative = jnp.cumsum(jax.nn.log_sigmoid(logit_blk) / decay_temp, axis=2)
    span_log = cumulative[:, :, -1:, :]
    growth = jnp.exp(cumulative)
    shrink = jnp.exp(-cumulative)
    to_end = jnp.exp(span_log - cumulative)
    query_decayed = scaled_query * growth
    key_back = key_blk * shrink
    key_to_end = key_blk * to_end
    causal = jnp.tril(jnp.ones((BLOCK, BLOCK), dtype=bool))
    scores = jnp.where(
        causal, jnp.einsum("hncd,hnsd->hncs", query_decayed, key_back, precision=highest), 0.0
    )
    within = jnp.einsum("hncs,hnsv->hncv", scores, value_blk, precision=highest)
    block_decay = jnp.moveaxis(jnp.exp(span_log[:, :, 0, :]), 1, 0)
    block_update = jnp.moveaxis(
        jnp.einsum("hncd,hncv->hndv", key_to_end, value_blk, precision=highest), 1, 0
    )
    identity_pair = (
        jnp.ones((head_dev, DK), jnp.float32),
        jnp.zeros((head_dev, DK, DV), jnp.float32),
    )

    def advance(carry_pair, inputs):
        return (combine_spans(carry_pair, inputs), carry_pair)

    span_total, before_pairs = lax.scan(advance, identity_pair, (block_decay, block_update))
    entry_pair = entering(span_total, "sp", combine_spans, identity_pair, False)
    entry_state = entry_pair[1]
    decay_before = jnp.moveaxis(before_pairs[0], 0, 1)
    block_state = decay_before[..., None] * entry_state[:, None] + jnp.moveaxis(
        before_pairs[1], 0, 1
    )
    span_end = span_total[0][..., None] * entry_state + span_total[1]
    outputs = within + jnp.einsum("hncd,hndv->hncv", query_decayed, block_state, precision=highest)
    mixer_out = from_blocks(outputs).astype(jnp.bfloat16)
    n_sp, n_tp = lax.axis_size("sp"), lax.axis_size("tp")
    gate_g, up_g, down_g, full_cot, mixer_cot = moe(
        layer_in,
        out_cot,
        route_ids,
        route_probs,
        group_prob.reshape(1, tok_rows),
        gate_weight[0],
        up_weight[0],
        down_weight[0],
        out_weight,
        n_sp,
        n_tp,
    )
    proj_part = jnp.einsum("btf,tv->bfv", full_cot, mixer_out, preferred_element_type=f32)
    proj_all = lax.all_to_all(proj_part.astype(bf16), "sp", 0, 0, tiled=True)
    proj_grad = jnp.sum(proj_all.astype(f32), axis=0)
    cot_blk = to_blocks(mixer_cot, head_dev)
    block_future = jnp.moveaxis(
        jnp.einsum("hncd,hncv->hndv", query_decayed, cot_blk, precision=highest), 1, 0
    )

    def retreat(carry_pair, inputs):
        return (combine_spans(carry_pair, inputs), carry_pair)

    span_back, after_pairs = lax.scan(
        retreat, identity_pair, (block_decay, block_future), reverse=True
    )
    beyond_pair = entering(span_back, "sp", combine_spans, identity_pair, True)
    future_state = beyond_pair[1]
    decay_after = jnp.moveaxis(after_pairs[0], 0, 1)
    block_future_state = decay_after[..., None] * future_state[:, None] + jnp.moveaxis(
        after_pairs[1], 0, 1
    )
    cot_values = jnp.where(
        causal, jnp.einsum("hncv,hnsv->hncs", cot_blk, value_blk, precision=highest), 0.0
    )
    query_scaled_grad = growth * (
        jnp.einsum("hncv,hndv->hncd", cot_blk, block_state, precision=highest)
        + jnp.einsum("hncs,hnsd->hncd", cot_values, key_back, precision=highest)
    )
    key_part = shrink * jnp.einsum("hncs,hncd->hnsd", cot_values, query_decayed, precision=highest)
    key_grad = key_part + to_end * jnp.einsum(
        "hnsv,hndv->hnsd", value_blk, block_future_state, precision=highest
    )
    value_grad = jnp.einsum("hncs,hncv->hnsv", scores, cot_blk, precision=highest) + jnp.einsum(
        "hnsd,hndv->hnsv", key_to_end, block_future_state, precision=highest
    )
    decay_terms = (scaled_query * query_scaled_grad - key_blk * key_grad).reshape(
        head_dev, tok_rows, DK
    )
    tail_sum = jnp.flip(jnp.cumsum(jnp.flip(decay_terms, 1), axis=1), 1)
    beyond_term = jnp.sum(future_state * span_end, axis=2)
    log_grad = tail_sum + beyond_term[:, None, :]
    logit_flat = logit_blk.reshape(head_dev, tok_rows, DK)
    logit_grad = (
        (log_grad * jax.nn.sigmoid(-logit_flat) / decay_temp)
        .transpose(1, 0, 2)
        .reshape(tok_rows, head_dev * DK)
    )
    query_grad = from_blocks(query_scaled_grad * DK ** (-0.5))
    return (
        gate_g[None],
        up_g[None],
        down_g[None],
        proj_grad,
        query_grad,
        from_blocks(key_grad),
        from_blocks(value_grad),
        logit_grad,
    )


def solution(mesh):
    in_specs = (
        P("sp", "tp"),
        P("sp", "tp"),
        P("sp", None),
        P("sp", None),
        P("sp"),
        P("sp", "tp", None),
        P("sp", "tp", None),
        P("sp", "tp", None),
        P(None, "tp"),
        P("sp", "tp"),
        P("sp", "tp"),
        P("sp", "tp"),
        P("sp", "tp"),
    )
    out_specs = (
        P("sp", "tp", None),
        P("sp", "tp", None),
        P("sp", "tp", None),
        P("sp", "tp"),
        P("sp", "tp"),
        P("sp", "tp"),
        P("sp", "tp"),
        P("sp", "tp"),
    )
    return jax.shard_map(local, mesh=mesh, in_specs=in_specs, out_specs=out_specs, check_vma=False)
```

```python
import functools

import jax
import jax.numpy as jnp
from jax import lax
from jax.experimental import pallas as pl
from jax.experimental.pallas import tpu as pltpu
from jax.sharding import PartitionSpec as P

DK = 64
DV = 128


decay_temp = 16.0
f32, bf16 = jnp.float32, jnp.bfloat16
MESH = pl.DeviceIdType.MESH


def dot_nt(a, b):
    return lax.dot_general(a, b, (((1,), (1,)), ((), ())), preferred_element_type=f32)


def dot_nn(a, b):
    return lax.dot_general(a, b, (((1,), (0,)), ((), ())), preferred_element_type=f32)


def dot_tn(a, b):
    return lax.dot_general(a, b, (((0,), (0,)), ((), ())), preferred_element_type=f32)


def parts_of(x, n):
    if x.dtype == bf16:
        return [x]
    found = []
    for _ in range(n):
        top = x.astype(bf16)
        found.append(top)
        x = x - top.astype(f32)
    return found


def fine(dot, a, b, n=2):
    a, b = parts_of(a, n), parts_of(b, n)
    terms = [dot(p, q) for i, p in enumerate(a) for j, q in enumerate(b) if i + j < n]
    total = terms[-1]
    for term in terms[-2::-1]:
        total = total + term
    return total


def moe_kernel(
    sizes,
    layer_in,
    out_cot,
    ids,
    probs,
    group,
    gate,
    up,
    down,
    out_w,
    query,
    key_in,
    value,
    logit,
    gate_g,
    up_g,
    down_g,
    proj_g,
    query_g,
    key_g,
    value_g,
    logit_g,
    full_cot,
    mixer_cot,
    q_dec,
    k_back,
    k_end,
    cumul,
    scores,
    within,
    mix_t,
    span_out,
    span_in,
    entry,
    fut_out,
    fut_in,
    pj_out,
    pj_in,
    send,
    sel_t,
    rows,
    pre,
    part_w,
    gu,
    gu_part,
    gu_t,
    hid_t,
    stage,
    inbox,
    ret_out,
    ret,
    a2a_s,
    a2a_r,
    back_s,
    back_r,
    ag_s,
    ag_r,
    agd_s,
    agd_r,
    rs_s,
    rs_r,
    tk_s,
    tk_r,
    tkd_s,
    tkd_r,
    misc_s,
    misc_r,
    fw_s,
    fw_r,
    bw_s,
    bw_r,
    pj_s,
    pj_r,
):
    n_sp, n_x, n_z, pieces = sizes
    n_y = n_sp // n_x
    half = n_z // 2
    toks, cols = layer_in.shape
    cap = 4 * toks // n_sp
    n_rows = n_sp * cap
    per = n_sp // pieces
    chunk = n_rows // pieces
    sp = lax.axis_index("sp")
    tp = lax.axis_index("tp")
    core = lax.rem(tp, 2)
    z = tp // 2
    z_up = lax.rem(z + 1, n_z)
    z_dn = lax.rem(z + n_z - 1, n_z)
    partner = (sp, 2 * z + 1 - core)
    above, below = (sp, 2 * z_up + core), (sp, 2 * z_dn + core)
    my_y, my_x = sp // n_x, lax.rem(sp, n_x)

    def there(r):
        ry, rx = r // n_x, lax.rem(r, n_x)
        return lax.rem(my_y + ry, n_y) * n_x + lax.rem(my_x + rx, n_x)

    def back_to(r):
        ry, rx = r // n_x, lax.rem(r, n_x)
        return lax.rem(my_y + n_y - ry, n_y) * n_x + lax.rem(my_x + n_x - rx, n_x)

    def zpos(d):
        return lax.rem(z + d + n_z, n_z)

    def remote(src, dst, s, r, dev):
        return pltpu.make_async_remote_copy(
            src_ref=src, dst_ref=dst, send_sem=s, recv_sem=r, device_id=dev, device_id_type=MESH
        )

    barrier = pltpu.get_barrier_semaphore()
    for r in range(1, n_sp):
        pl.semaphore_signal(barrier, inc=1, device_id=(there(r), tp), device_id_type=MESH)
    for dev in (partner, above, below):
        pl.semaphore_signal(barrier, inc=1, device_id=dev, device_id_type=MESH)

    t_row = lax.broadcasted_iota(jnp.int32, (toks, toks), 0)
    t_col = lax.broadcasted_iota(jnp.int32, (toks, toks), 1)
    diagonal = t_row == t_col

    def as_row(column):
        return jnp.sum(jnp.where(diagonal, column, 0.0), axis=0, keepdims=True)

    def as_column(row):
        return jnp.sum(jnp.where(diagonal, row, 0.0), axis=1, keepdims=True)

    experts = lax.broadcasted_iota(jnp.int32, (toks, 128), 1)
    id0 = as_column(ids[0:1, :].astype(f32)).astype(jnp.int32)
    id1 = as_column(ids[1:2, :].astype(f32)).astype(jnp.int32)
    hit0, hit1 = experts == id0, experts == id1
    chosen = (jnp.where(hit0, 1.0, 0.0) + jnp.where(hit1, 1.0, 0.0)).astype(bf16)
    earlier = jnp.where(t_col < t_row, 1.0, 0.0).astype(bf16)
    count = dot_nn(earlier, chosen)
    pos0 = jnp.sum(jnp.where(hit0, count, 0.0), axis=1, keepdims=True)
    pos1 = jnp.sum(jnp.where(hit1, count, 0.0), axis=1, keepdims=True)

    def offset_of(expert):
        ey, ex = expert // n_x, lax.rem(expert, n_x)
        return lax.rem(ey + n_y - my_y, n_y) * n_x + lax.rem(ex + n_x - my_x, n_x)

    slot0 = offset_of(id0) * cap + pos0.astype(jnp.int32)
    slot1 = offset_of(id1) * cap + pos1.astype(jnp.int32)
    slots = lax.broadcasted_iota(jnp.int32, (toks, n_rows), 1)
    sel_t[...] = (
        jnp.where(slots == slot0, 1.0, 0.0) + jnp.where(slots == slot1, 1.0, 0.0)
    ).astype(bf16)
    p0, p1 = probs[0:1, :], probs[1:2, :]
    w0 = group[...] * p0 / (p0 + p1)
    w1 = group[...] * p1 / (p0 + p1)
    slot0_row, slot1_row = as_row(slot0.astype(f32)), as_row(slot1.astype(f32))
    both = jnp.concatenate([layer_in[...], out_cot[...]], axis=1)

    def select(p, carry):
        base = pl.multiple_of(p * chunk, chunk)
        here = (lax.broadcasted_iota(jnp.int32, (chunk, toks), 0) + p * chunk).astype(f32)
        m0, m1 = here == slot0_row, here == slot1_row
        pick = (jnp.where(m0, 1.0, 0.0) + jnp.where(m1, 1.0, 0.0)).astype(bf16)
        weight = jnp.sum(jnp.where(m0, w0, 0.0) + jnp.where(m1, w1, 0.0), axis=1, keepdims=True)
        picked = dot_nn(pick, both)
        send[0, pl.ds(base, chunk), :] = picked[:, :cols].astype(bf16)
        send[1, pl.ds(base, chunk), :] = (picked[:, cols:] * weight).astype(bf16)
        return carry

    lax.fori_loop(0, pieces, select, 0)
    pl.semaphore_wait(barrier, n_sp + 2)

    give_w = [
        remote(w, part_w.at[k], misc_s.at[k], misc_r.at[k], partner)
        for k, w in enumerate((gate, up))
    ]
    for copy in give_w:
        copy.start()

    def slot_rows(r):
        return pl.ds(pl.multiple_of(r * cap, cap), cap)

    def dispatch(r):
        return remote(
            send.at[:, slot_rows(r), :],
            rows.at[tp, :, slot_rows(r), :],
            a2a_s.at[r],
            a2a_r.at[r],
            (there(r), tp),
        )

    def start_dispatch(r, carry):
        dispatch(r).start()
        return carry

    lax.fori_loop(1, n_sp, start_dispatch, 0)
    rows[tp, :, slot_rows(0), :] = send[:, slot_rows(0), :]

    last = (half - 1) * pieces

    def ring(n_pieces, where, sems_s, sems_r, sems_ds, sems_dr, own_ready, compute, beside):
        h_p = n_pieces // 2
        total = (half - 1) * n_pieces + h_p

        def along(block, p, d, k):
            ref = where(block, p)
            return remote(ref, ref, sems_s.at[d, k], sems_r.at[d, k], above if d == 0 else below)

        def across(block, p, k):
            ref = where(block, p)
            return remote(ref, ref, sems_ds.at[k], sems_dr.at[k], partner)

        def own(p, carry):
            own_ready(p)
            along(tp, p, 0, p).start()
            along(tp, p, 1, p).start()
            across(tp, p, p).start()
            return carry

        lax.fori_loop(0, n_pieces, own, 0)
        beside()

        def own_compute(p, carry):
            across(tp, p, p).wait_recv()
            compute(z, p)
            return carry

        lax.fori_loop(0, n_pieces, own_compute, 0)

        def at(t):
            in_half = t >= (half - 1) * n_pieces
            p_up = lax.rem(t, n_pieces)
            p_dn = jnp.where(in_half, p_up + h_p, p_up)
            hop = t // n_pieces
            return hop, p_up, p_dn

        def step(t, carry):
            hop, p_up, p_dn = at(t)
            b_up, b_dn = zpos(-1 - hop), zpos(1 + hop)
            along(2 * b_up + core, p_up, 0, t).wait_recv()

            @pl.when((hop < half - 2) | ((hop == half - 2) & (p_up < h_p)))
            def _():
                along(2 * b_up + core, p_up, 0, t + n_pieces).start()

            across(2 * b_up + core, p_up, n_pieces + 2 * t).start()
            along(2 * b_dn + core, p_dn, 1, t).wait_recv()

            @pl.when(hop < half - 2)
            def _():
                along(2 * b_dn + core, p_dn, 1, t + n_pieces).start()

            @pl.when((hop == half - 2) & (p_dn >= h_p))
            def _():
                along(2 * b_dn + core, p_dn, 1, t + n_pieces - h_p).start()

            across(2 * b_dn + core, p_dn, n_pieces + 2 * t + 1).start()

            @pl.when(t > 0)
            def _():
                use(t - 1)

            return carry

        def use(t):
            hop, p_up, p_dn = at(t)
            b_up, b_dn = zpos(-1 - hop), zpos(1 + hop)
            across(2 * b_up + 1 - core, p_up, n_pieces + 2 * t).wait_recv()
            compute(b_up, p_up)
            across(2 * b_dn + 1 - core, p_dn, n_pieces + 2 * t + 1).wait_recv()
            compute(b_dn, p_dn)

        lax.fori_loop(0, total, step, 0)
        use(total - 1)

        def drain():
            def one(k, carry):
                along(tp, 0, 0, k).wait_send()
                along(tp, 0, 1, k).wait_send()
                return carry

            lax.fori_loop(0, total, one, 0)

            def other(k, carry):
                across(tp, 0, k).wait_send()
                return carry

            lax.fori_loop(0, n_pieces + 2 * total, other, 0)

        return drain

    def piece_rows(p):
        return pl.ds(pl.multiple_of(p * chunk, chunk), chunk)

    def rows_ready(p):
        for i in range(per):
            r = p * per + i

            @pl.when(r > 0)
            def _():
                dispatch(r).wait_recv()

    def feats(b):
        return pl.ds(pl.multiple_of(b * 2 * cols, 2 * cols), 2 * cols)

    causal = t_col <= t_row

    def to_peers(copy_of):
        def one(r, carry):
            copy_of(r).start()
            return carry

        lax.fori_loop(1, n_sp, one, 0)

    def span_copy(r):
        return remote(span_out, span_in.at[sp], fw_s.at[r], fw_r.at[r], (there(r), tp))

    def future_copy(r):
        return remote(fut_out, fut_in.at[sp], bw_s.at[r], bw_r.at[r], (there(r), tp))

    def attend():
        log_decay = jax.nn.log_sigmoid(logit[...].astype(f32)) / decay_temp
        upto = jnp.where(causal, 1.0, 0.0).astype(bf16)
        cum = fine(dot_nn, upto, log_decay, 3)
        total = cum[toks - 1 : toks, :]
        cumul[...] = cum
        k = key_in[...].astype(f32)
        q_dec[...] = query[...].astype(f32) * DK ** (-0.5) * jnp.exp(cum)
        k_back[...] = k * jnp.exp(-cum)
        k_end[...] = k * jnp.exp(total - cum)
        span_out[0:DK, :] = fine(dot_tn, k_end[...], value[...])
        span_out[DK : 2 * DK, :] = jnp.exp(fine(dot_tn, log_decay, jnp.ones((toks, DV), bf16), 3))
        to_peers(span_copy)
        span_in[sp] = span_out[...]
        found = jnp.where(causal, fine(dot_nt, q_dec[...], k_back[...]), 0.0)
        scores[...] = found
        within[...] = fine(dot_nn, found, value[...])
        pre[...] = jnp.zeros_like(pre)

    def enter():
        def arrived(r, carry):
            span_copy(r).wait_recv()
            return carry

        lax.fori_loop(1, n_sp, arrived, 0)

        def pass_on(s, state):
            return jnp.where(s < sp, span_in[s, DK : 2 * DK, :] * state + span_in[s, 0:DK, :], state)

        entry[...] = lax.fori_loop(0, n_sp, pass_on, jnp.zeros((DK, DV), f32))
        mixed_out = within[...] + fine(dot_nn, q_dec[...], entry[...])
        mix_t[...] = mixed_out.T.astype(bf16)


    def expert_in(b, p):
        w_gu = jnp.concatenate([gate[:, feats(b)], up[:, feats(b)]], axis=0)
        at = piece_rows(p)
        x = jnp.concatenate([rows[2 * b, 0, at, :], rows[2 * b + 1, 0, at, :]], axis=1)
        c = jnp.concatenate([rows[2 * b, 1, at, :], rows[2 * b + 1, 1, at, :]], axis=1)
        pre[at, 0:256] += dot_nt(x, w_gu)
        pre[at, 256:384] += dot_nt(c, down[:, feats(b)])

    drain_rows = ring(
        pieces,
        lambda block, p: rows.at[block, :, piece_rows(p), :],
        ag_s,
        ag_r,
        agd_s,
        agd_r,
        rows_ready,
        expert_in,
        attend,
    )

    def middle(p, carry):
        at = piece_rows(p)
        gate_pre, up_pre, hidden_cot = pre[at, 0:128], pre[at, 128:256], pre[at, 256:384]
        sig = jax.nn.sigmoid(gate_pre)
        active = gate_pre * sig
        hidden = active * up_pre
        up_cot = (hidden_cot * active).astype(bf16)
        gate_cot = (hidden_cot * up_pre * sig * (1.0 + gate_pre * (1.0 - sig))).astype(bf16)
        gu[at, 0:128] = gate_cot
        gu[at, 128:256] = up_cot
        pre[at, 0:128] = hidden
        return carry

    lax.fori_loop(0, pieces, middle, 0)
    give_gu = remote(gu, gu_part, misc_s.at[2], misc_r.at[2], partner)
    give_gu.start()
    gu_t[...] = gu[...].T
    hid_t[...] = pre[:, 0:128].astype(bf16).T
    for copy in give_w:
        copy.wait_recv()
    give_gu.wait_recv()

    h_p = pieces // 2
    rs_total = h_p + (half - 1) * pieces

    def partial(b, p):
        cols_at = pl.ds(pl.multiple_of((2 * b + core) * cols, cols), cols)
        mine = jnp.concatenate([gate[:, cols_at], up[:, cols_at]], axis=0)
        theirs = jnp.concatenate([part_w[0, :, cols_at], part_w[1, :, cols_at]], axis=0)
        at = piece_rows(p)
        return dot_nn(gu[at, :], mine) + dot_nn(gu_part[at, :], theirs)

    def hop_sum(d, k):
        return remote(
            stage.at[d, k],
            inbox.at[d, k],
            rs_s.at[d, k],
            rs_r.at[d, k],
            above if d == 0 else below,
        )

    def first(t, carry):
        for d in range(2):
            stage[d, t] = partial(zpos(half), t + d * h_p).astype(bf16)
            hop_sum(d, t).start()
        return carry

    lax.fori_loop(0, h_p, first, 0)
    enter()

    def gradients(b):
        x = jnp.concatenate([rows[2 * b, 0], rows[2 * b + 1, 0]], axis=1)
        c = jnp.concatenate([rows[2 * b, 1], rows[2 * b + 1, 1]], axis=1)
        both_g = dot_nn(gu_t[...], x)
        gate_g[:, feats(b)] = both_g[0:128]
        up_g[:, feats(b)] = both_g[128:256]
        down_g[:, feats(b)] = dot_nn(hid_t[...], c)

    def later(u, carry):
        t = u + h_p
        hop, p = 1 + u // pieces, lax.rem(u, pieces)
        for d in range(2):
            dest = zpos(half - hop) if d == 0 else zpos(hop - half)
            value = partial(dest, p)
            mine_first = (p >= h_p) if d == 0 else (p < h_p)
            alone = (hop == 1) & mine_first
            k_in = jnp.where(hop == 1, p - d * h_p, t - pieces)

            @pl.when(alone)
            def _():
                stage[d, t] = value.astype(bf16)

            @pl.when(jnp.logical_not(alone))
            def _():
                hop_sum(d, k_in).wait_recv()
                stage[d, t] = (value + inbox[d, k_in].astype(f32)).astype(bf16)

            hop_sum(d, t).start()

        @pl.when(u < n_z)
        def _():
            gradients(u)

        return carry

    lax.fori_loop(0, rs_total - h_p, later, 0)

    def give_back(r):
        return remote(
            ret_out.at[slot_rows(r), :],
            ret.at[slot_rows(r), :],
            back_s.at[r],
            back_r.at[r],
            (back_to(r), tp),
        )

    def finish(p, carry):
        k_in = rs_total - pieces + p
        value = partial(z, p)
        for d in range(2):
            hop_sum(d, k_in).wait_recv()
            value = value + inbox[d, k_in].astype(f32)
        ret_out[piece_rows(p), :] = value.astype(bf16)
        for i in range(per):
            r = p * per + i

            @pl.when(r > 0)
            def _():
                give_back(r).start()

        return carry

    lax.fori_loop(0, pieces, finish, 0)
    for g in range(rs_total - h_p, n_z):
        gradients(g)
    ret[slot_rows(0), :] = ret_out[slot_rows(0), :]

    def take_back(r, carry):
        give_back(r).wait_recv()
        return carry

    lax.fori_loop(1, n_sp, take_back, 0)
    mixed = (out_cot[...].astype(f32) + dot_nn(sel_t[...], ret[...])).astype(bf16)
    full_cot[tp] = mixed

    tok_half = toks // 2
    mixer_cot[...] = jnp.zeros_like(mixer_cot)

    wide = 2 * n_z // n_sp

    def proj_copy(j):
        return remote(
            pj_out.at[j],
            pj_in.at[sp, lax.rem(j, wide)],
            pj_s.at[j],
            pj_r.at[sp, lax.rem(j, wide)],
            (j // wide, tp),
        )

    def project(b, p):
        at = pl.ds(pl.multiple_of(p * tok_half, tok_half), tok_half)
        c = jnp.concatenate([full_cot[2 * b, at, :], full_cot[2 * b + 1, at, :]], axis=1)
        mixer_cot[at, :] += dot_nn(c, out_w[feats(b), :])

        @pl.when(p == 1)
        def _():
            whole = jnp.concatenate([full_cot[2 * b], full_cot[2 * b + 1]], axis=1)
            found = dot_nn(mix_t[...], whole).astype(bf16)
            for i in range(2):
                j = 2 * b + i
                pj_out[j] = found[:, i * cols : (i + 1) * cols]

                @pl.when(j // wide == sp)
                def _():
                    pj_in[sp, lax.rem(j, wide)] = pj_out[j]

                @pl.when(j // wide != sp)
                def _():
                    proj_copy(j).start()

    drain_toks = ring(
        2,
        lambda block, p: full_cot.at[block, pl.ds(pl.multiple_of(p * tok_half, tok_half), tok_half), :],
        tk_s,
        tk_r,
        tkd_s,
        tkd_r,
        lambda p: None,
        project,
        lambda: None,
    )

    cot = mixer_cot[...]
    fut = fine(dot_tn, q_dec[...], cot)
    fut_out[...] = fut.astype(bf16)
    to_peers(future_copy)
    cot_values = jnp.where(causal, fine(dot_nt, cot, value[...]), 0.0)
    cum = cumul[...]
    q_grad = jnp.exp(cum) * (fine(dot_nt, cot, entry[...]) + fine(dot_nn, cot_values, k_back[...]))
    query_g[...] = q_grad * DK ** (-0.5)
    key_part = jnp.exp(-cum) * fine(dot_tn, cot_values, q_dec[...])
    value_g[...] = fine(dot_tn, scores[...], cot)

    def fut_arrived(r, carry):
        future_copy(r).wait_recv()
        return carry

    lax.fori_loop(1, n_sp, fut_arrived, 0)

    def pass_back(i, state):
        s = n_sp - 1 - i
        return jnp.where(
            s > sp, span_in[s, DK : 2 * DK, :] * state + fut_in[s].astype(f32), state
        )

    future = lax.fori_loop(0, n_sp, pass_back, jnp.zeros((DK, DV), f32))
    k_grad = key_part + jnp.exp(cum[toks - 1 : toks, :] - cum) * fine(dot_nt, value[...], future)
    key_g[...] = k_grad
    value_g[...] += fine(dot_nn, k_end[...], future)
    span_end = span_out[DK : 2 * DK, :] * entry[...] + span_out[0:DK, :]
    beyond = fine(dot_nt, jnp.ones((8, DV), bf16), future * span_end, 3)[0:1, :]
    terms = query[...].astype(f32) * DK ** (-0.5) * q_grad - key_in[...].astype(f32) * k_grad
    since = jnp.where(t_col >= t_row, 1.0, 0.0).astype(bf16)
    tail = fine(dot_nn, since, terms, 3) + beyond
    logit_g[...] = tail * jax.nn.sigmoid(-logit[...].astype(f32)) / decay_temp

    def proj_arrived(s, carry):
        for i in range(wide):
            @pl.when(s != sp)
            def _():
                remote(
                    pj_out.at[0], pj_in.at[s, i], pj_s.at[0], pj_r.at[s, i], (sp, tp)
                ).wait_recv()

        return carry

    lax.fori_loop(0, n_sp, proj_arrived, 0)
    for i in range(wide):
        sums = jnp.zeros((128, cols), f32)
        for s in range(n_sp):
            sums = sums + pj_in[s, i].astype(f32)
        proj_g[i * cols : (i + 1) * cols, :] = sums.T

    def sent(r, carry):
        dispatch(r).wait_send()
        give_back(r).wait_send()
        span_copy(r).wait_send()
        future_copy(r).wait_send()
        return carry

    lax.fori_loop(1, n_sp, sent, 0)
    for copy in (*give_w, give_gu):
        copy.wait_send()

    def sums_sent(k, carry):
        for d in range(2):
            hop_sum(d, k).wait_send()
        return carry

    lax.fori_loop(0, rs_total, sums_sent, 0)

    def proj_sent(j, carry):
        @pl.when(j // wide != sp)
        def _():
            proj_copy(j).wait_send()

        return carry

    lax.fori_loop(0, 2 * n_z, proj_sent, 0)
    drain_rows()
    drain_toks()


def local(
    layer_in,
    out_cot,
    route_ids,
    route_probs,
    group_prob,
    gate_weight,
    up_weight,
    down_weight,
    out_weight,
    query,
    key_in,
    value,
    decay_logit,
):
    toks, cols = layer_in.shape
    n_sp, n_tp = lax.axis_size("sp"), lax.axis_size("tp")
    n_x = 4 if n_sp == 16 else n_sp
    n_z = n_tp // 2
    half = n_z // 2
    pieces = 4 if n_sp % 4 == 0 else 2
    width = gate_weight.shape[2]
    n_rows = 4 * toks
    total = (half - 1) * pieces + pieces // 2
    tk_total = (half - 1) * 2 + 1
    chunk = n_rows // pieces
    wide = n_tp // n_sp
    dma = pltpu.SemaphoreType.DMA
    vmem = pl.BlockSpec(memory_space=pltpu.VMEM)
    gate_g, up_g, down_g, *rest = pl.pallas_call(
        functools.partial(moe_kernel, (n_sp, n_x, n_z, pieces)),
        out_shape=(
            jax.ShapeDtypeStruct((128, width), f32),
            jax.ShapeDtypeStruct((128, width), f32),
            jax.ShapeDtypeStruct((128, width), f32),
            jax.ShapeDtypeStruct((wide * cols, DV), f32),
            jax.ShapeDtypeStruct((toks, DK), f32),
            jax.ShapeDtypeStruct((toks, DK), f32),
            jax.ShapeDtypeStruct((toks, DV), f32),
            jax.ShapeDtypeStruct((toks, DK), f32),
        ),
        in_specs=[vmem] * 13,
        out_specs=[vmem] * 8,
        scratch_shapes=[
            pltpu.VMEM((n_tp, toks, cols), bf16),
            pltpu.VMEM((toks, DV), f32),
            pltpu.VMEM((toks, DK), f32),
            pltpu.VMEM((toks, DK), f32),
            pltpu.VMEM((toks, DK), f32),
            pltpu.VMEM((toks, DK), f32),
            pltpu.VMEM((toks, toks), f32),
            pltpu.VMEM((toks, DV), f32),
            pltpu.VMEM((DV, toks), bf16),
            pltpu.VMEM((2 * DK, DV), f32),
            pltpu.VMEM((n_sp, 2 * DK, DV), f32),
            pltpu.VMEM((DK, DV), f32),
            pltpu.VMEM((DK, DV), bf16),
            pltpu.VMEM((n_sp, DK, DV), bf16),
            pltpu.VMEM((n_tp, DV, cols), bf16),
            pltpu.VMEM((n_sp, wide, DV, cols), bf16),
            pltpu.VMEM((2, n_rows, cols), bf16),
            pltpu.VMEM((toks, n_rows), bf16),
            pltpu.VMEM((n_tp, 2, n_rows, cols), bf16),
            pltpu.VMEM((n_rows, 384), f32),
            pltpu.VMEM((2, 128, width), bf16),
            pltpu.VMEM((n_rows, 256), bf16),
            pltpu.VMEM((n_rows, 256), bf16),
            pltpu.VMEM((256, n_rows), bf16),
            pltpu.VMEM((128, n_rows), bf16),
            pltpu.VMEM((2, total, chunk, cols), bf16),
            pltpu.VMEM((2, total, chunk, cols), bf16),
            pltpu.VMEM((n_rows, cols), bf16),
            pltpu.VMEM((n_rows, cols), bf16),
            dma((n_sp,)),
            dma((n_sp,)),
            dma((n_sp,)),
            dma((n_sp,)),
            dma((2, total)),
            dma((2, total)),
            dma((pieces + 2 * total,)),
            dma((pieces + 2 * total,)),
            dma((2, total)),
            dma((2, total)),
            dma((2, tk_total)),
            dma((2, tk_total)),
            dma((2 + 2 * tk_total,)),
            dma((2 + 2 * tk_total,)),
            dma((3,)),
            dma((3,)),
            dma((n_sp,)),
            dma((n_sp,)),
            dma((n_sp,)),
            dma((n_sp,)),
            dma((n_tp,)),
            dma((n_sp, wide)),
        ],
        compiler_params=pltpu.CompilerParams(
            collective_id=0, has_side_effects=True, vmem_limit_bytes=60 * 1024 * 1024
        ),
    )(
        layer_in,
        out_cot,
        route_ids.T,
        route_probs.T,
        group_prob.reshape(1, toks),
        gate_weight[0],
        up_weight[0],
        down_weight[0],
        out_weight,
        query,
        key_in,
        value,
        decay_logit,
    )
    return (gate_g[None], up_g[None], down_g[None], *rest)


def solution(mesh):
    in_specs = (
        P("sp", "tp"),
        P("sp", "tp"),
        P("sp", None),
        P("sp", None),
        P("sp"),
        P("sp", "tp", None),
        P("sp", "tp", None),
        P("sp", "tp", None),
        P(None, "tp"),
        P("sp", "tp"),
        P("sp", "tp"),
        P("sp", "tp"),
        P("sp", "tp"),
    )
    out_specs = (
        P("sp", "tp", None),
        P("sp", "tp", None),
        P("sp", "tp", None),
        P("sp", "tp"),
        P("sp", "tp"),
        P("sp", "tp"),
        P("sp", "tp"),
        P("sp", "tp"),
    )
    return jax.shard_map(local, mesh=mesh, in_specs=in_specs, out_specs=out_specs, check_vma=False)
```

```python
import functools

import jax
import jax.numpy as jnp
from jax import lax
from jax.experimental import pallas as pl
from jax.experimental.pallas import tpu as pltpu
from jax.sharding import PartitionSpec as P

DK = 64
DV = 128


decay_temp = 16.0
f32, bf16 = jnp.float32, jnp.bfloat16
MESH = pl.DeviceIdType.MESH


def dot_nt(a, b):
    return lax.dot_general(a, b, (((1,), (1,)), ((), ())), preferred_element_type=f32)


def dot_nn(a, b):
    return lax.dot_general(a, b, (((1,), (0,)), ((), ())), preferred_element_type=f32)


def dot_tn(a, b):
    return lax.dot_general(a, b, (((0,), (0,)), ((), ())), preferred_element_type=f32)


def parts_of(x, n):
    if x.dtype == bf16:
        return [x]
    found = []
    for _ in range(n):
        top = x.astype(bf16)
        found.append(top)
        x = x - top.astype(f32)
    return found


def fine(dot, a, b, n=2):
    a, b = parts_of(a, n), parts_of(b, n)
    terms = [dot(p, q) for i, p in enumerate(a) for j, q in enumerate(b) if i + j < n]
    total = terms[-1]
    for term in terms[-2::-1]:
        total = total + term
    return total


def moe_kernel(
    sizes,
    ids,
    probs,
    group,
    *refs,
):
    held, given, kept = refs[:10], refs[10:18], refs[18:]
    expert_kernel(sizes, ids, probs, group, held, given, *kept)


def expert_kernel(
    sizes,
    ids,
    probs,
    group,
    held,
    given,
    layer_in,
    out_cot,
    gate,
    up,
    down,
    out_w,
    query,
    key_in,
    value,
    logit,
    gate_g,
    up_g,
    down_g,
    proj_g,
    query_g,
    key_g,
    value_g,
    logit_g,
    full_cot,
    mixer_cot,
    q_dec,
    k_back,
    k_end,
    cumul,
    scores,
    within,
    mix_t,
    span_out,
    span_in,
    entry,
    fut_out,
    fut_in,
    pj_out,
    pj_in,
    send,
    sel_t,
    rows,
    pre,
    part_w,
    gu,
    gu_part,
    gu_t,
    hid_t,
    stage,
    inbox,
    ret_out,
    ret,
    a2a_s,
    a2a_r,
    back_s,
    back_r,
    ag_s,
    ag_r,
    agd_s,
    agd_r,
    rs_s,
    rs_r,
    tk_s,
    tk_r,
    tkd_s,
    tkd_r,
    misc_s,
    misc_r,
    gu_s,
    gu_r,
    fw_s,
    fw_r,
    bw_s,
    bw_r,
    pj_s,
    pj_r,
    load_s,
    give_s,
):
    n_sp, n_x, n_z, pieces = sizes
    n_y = n_sp // n_x
    half = n_z // 2
    targets = (layer_in, out_cot, gate, up, down, out_w, query, key_in, value, logit)
    loaded = [
        pltpu.make_async_copy(source, target, load_s.at[k])
        for k, (source, target) in enumerate(zip(held, targets))
    ]
    for k in (0, 1, 2, 3, 6, 7, 8, 9, 4, 5):
        loaded[k].start()
    results = (gate_g, up_g, down_g, proj_g, query_g, key_g, value_g, logit_g)
    stored = [
        pltpu.make_async_copy(source, target, give_s.at[k])
        for k, (source, target) in enumerate(zip(results, given))
    ]
    toks, cols = layer_in.shape
    cap = 4 * toks // n_sp
    n_rows = n_sp * cap
    per = n_sp // pieces
    chunk = n_rows // pieces
    sp = lax.axis_index("sp")
    tp = lax.axis_index("tp")
    core = lax.rem(tp, 2)
    z = tp // 2
    z_up = lax.rem(z + 1, n_z)
    z_dn = lax.rem(z + n_z - 1, n_z)
    partner = (sp, 2 * z + 1 - core)
    above, below = (sp, 2 * z_up + core), (sp, 2 * z_dn + core)
    my_y, my_x = sp // n_x, lax.rem(sp, n_x)

    def there(r):
        ry, rx = r // n_x, lax.rem(r, n_x)
        return lax.rem(my_y + ry, n_y) * n_x + lax.rem(my_x + rx, n_x)

    def back_to(r):
        ry, rx = r // n_x, lax.rem(r, n_x)
        return lax.rem(my_y + n_y - ry, n_y) * n_x + lax.rem(my_x + n_x - rx, n_x)

    def zpos(d):
        return lax.rem(z + d + n_z, n_z)

    def remote(src, dst, s, r, dev):
        return pltpu.make_async_remote_copy(
            src_ref=src, dst_ref=dst, send_sem=s, recv_sem=r, device_id=dev, device_id_type=MESH
        )

    barrier = pltpu.get_barrier_semaphore()
    for r in range(1, n_sp):
        pl.semaphore_signal(barrier, inc=1, device_id=(there(r), tp), device_id_type=MESH)
    for dev in (partner, above, below):
        pl.semaphore_signal(barrier, inc=1, device_id=dev, device_id_type=MESH)

    t_row = lax.broadcasted_iota(jnp.int32, (toks, toks), 0)
    t_col = lax.broadcasted_iota(jnp.int32, (toks, toks), 1)
    diagonal = t_row == t_col

    def as_row(column):
        return jnp.sum(jnp.where(diagonal, column, 0.0), axis=0, keepdims=True)

    def as_column(row):
        return jnp.sum(jnp.where(diagonal, row, 0.0), axis=1, keepdims=True)

    experts = lax.broadcasted_iota(jnp.int32, (toks, 128), 1)
    id0 = as_column(ids[0:1, :].astype(f32)).astype(jnp.int32)
    id1 = as_column(ids[1:2, :].astype(f32)).astype(jnp.int32)
    hit0, hit1 = experts == id0, experts == id1
    chosen = (jnp.where(hit0, 1.0, 0.0) + jnp.where(hit1, 1.0, 0.0)).astype(bf16)
    earlier = jnp.where(t_col < t_row, 1.0, 0.0).astype(bf16)
    count = dot_nn(earlier, chosen)
    pos0 = jnp.sum(jnp.where(hit0, count, 0.0), axis=1, keepdims=True)
    pos1 = jnp.sum(jnp.where(hit1, count, 0.0), axis=1, keepdims=True)

    def offset_of(expert):
        ey, ex = expert // n_x, lax.rem(expert, n_x)
        return lax.rem(ey + n_y - my_y, n_y) * n_x + lax.rem(ex + n_x - my_x, n_x)

    slot0 = offset_of(id0) * cap + pos0.astype(jnp.int32)
    slot1 = offset_of(id1) * cap + pos1.astype(jnp.int32)
    slots = lax.broadcasted_iota(jnp.int32, (toks, n_rows), 1)
    sel_t[...] = (
        jnp.where(slots == slot0, 1.0, 0.0) + jnp.where(slots == slot1, 1.0, 0.0)
    ).astype(bf16)
    p0, p1 = probs[0:1, :], probs[1:2, :]
    group_row = group[...].reshape(1, toks)
    w0 = group_row * p0 / (p0 + p1)
    w1 = group_row * p1 / (p0 + p1)
    slot0_row, slot1_row = as_row(slot0.astype(f32)), as_row(slot1.astype(f32))
    loaded[0].wait()
    loaded[1].wait()
    both = jnp.concatenate([layer_in[...], out_cot[...]], axis=1)

    def select(p, carry):
        base = pl.multiple_of(p * chunk, chunk)
        here = (lax.broadcasted_iota(jnp.int32, (chunk, toks), 0) + p * chunk).astype(f32)
        m0, m1 = here == slot0_row, here == slot1_row
        pick = (jnp.where(m0, 1.0, 0.0) + jnp.where(m1, 1.0, 0.0)).astype(bf16)
        weight = jnp.sum(jnp.where(m0, w0, 0.0) + jnp.where(m1, w1, 0.0), axis=1, keepdims=True)
        picked = dot_nn(pick, both)
        send[0, pl.ds(base, chunk), :] = picked[:, :cols].astype(bf16)
        send[1, pl.ds(base, chunk), :] = (picked[:, cols:] * weight).astype(bf16)
        return carry

    lax.fori_loop(0, pieces, select, 0)
    pl.semaphore_wait(barrier, n_sp + 2)

    give_w = [
        remote(w, part_w.at[k], misc_s.at[k], misc_r.at[k], partner)
        for k, w in enumerate((gate, up))
    ]
    loaded[2].wait()
    loaded[3].wait()
    for copy in give_w:
        copy.start()

    def slot_rows(r):
        return pl.ds(pl.multiple_of(r * cap, cap), cap)

    def dispatch(r):
        return remote(
            send.at[:, slot_rows(r), :],
            rows.at[tp, :, slot_rows(r), :],
            a2a_s,
            a2a_r.at[r // per],
            (there(r), tp),
        )

    def start_dispatch(r, carry):
        dispatch(r).start()
        return carry

    lax.fori_loop(1, n_sp, start_dispatch, 0)
    rows[tp, :, slot_rows(0), :] = send[:, slot_rows(0), :]

    last = (half - 1) * pieces

    def ring(n_pieces, where, sems_s, sems_r, sems_ds, sems_dr, own_ready, compute, beside):
        h_p = n_pieces // 2
        total = (half - 1) * n_pieces + h_p

        def along(block, p, d, k):
            ref = where(block, p)
            return remote(ref, ref, sems_s, sems_r.at[d, k], above if d == 0 else below)

        def across(block, p, k):
            ref = where(block, p)
            return remote(ref, ref, sems_ds, sems_dr.at[k], partner)

        def own(p, carry):
            own_ready(p)
            along(tp, p, 0, p).start()
            along(tp, p, 1, p).start()
            across(tp, p, p).start()
            return carry

        lax.fori_loop(0, n_pieces, own, 0)
        beside()

        def own_compute(p, carry):
            across(tp, p, p).wait_recv()
            compute(z, p)
            return carry

        lax.fori_loop(0, n_pieces, own_compute, 0)

        def at(t):
            in_half = t >= (half - 1) * n_pieces
            p_up = lax.rem(t, n_pieces)
            p_dn = jnp.where(in_half, p_up + h_p, p_up)
            hop = t // n_pieces
            return hop, p_up, p_dn

        def step(t, carry):
            hop, p_up, p_dn = at(t)
            b_up, b_dn = zpos(-1 - hop), zpos(1 + hop)
            along(2 * b_up + core, p_up, 0, t).wait_recv()

            @pl.when((hop < half - 2) | ((hop == half - 2) & (p_up < h_p)))
            def _():
                along(2 * b_up + core, p_up, 0, t + n_pieces).start()

            across(2 * b_up + core, p_up, n_pieces + 2 * t).start()
            along(2 * b_dn + core, p_dn, 1, t).wait_recv()

            @pl.when(hop < half - 2)
            def _():
                along(2 * b_dn + core, p_dn, 1, t + n_pieces).start()

            @pl.when((hop == half - 2) & (p_dn >= h_p))
            def _():
                along(2 * b_dn + core, p_dn, 1, t + n_pieces - h_p).start()

            across(2 * b_dn + core, p_dn, n_pieces + 2 * t + 1).start()

            @pl.when(t > 0)
            def _():
                use(t - 1)

            return carry

        def use(t):
            hop, p_up, p_dn = at(t)
            b_up, b_dn = zpos(-1 - hop), zpos(1 + hop)
            across(2 * b_up + 1 - core, p_up, n_pieces + 2 * t).wait_recv()
            compute(b_up, p_up)
            across(2 * b_dn + 1 - core, p_dn, n_pieces + 2 * t + 1).wait_recv()
            compute(b_dn, p_dn)

        lax.fori_loop(0, total, step, 0)
        use(total - 1)


    def piece_rows(p):
        return pl.ds(pl.multiple_of(p * chunk, chunk), chunk)

    def rows_ready(p):
        @pl.when((p == 0) & (per > 1))
        def _():
            came = rows.at[tp, :, cap:chunk, :]
            remote(came, came, a2a_s, a2a_r.at[0], partner).wait_recv()

        @pl.when(p > 0)
        def _():
            came = rows.at[tp, :, piece_rows(p), :]
            remote(came, came, a2a_s, a2a_r.at[p], partner).wait_recv()

    def feats(b):
        return pl.ds(pl.multiple_of(b * 2 * cols, 2 * cols), 2 * cols)

    causal = t_col <= t_row

    def to_peers(copy_of):
        def one(r, carry):
            copy_of(r).start()
            return carry

        lax.fori_loop(1, n_sp, one, 0)

    def span_copy(r):
        return remote(span_out, span_in.at[sp], fw_s, fw_r, (there(r), tp))

    def future_copy(r):
        return remote(fut_out, fut_in.at[sp], bw_s.at[r], bw_r.at[sp], (there(r), tp))

    def to_earlier(r, carry):
        @pl.when(there(r) < sp)
        def _():
            future_copy(r).start()

        return carry

    def attend():
        for k in (6, 7, 8, 9, 4, 5):
            loaded[k].wait()
        log_decay = jax.nn.log_sigmoid(logit[...].astype(f32).T) / decay_temp
        upto = jnp.where(causal, 1.0, 0.0).astype(bf16)
        cum = fine(dot_nn, upto, log_decay, 3)
        total = cum[toks - 1 : toks, :]
        cumul[...] = cum
        k = key_in[...].astype(f32).T
        q_dec[...] = query[...].astype(f32).T * DK ** (-0.5) * jnp.exp(cum)
        k_back[...] = k * jnp.exp(-cum)
        k_end[...] = k * jnp.exp(total - cum)
        span_out[0:DK, :] = fine(dot_tn, k_end[...], value[...])
        span_out[DK : 2 * DK, :] = jnp.exp(fine(dot_tn, log_decay, jnp.ones((toks, DV), bf16), 3))
        to_peers(span_copy)
        span_in[sp] = span_out[...]
        found = jnp.where(causal, fine(dot_nt, q_dec[...], k_back[...]), 0.0)
        scores[...] = found
        within[...] = fine(dot_nn, found, value[...])
        pre[...] = jnp.zeros_like(pre)

    def enter():
        came = span_in.at[1:]
        remote(came, came, fw_s, fw_r, partner).wait_recv()

        def pass_on(s, state):
            return jnp.where(s < sp, span_in[s, DK : 2 * DK, :] * state + span_in[s, 0:DK, :], state)

        entry[...] = lax.fori_loop(0, n_sp, pass_on, jnp.zeros((DK, DV), f32))
        mixed_out = within[...] + fine(dot_nn, q_dec[...], entry[...])
        mix_t[...] = mixed_out.T.astype(bf16)


    def expert_in(b, p):
        w_gu = jnp.concatenate([gate[:, feats(b)], up[:, feats(b)]], axis=0)
        at = piece_rows(p)
        x = jnp.concatenate([rows[2 * b, 0, at, :], rows[2 * b + 1, 0, at, :]], axis=1)
        c = jnp.concatenate([rows[2 * b, 1, at, :], rows[2 * b + 1, 1, at, :]], axis=1)
        pre[at, 0:256] += dot_nt(x, w_gu)
        pre[at, 256:384] += dot_nt(c, down[:, feats(b)])

    ring(
        pieces,
        lambda block, p: rows.at[block, :, piece_rows(p), :],
        ag_s,
        ag_r,
        agd_s,
        agd_r,
        rows_ready,
        expert_in,
        attend,
    )

    h_p = pieces // 2

    def give_gu(p):
        at = piece_rows(p)
        return remote(gu.at[at, :], gu_part.at[at, :], gu_s, gu_r.at[p], partner)

    def middle(i, carry):
        p = i // 2 + lax.rem(i, 2) * h_p
        at = piece_rows(p)
        gate_pre, up_pre, hidden_cot = pre[at, 0:128], pre[at, 128:256], pre[at, 256:384]
        sig = jax.nn.sigmoid(gate_pre)
        active = gate_pre * sig
        gu[at, 0:128] = (hidden_cot * up_pre * sig * (1.0 + gate_pre * (1.0 - sig))).astype(bf16)
        gu[at, 128:256] = (hidden_cot * active).astype(bf16)
        give_gu(p).start()
        pre[at, 0:128] = active * up_pre
        return carry

    lax.fori_loop(0, pieces, middle, 0)
    for copy in give_w:
        copy.wait_recv()

    rs_total = h_p + (half - 1) * pieces

    def partial(b, p):
        cols_at = pl.ds(pl.multiple_of((2 * b + core) * cols, cols), cols)
        mine = jnp.concatenate([gate[:, cols_at], up[:, cols_at]], axis=0)
        theirs = jnp.concatenate([part_w[0, :, cols_at], part_w[1, :, cols_at]], axis=0)
        at = piece_rows(p)
        return dot_nn(gu[at, :], mine) + dot_nn(gu_part[at, :], theirs)

    def hop_sum(d, k):
        return remote(
            stage.at[d, k],
            inbox.at[d, k],
            rs_s,
            rs_r.at[d, k],
            above if d == 0 else below,
        )

    def first(t, carry):
        for d in range(2):
            give_gu(t + d * h_p).wait_recv()
            stage[d, t] = partial(zpos(half), t + d * h_p).astype(bf16)
            hop_sum(d, t).start()
        return carry

    lax.fori_loop(0, h_p, first, 0)
    gu_t[...] = gu[...].T
    hid_t[...] = pre[:, 0:128].astype(bf16).T
    enter()

    def gradients(b):
        x = jnp.concatenate([rows[2 * b, 0], rows[2 * b + 1, 0]], axis=1)
        c = jnp.concatenate([rows[2 * b, 1], rows[2 * b + 1, 1]], axis=1)
        both_g = dot_nn(gu_t[...], x)
        gate_g[:, feats(b)] = both_g[0:128]
        up_g[:, feats(b)] = both_g[128:256]
        down_g[:, feats(b)] = dot_nn(hid_t[...], c)

    def later(u, carry):
        t = u + h_p
        hop, p = 1 + u // pieces, lax.rem(u, pieces)
        for d in range(2):
            dest = zpos(half - hop) if d == 0 else zpos(hop - half)
            value = partial(dest, p)
            mine_first = (p >= h_p) if d == 0 else (p < h_p)
            alone = (hop == 1) & mine_first
            k_in = jnp.where(hop == 1, p - d * h_p, t - pieces)

            @pl.when(alone)
            def _():
                stage[d, t] = value.astype(bf16)

            @pl.when(jnp.logical_not(alone))
            def _():
                hop_sum(d, k_in).wait_recv()
                stage[d, t] = (value + inbox[d, k_in].astype(f32)).astype(bf16)

            hop_sum(d, t).start()

        @pl.when(u < n_z)
        def _():
            gradients(u)

        return carry

    lax.fori_loop(0, rs_total - h_p, later, 0)

    def give_back(r):
        return remote(
            ret_out.at[slot_rows(r), :],
            ret.at[slot_rows(r), :],
            back_s,
            back_r,
            (back_to(r), tp),
        )

    def finish(p, carry):
        k_in = rs_total - pieces + p
        value = partial(z, p)
        for d in range(2):
            hop_sum(d, k_in).wait_recv()
            value = value + inbox[d, k_in].astype(f32)
        ret_out[piece_rows(p), :] = value.astype(bf16)
        for i in range(per):
            r = p * per + i

            @pl.when(r > 0)
            def _():
                give_back(r).start()

        return carry

    lax.fori_loop(0, pieces, finish, 0)
    for g in range(rs_total - h_p, n_z):
        gradients(g)
    for k in range(3):
        stored[k].start()
    ret[slot_rows(0), :] = ret_out[slot_rows(0), :]

    others = ret.at[cap:, :]
    remote(others, others, back_s, back_r, partner).wait_recv()
    mixed = (out_cot[...].astype(f32) + dot_nn(sel_t[...], ret[...])).astype(bf16)
    full_cot[tp] = mixed

    tok_half = toks // 2
    mixer_cot[...] = jnp.zeros_like(mixer_cot)

    wide = 2 * n_z // n_sp

    def proj_copy(j):
        return remote(
            pj_out.at[j],
            pj_in.at[sp, lax.rem(j, wide)],
            pj_s,
            pj_r,
            (j // wide, tp),
        )

    def proj_send(j):
        @pl.when(j // wide != sp)
        def _():
            proj_copy(j).start()

    def project(b, p):
        at = pl.ds(pl.multiple_of(p * tok_half, tok_half), tok_half)
        c = jnp.concatenate([full_cot[2 * b, at, :], full_cot[2 * b + 1, at, :]], axis=1)
        mixer_cot[at, :] += dot_nn(c, out_w[feats(b), :])

        @pl.when(p == 1)
        def _():
            whole = jnp.concatenate([full_cot[2 * b], full_cot[2 * b + 1]], axis=1)
            found = dot_nn(mix_t[...], whole).astype(bf16)
            for i in range(2):
                j = 2 * b + i
                pj_out[j] = found[:, i * cols : (i + 1) * cols]

                @pl.when(j // wide == sp)
                def _():
                    pj_in[sp, lax.rem(j, wide)] = pj_out[j]

                away = lax.rem(b - z + n_z, n_z)

                @pl.when((away < half - 1) | (away > half + 1))
                def _():
                    proj_send(j)

    ring(
        2,
        lambda block, p: full_cot.at[block, pl.ds(pl.multiple_of(p * tok_half, tok_half), tok_half), :],
        tk_s,
        tk_r,
        tkd_s,
        tkd_r,
        lambda p: None,
        project,
        lambda: None,
    )

    cot = mixer_cot[...]
    fut = fine(dot_tn, q_dec[...], cot)
    fut_out[...] = fut.astype(bf16)
    lax.fori_loop(1, n_sp, to_earlier, 0)
    for d in (half - 1, half, half + 1):
        for i in range(2):
            proj_send(2 * zpos(d) + i)
    cot_values = jnp.where(causal, fine(dot_nt, cot, value[...]), 0.0)
    cum = cumul[...]
    q_grad = jnp.exp(cum) * (fine(dot_nt, cot, entry[...]) + fine(dot_nn, cot_values, k_back[...]))
    query_g[...] = (q_grad * DK ** (-0.5)).T
    key_part = jnp.exp(-cum) * fine(dot_tn, cot_values, q_dec[...])
    value_g[...] = fine(dot_tn, scores[...], cot)

    def fut_arrived(s, carry):
        @pl.when(s > sp)
        def _():
            remote(fut_out, fut_in.at[s], bw_s.at[0], bw_r.at[s], partner).wait_recv()

        return carry

    lax.fori_loop(0, n_sp, fut_arrived, 0)

    def pass_back(i, state):
        s = n_sp - 1 - i
        later_on = span_in[s, DK : 2 * DK, :] * state + fut_in[s].astype(f32)
        return jnp.where(s > sp, later_on, state)

    future = lax.fori_loop(0, n_sp, pass_back, jnp.zeros((DK, DV), f32))
    k_grad = key_part + jnp.exp(cum[toks - 1 : toks, :] - cum) * fine(dot_nt, value[...], future)
    k_grad_t = k_grad.T
    key_g[...] = k_grad_t
    value_g[...] += fine(dot_nn, k_end[...], future)
    span_end = span_out[DK : 2 * DK, :] * entry[...] + span_out[0:DK, :]
    beyond = jnp.sum(future * span_end, axis=1, keepdims=True)
    terms = query[...].astype(f32) * query_g[...] - key_in[...].astype(f32) * k_grad_t
    since = jnp.where(t_row >= t_col, 1.0, 0.0).astype(bf16)
    tail = fine(dot_nn, terms, since, 3) + beyond
    logit_g[...] = tail * jax.nn.sigmoid(-logit[...].astype(f32)) / decay_temp

    came = pj_in.at[1:]
    remote(came, came, pj_s, pj_r, partner).wait_recv()
    for i in range(wide):
        sums = jnp.zeros((128, cols), f32)
        for s in range(n_sp):
            sums = sums + pj_in[s, i].astype(f32)
        proj_g[i * cols : (i + 1) * cols, :] = sums.T

    for k in range(3, 8):
        stored[k].start()

    for copy in give_w:
        copy.wait_send()

    def fut_sent(r, carry):
        @pl.when(there(r) < sp)
        def _():
            future_copy(r).wait_send()

        return carry

    lax.fori_loop(1, n_sp, fut_sent, 0)
    for sent, sem in (
        (send.at[:, cap:, :], a2a_s),
        (ret.at[cap:, :], back_s),
        (span_in.at[1:], fw_s),
        (pj_in.at[1:], pj_s),
        (rows.at[: n_z - 1], ag_s),
        (rows.at[:n_z], agd_s),
        (full_cot.at[: n_z - 1], tk_s),
        (full_cot.at[:n_z], tkd_s),
        (stage, rs_s),
        (gu, gu_s),
    ):
        remote(sent, sent, sem, back_r, partner).wait_send()
    for copy in stored:
        copy.wait()


def store_kernel(*refs):
    taken = [
        pltpu.make_async_copy(source, target, refs[24].at[k])
        for k, (source, target) in enumerate(zip(refs[:8], refs[16:24]))
    ]
    stored = [
        pltpu.make_async_copy(source, target, refs[25].at[k])
        for k, (source, target) in enumerate(zip(refs[16:24], refs[8:16]))
    ]
    for copy in taken:
        copy.start()
    for first, second in zip(taken, stored):
        first.wait()
        second.start()
    for copy in stored:
        copy.wait()


def local(
    layer_in,
    out_cot,
    route_ids,
    route_probs,
    group_prob,
    gate_weight,
    up_weight,
    down_weight,
    out_weight,
    query,
    key_in,
    value,
    decay_logit,
):
    toks, cols = layer_in.shape
    n_sp, n_tp = lax.axis_size("sp"), lax.axis_size("tp")
    n_x = 4 if n_sp == 16 else n_sp
    n_z = n_tp // 2
    half = n_z // 2
    pieces = 4 if n_sp % 4 == 0 else 2
    width = gate_weight.shape[2]
    n_rows = 4 * toks
    total = (half - 1) * pieces + pieces // 2
    tk_total = (half - 1) * 2 + 1
    chunk = n_rows // pieces
    wide = n_tp // n_sp
    dma = pltpu.SemaphoreType.DMA
    vmem = pl.BlockSpec(memory_space=pltpu.VMEM)
    hbm = pl.BlockSpec(memory_space=pltpu.HBM)
    small = (DK, toks)
    shapes = ((128, width),) * 3 + ((wide * cols, DV), small, small, (toks, DV), small)
    grads = pl.pallas_call(
        functools.partial(moe_kernel, (n_sp, n_x, n_z, pieces)),
        out_shape=tuple(jax.ShapeDtypeStruct(shape, f32) for shape in shapes),
        in_specs=[vmem] * 3 + [hbm] * 10,
        out_specs=[hbm] * 8,
        scratch_shapes=[
            pltpu.VMEM((toks, cols), bf16),
            pltpu.VMEM((toks, cols), bf16),
            pltpu.VMEM((128, width), bf16),
            pltpu.VMEM((128, width), bf16),
            pltpu.VMEM((128, width), bf16),
            pltpu.VMEM((width, DV), bf16),
            pltpu.VMEM((DK, toks), bf16),
            pltpu.VMEM((DK, toks), bf16),
            pltpu.VMEM((toks, DV), bf16),
            pltpu.VMEM((DK, toks), bf16),
            *(pltpu.VMEM(shape, f32) for shape in shapes),
            pltpu.VMEM((n_tp, toks, cols), bf16),
            pltpu.VMEM((toks, DV), f32),
            pltpu.VMEM((toks, DK), f32),
            pltpu.VMEM((toks, DK), f32),
            pltpu.VMEM((toks, DK), f32),
            pltpu.VMEM((toks, DK), f32),
            pltpu.VMEM((toks, toks), f32),
            pltpu.VMEM((toks, DV), f32),
            pltpu.VMEM((DV, toks), bf16),
            pltpu.VMEM((2 * DK, DV), f32),
            pltpu.VMEM((n_sp, 2 * DK, DV), f32),
            pltpu.VMEM((DK, DV), f32),
            pltpu.VMEM((DK, DV), bf16),
            pltpu.VMEM((n_sp, DK, DV), bf16),
            pltpu.VMEM((n_tp, DV, cols), bf16),
            pltpu.VMEM((n_sp, wide, DV, cols), bf16),
            pltpu.VMEM((2, n_rows, cols), bf16),
            pltpu.VMEM((toks, n_rows), bf16),
            pltpu.VMEM((n_tp, 2, n_rows, cols), bf16),
            pltpu.VMEM((n_rows, 384), f32),
            pltpu.VMEM((2, 128, width), bf16),
            pltpu.VMEM((n_rows, 256), bf16),
            pltpu.VMEM((n_rows, 256), bf16),
            pltpu.VMEM((256, n_rows), bf16),
            pltpu.VMEM((128, n_rows), bf16),
            pltpu.VMEM((2, total, chunk, cols), bf16),
            pltpu.VMEM((2, total, chunk, cols), bf16),
            pltpu.VMEM((n_rows, cols), bf16),
            pltpu.VMEM((n_rows, cols), bf16),
            dma(()),
            dma((pieces,)),
            dma(()),
            dma(()),
            dma(()),
            dma((2, total)),
            dma(()),
            dma((pieces + 2 * total,)),
            dma(()),
            dma((2, total)),
            dma(()),
            dma((2, tk_total)),
            dma(()),
            dma((2 + 2 * tk_total,)),
            dma((2,)),
            dma((2,)),
            dma(()),
            dma((pieces,)),
            dma(()),
            dma(()),
            dma((n_sp,)),
            dma((n_sp,)),
            dma(()),
            dma(()),
            dma((10,)),
            dma((8,)),
        ],
        compiler_params=pltpu.CompilerParams(
            collective_id=0, has_side_effects=True, vmem_limit_bytes=60 * 1024 * 1024
        ),
    )(
        route_ids.T,
        route_probs.T,
        group_prob,
        layer_in,
        out_cot,
        gate_weight[0],
        up_weight[0],
        down_weight[0],
        out_weight,
        query.T,
        key_in.T,
        value,
        decay_logit.T,
    )
    gate_g, up_g, down_g, proj_g, query_g, key_g, value_g, logit_g = pl.pallas_call(
        store_kernel,
        out_shape=tuple(jax.ShapeDtypeStruct(g.shape, g.dtype) for g in grads),
        in_specs=[hbm] * 8,
        out_specs=[hbm] * 8,
        scratch_shapes=[*(pltpu.VMEM(g.shape, g.dtype) for g in grads), dma((8,)), dma((8,))],
        compiler_params=pltpu.CompilerParams(vmem_limit_bytes=60 * 1024 * 1024),
    )(*grads)
    return (
        gate_g[None],
        up_g[None],
        down_g[None],
        proj_g,
        query_g.T,
        key_g.T,
        value_g,
        logit_g.T,
    )


def solution(mesh):
    in_specs = (
        P("sp", "tp"),
        P("sp", "tp"),
        P("sp", None),
        P("sp", None),
        P("sp"),
        P("sp", "tp", None),
        P("sp", "tp", None),
        P("sp", "tp", None),
        P(None, "tp"),
        P("sp", "tp"),
        P("sp", "tp"),
        P("sp", "tp"),
        P("sp", "tp"),
    )
    out_specs = (
        P("sp", "tp", None),
        P("sp", "tp", None),
        P("sp", "tp", None),
        P("sp", "tp"),
        P("sp", "tp"),
        P("sp", "tp"),
        P("sp", "tp"),
        P("sp", "tp"),
    )
    return jax.shard_map(local, mesh=mesh, in_specs=in_specs, out_specs=out_specs, check_vma=False)
```

```python
import functools

import jax
import jax.numpy as jnp
from jax import lax
from jax.experimental import pallas as pl
from jax.experimental.pallas import tpu as pltpu
from jax.sharding import PartitionSpec as P

DK = 64
DV = 128


decay_temp = 16.0
f32, bf16 = jnp.float32, jnp.bfloat16
MESH = pl.DeviceIdType.MESH


def dot_nt(a, b):
    return lax.dot_general(a, b, (((1,), (1,)), ((), ())), preferred_element_type=f32)


def dot_nn(a, b):
    return lax.dot_general(a, b, (((1,), (0,)), ((), ())), preferred_element_type=f32)


def dot_tn(a, b):
    return lax.dot_general(a, b, (((0,), (0,)), ((), ())), preferred_element_type=f32)


def parts_of(x, n):
    if x.dtype == bf16:
        return [x]
    found = []
    for _ in range(n):
        top = x.astype(bf16)
        found.append(top)
        x = x - top.astype(f32)
    return found


def fine(dot, a, b, n=2):
    a, b = parts_of(a, n), parts_of(b, n)
    terms = [dot(p, q) for i, p in enumerate(a) for j, q in enumerate(b) if i + j < n]
    total = terms[-1]
    for term in terms[-2::-1]:
        total = total + term
    return total


def moe_kernel(
    sizes,
    ids,
    probs,
    group,
    *refs,
):
    held, given, kept = refs[:10], refs[10:18], refs[18:]
    expert_kernel(sizes, ids, probs, group, held, given, *kept)


def expert_kernel(
    sizes,
    ids,
    probs,
    group,
    held,
    given,
    layer_in,
    out_cot,
    gate,
    up,
    down,
    out_w,
    query,
    key_in,
    value,
    logit,
    gate_g,
    up_g,
    down_g,
    proj_g,
    query_g,
    key_g,
    value_g,
    logit_g,
    full_cot,
    mixer_cot,
    q_dec,
    k_back,
    k_end,
    cumul,
    scores,
    within,
    mix_t,
    span_out,
    span_in,
    entry,
    fut_out,
    fut_in,
    pj_out,
    pj_in,
    send,
    sel_t,
    rows,
    pre,
    part_w,
    gu,
    gu_part,
    gu_t,
    hid_t,
    stage,
    inbox,
    ret_out,
    ret,
    a2a_s,
    a2a_r,
    back_s,
    back_r,
    ag_s,
    ag_r,
    agd_s,
    agd_r,
    rs_s,
    rs_r,
    tk_s,
    tk_r,
    tkd_s,
    tkd_r,
    misc_s,
    misc_r,
    gu_s,
    gu_r,
    fw_s,
    fw_r,
    bw_s,
    bw_r,
    pj_s,
    pj_r,
    load_s,
    give_s,
):
    n_sp, n_x, n_z, pieces = sizes
    n_y = n_sp // n_x
    half = n_z // 2
    targets = (layer_in, out_cot, gate, up, down, out_w, query, key_in, value, logit)
    loaded = [
        pltpu.make_async_copy(source, target, load_s.at[k])
        for k, (source, target) in enumerate(zip(held, targets))
    ]
    for k in (0, 1, 2, 3, 6, 7, 8, 9, 4, 5):
        loaded[k].start()
    results = (gate_g, up_g, down_g, proj_g, query_g, key_g, value_g, logit_g)
    stored = [
        pltpu.make_async_copy(source, target, give_s.at[k])
        for k, (source, target) in enumerate(zip(results, given))
    ]
    toks, cols = layer_in.shape
    cap = 4 * toks // n_sp
    n_rows = n_sp * cap
    per = n_sp // pieces
    chunk = n_rows // pieces
    sp = lax.axis_index("sp")
    tp = lax.axis_index("tp")
    core = lax.rem(tp, 2)
    z = tp // 2
    z_up = lax.rem(z + 1, n_z)
    z_dn = lax.rem(z + n_z - 1, n_z)
    partner = (sp, 2 * z + 1 - core)
    above, below = (sp, 2 * z_up + core), (sp, 2 * z_dn + core)
    two_up = (sp, 2 * lax.rem(z + 2, n_z) + core)
    two_dn = (sp, 2 * lax.rem(z + n_z - 2, n_z) + core)
    my_y, my_x = sp // n_x, lax.rem(sp, n_x)

    def there(r):
        ry, rx = r // n_x, lax.rem(r, n_x)
        return lax.rem(my_y + ry, n_y) * n_x + lax.rem(my_x + rx, n_x)

    def back_to(r):
        ry, rx = r // n_x, lax.rem(r, n_x)
        return lax.rem(my_y + n_y - ry, n_y) * n_x + lax.rem(my_x + n_x - rx, n_x)

    def zpos(d):
        return lax.rem(z + d + n_z, n_z)

    def remote(src, dst, s, r, dev):
        return pltpu.make_async_remote_copy(
            src_ref=src, dst_ref=dst, send_sem=s, recv_sem=r, device_id=dev, device_id_type=MESH
        )

    barrier = pltpu.get_barrier_semaphore()
    for r in range(1, n_sp):
        pl.semaphore_signal(barrier, inc=1, device_id=(there(r), tp), device_id_type=MESH)
    greeted = (partner, above, below) + ((two_up, two_dn) if half == 4 else ())
    for dev in greeted:
        pl.semaphore_signal(barrier, inc=1, device_id=dev, device_id_type=MESH)

    t_row = lax.broadcasted_iota(jnp.int32, (toks, toks), 0)
    t_col = lax.broadcasted_iota(jnp.int32, (toks, toks), 1)
    diagonal = t_row == t_col

    def as_row(column):
        return jnp.sum(jnp.where(diagonal, column, 0.0), axis=0, keepdims=True)

    def as_column(row):
        return jnp.sum(jnp.where(diagonal, row, 0.0), axis=1, keepdims=True)

    experts = lax.broadcasted_iota(jnp.int32, (toks, 128), 1)
    id0 = as_column(ids[0:1, :].astype(f32)).astype(jnp.int32)
    id1 = as_column(ids[1:2, :].astype(f32)).astype(jnp.int32)
    hit0, hit1 = experts == id0, experts == id1
    chosen = (jnp.where(hit0, 1.0, 0.0) + jnp.where(hit1, 1.0, 0.0)).astype(bf16)
    earlier = jnp.where(t_col < t_row, 1.0, 0.0).astype(bf16)
    count = dot_nn(earlier, chosen)
    pos0 = jnp.sum(jnp.where(hit0, count, 0.0), axis=1, keepdims=True)
    pos1 = jnp.sum(jnp.where(hit1, count, 0.0), axis=1, keepdims=True)

    def offset_of(expert):
        ey, ex = expert // n_x, lax.rem(expert, n_x)
        return lax.rem(ey + n_y - my_y, n_y) * n_x + lax.rem(ex + n_x - my_x, n_x)

    slot0 = offset_of(id0) * cap + pos0.astype(jnp.int32)
    slot1 = offset_of(id1) * cap + pos1.astype(jnp.int32)
    slots = lax.broadcasted_iota(jnp.int32, (toks, n_rows), 1)
    sel_t[...] = (
        jnp.where(slots == slot0, 1.0, 0.0) + jnp.where(slots == slot1, 1.0, 0.0)
    ).astype(bf16)
    p0, p1 = probs[0:1, :], probs[1:2, :]
    group_row = group[...].reshape(1, toks)
    w0 = group_row * p0 / (p0 + p1)
    w1 = group_row * p1 / (p0 + p1)
    slot0_row, slot1_row = as_row(slot0.astype(f32)), as_row(slot1.astype(f32))
    loaded[0].wait()
    loaded[1].wait()
    both = jnp.concatenate([layer_in[...], out_cot[...]], axis=1)

    def select(p, carry):
        base = pl.multiple_of(p * chunk, chunk)
        here = (lax.broadcasted_iota(jnp.int32, (chunk, toks), 0) + p * chunk).astype(f32)
        m0, m1 = here == slot0_row, here == slot1_row
        pick = (jnp.where(m0, 1.0, 0.0) + jnp.where(m1, 1.0, 0.0)).astype(bf16)
        weight = jnp.sum(jnp.where(m0, w0, 0.0) + jnp.where(m1, w1, 0.0), axis=1, keepdims=True)
        picked = dot_nn(pick, both)
        send[0, pl.ds(base, chunk), :] = picked[:, :cols].astype(bf16)
        send[1, pl.ds(base, chunk), :] = (picked[:, cols:] * weight).astype(bf16)
        return carry

    lax.fori_loop(0, pieces, select, 0)
    pl.semaphore_wait(barrier, n_sp - 1 + len(greeted))

    give_w = [
        remote(w, part_w.at[k], misc_s.at[k], misc_r.at[k], partner)
        for k, w in enumerate((gate, up))
    ]
    loaded[2].wait()
    loaded[3].wait()
    for copy in give_w:
        copy.start()

    def slot_rows(r):
        return pl.ds(pl.multiple_of(r * cap, cap), cap)

    def dispatch(r):
        return remote(
            send.at[:, slot_rows(r), :],
            rows.at[tp, :, slot_rows(r), :],
            a2a_s,
            a2a_r.at[r // per],
            (there(r), tp),
        )

    def start_dispatch(r, carry):
        dispatch(r).start()
        return carry

    lax.fori_loop(1, n_sp, start_dispatch, 0)
    rows[tp, :, slot_rows(0), :] = send[:, slot_rows(0), :]

    last = (half - 1) * pieces

    def ring(n_pieces, where, sems_s, sems_r, sems_ds, sems_dr, own_ready, compute, beside, stop, leap):
        h_p = n_pieces // 2
        total = (half - 1) * n_pieces + h_p

        def along(block, p, d, k, far=False):
            ref = where(block, p)
            return remote(ref, ref, sems_s, sems_r.at[d, k], (two_up, two_dn)[d] if far else (above, below)[d])

        def across(block, p, k):
            ref = where(block, p)
            return remote(ref, ref, sems_ds, sems_dr.at[k], partner)

        def own(p, carry):
            own_ready(p)
            if leap:
                along(tp, p, 0, n_pieces + p, True).start()
                along(tp, p, 1, n_pieces + p, True).start()
            along(tp, p, 0, p).start()
            along(tp, p, 1, p).start()
            across(tp, p, p).start()
            return carry

        lax.fori_loop(0, n_pieces, own, 0)
        beside()

        def own_compute(p, carry):
            across(tp, p, p).wait_recv()
            compute(z, p)
            return carry

        lax.fori_loop(0, n_pieces, own_compute, 0)

        def at(t):
            in_half = t >= (half - 1) * n_pieces
            p_up = lax.rem(t, n_pieces)
            p_dn = jnp.where(in_half, p_up + h_p, p_up)
            hop = t // n_pieces
            return hop, p_up, p_dn

        def move(t):
            hop, p_up, p_dn = at(t)
            b_up, b_dn = zpos(-1 - hop), zpos(1 + hop)
            along(2 * b_up + core, p_up, 0, t).wait_recv()
            pass_up = (hop < half - 2) | ((hop == half - 2) & (p_up < h_p))

            @pl.when((hop == 1) if leap else pass_up)
            def _():
                along(2 * b_up + core, p_up, 0, t + n_pieces).start()

            if leap:
                @pl.when((hop == 1) & (p_up < h_p))
                def _():
                    along(2 * b_up + core, p_up, 0, t + 2 * n_pieces, True).start()

            across(2 * b_up + core, p_up, n_pieces + 2 * t).start()
            along(2 * b_dn + core, p_dn, 1, t).wait_recv()

            @pl.when((hop == 1) if leap else (hop < half - 2))
            def _():
                along(2 * b_dn + core, p_dn, 1, t + n_pieces).start()

            if leap:
                @pl.when((hop == 1) & (p_dn >= h_p))
                def _():
                    along(2 * b_dn + core, p_dn, 1, t + 2 * n_pieces - h_p, True).start()
            else:
                @pl.when((hop == half - 2) & (p_dn >= h_p))
                def _():
                    along(2 * b_dn + core, p_dn, 1, t + n_pieces - h_p).start()

            across(2 * b_dn + core, p_dn, n_pieces + 2 * t + 1).start()

        def turn(u):
            if not leap:
                return u
            return jnp.where(u < n_pieces, u + n_pieces, jnp.where(u < 2 * n_pieces, u - n_pieces, u))

        def step(u, carry):
            move(turn(u))

            @pl.when(u > 0)
            def _():
                use(turn(u - 1))

            return carry

        def use(t):
            hop, p_up, p_dn = at(t)
            b_up, b_dn = zpos(-1 - hop), zpos(1 + hop)
            across(2 * b_up + 1 - core, p_up, n_pieces + 2 * t).wait_recv()
            compute(b_up, p_up)
            across(2 * b_dn + 1 - core, p_dn, n_pieces + 2 * t + 1).wait_recv()
            compute(b_dn, p_dn)

        lax.fori_loop(0, total - stop, step, 0)
        use(total - stop - 1)
        return move, use


    def piece_rows(p):
        return pl.ds(pl.multiple_of(p * chunk, chunk), chunk)

    def rows_ready(p):
        @pl.when((p == 0) & (per > 1))
        def _():
            came = rows.at[tp, :, cap:chunk, :]
            remote(came, came, a2a_s, a2a_r.at[0], partner).wait_recv()

        @pl.when(p > 0)
        def _():
            came = rows.at[tp, :, piece_rows(p), :]
            remote(came, came, a2a_s, a2a_r.at[p], partner).wait_recv()

    def feats(b):
        return pl.ds(pl.multiple_of(b * 2 * cols, 2 * cols), 2 * cols)

    causal = t_col <= t_row

    def to_peers(copy_of):
        def one(r, carry):
            copy_of(r).start()
            return carry

        lax.fori_loop(1, n_sp, one, 0)

    def span_copy(r):
        return remote(span_out, span_in.at[sp], fw_s, fw_r, (there(r), tp))

    def future_copy(r):
        return remote(fut_out, fut_in.at[sp], bw_s.at[r], bw_r.at[sp], (there(r), tp))

    def to_earlier(r, carry):
        @pl.when(there(r) < sp)
        def _():
            future_copy(r).start()

        return carry

    def attend():
        for k in (6, 7, 8, 9, 4, 5):
            loaded[k].wait()
        log_decay = jax.nn.log_sigmoid(logit[...].astype(f32).T) / decay_temp
        upto = jnp.where(causal, 1.0, 0.0).astype(bf16)
        cum = fine(dot_nn, upto, log_decay, 3)
        total = cum[toks - 1 : toks, :]
        cumul[...] = cum
        k = key_in[...].astype(f32).T
        q_dec[...] = query[...].astype(f32).T * DK ** (-0.5) * jnp.exp(cum)
        k_back[...] = k * jnp.exp(-cum)
        k_end[...] = k * jnp.exp(total - cum)
        span_out[0:DK, :] = fine(dot_tn, k_end[...], value[...])
        span_out[DK : 2 * DK, :] = jnp.exp(fine(dot_tn, log_decay, jnp.ones((toks, DV), bf16), 3))
        to_peers(span_copy)
        span_in[sp] = span_out[...]
        found = jnp.where(causal, fine(dot_nt, q_dec[...], k_back[...]), 0.0)
        scores[...] = found
        within[...] = fine(dot_nn, found, value[...])
        pre[...] = jnp.zeros_like(pre)

    def enter():
        came = span_in.at[1:]
        remote(came, came, fw_s, fw_r, partner).wait_recv()

        def pass_on(s, state):
            return jnp.where(s < sp, span_in[s, DK : 2 * DK, :] * state + span_in[s, 0:DK, :], state)

        entry[...] = lax.fori_loop(0, n_sp, pass_on, jnp.zeros((DK, DV), f32))
        mixed_out = within[...] + fine(dot_nn, q_dec[...], entry[...])
        mix_t[...] = mixed_out.T.astype(bf16)


    def expert_in(b, p):
        w_gu = jnp.concatenate([gate[:, feats(b)], up[:, feats(b)]], axis=0)
        at = piece_rows(p)
        x = jnp.concatenate([rows[2 * b, 0, at, :], rows[2 * b + 1, 0, at, :]], axis=1)
        c = jnp.concatenate([rows[2 * b, 1, at, :], rows[2 * b + 1, 1, at, :]], axis=1)
        pre[at, 0:256] += dot_nt(x, w_gu)
        pre[at, 256:384] += dot_nt(c, down[:, feats(b)])

    early = 1 if pieces == 4 else 0
    move, use = ring(
        pieces,
        lambda block, p: rows.at[block, :, piece_rows(p), :],
        ag_s,
        ag_r,
        agd_s,
        agd_r,
        rows_ready,
        expert_in,
        attend,
        early,
        False,
    )

    h_p = pieces // 2

    def give_gu(p):
        at = piece_rows(p)
        return remote(gu.at[at, :], gu_part.at[at, :], gu_s, gu_r.at[p], partner)

    def middle(i, carry):
        p = i // 2 + lax.rem(i, 2) * h_p
        at = piece_rows(p)
        gate_pre, up_pre, hidden_cot = pre[at, 0:128], pre[at, 128:256], pre[at, 256:384]
        sig = jax.nn.sigmoid(gate_pre)
        active = gate_pre * sig
        gu[at, 0:128] = (hidden_cot * up_pre * sig * (1.0 + gate_pre * (1.0 - sig))).astype(bf16)
        gu[at, 128:256] = (hidden_cot * active).astype(bf16)
        give_gu(p).start()
        pre[at, 0:128] = active * up_pre
        return carry

    rs_total = h_p + (half - 1) * pieces

    def partial(b, p):
        cols_at = pl.ds(pl.multiple_of((2 * b + core) * cols, cols), cols)
        mine = jnp.concatenate([gate[:, cols_at], up[:, cols_at]], axis=0)
        theirs = jnp.concatenate([part_w[0, :, cols_at], part_w[1, :, cols_at]], axis=0)
        at = piece_rows(p)
        return dot_nn(gu[at, :], mine) + dot_nn(gu_part[at, :], theirs)

    def hop_sum(d, k):
        return remote(
            stage.at[d, k],
            inbox.at[d, k],
            rs_s,
            rs_r.at[d, k],
            above if d == 0 else below,
        )

    def first(t, carry):
        for d in range(2):
            give_gu(t + d * h_p).wait_recv()
            stage[d, t] = partial(zpos(half), t + d * h_p).astype(bf16)
            hop_sum(d, t).start()
        return carry

    if early:
        lax.fori_loop(0, 2, middle, 0)
        for copy in give_w:
            copy.wait_recv()
        move(rs_total - 1)
        first(0, 0)
        use(rs_total - 1)
        lax.fori_loop(2, pieces, middle, 0)
        lax.fori_loop(1, h_p, first, 0)
    else:
        lax.fori_loop(0, pieces, middle, 0)
        for copy in give_w:
            copy.wait_recv()
        lax.fori_loop(0, h_p, first, 0)
    gu_t[...] = gu[...].T
    hid_t[...] = pre[:, 0:128].astype(bf16).T
    enter()

    def gradients(b):
        x = jnp.concatenate([rows[2 * b, 0], rows[2 * b + 1, 0]], axis=1)
        c = jnp.concatenate([rows[2 * b, 1], rows[2 * b + 1, 1]], axis=1)
        both_g = dot_nn(gu_t[...], x)
        gate_g[:, feats(b)] = both_g[0:128]
        up_g[:, feats(b)] = both_g[128:256]
        down_g[:, feats(b)] = dot_nn(hid_t[...], c)

    def later(u, carry):
        t = u + h_p
        hop, p = 1 + u // pieces, lax.rem(u, pieces)
        for d in range(2):
            dest = zpos(half - hop) if d == 0 else zpos(hop - half)
            value = partial(dest, p)
            mine_first = (p >= h_p) if d == 0 else (p < h_p)
            alone = (hop == 1) & mine_first
            k_in = jnp.where(hop == 1, p - d * h_p, t - pieces)

            @pl.when(alone)
            def _():
                stage[d, t] = value.astype(bf16)

            @pl.when(jnp.logical_not(alone))
            def _():
                hop_sum(d, k_in).wait_recv()
                stage[d, t] = (value + inbox[d, k_in].astype(f32)).astype(bf16)

            hop_sum(d, t).start()

        @pl.when(u < n_z)
        def _():
            gradients(u)

        return carry

    lax.fori_loop(0, rs_total - h_p, later, 0)

    def give_back(r):
        return remote(
            ret_out.at[slot_rows(r), :],
            ret.at[slot_rows(r), :],
            back_s,
            back_r,
            (back_to(r), tp),
        )

    def finish(p, carry):
        k_in = rs_total - pieces + p
        value = partial(z, p)
        for d in range(2):
            hop_sum(d, k_in).wait_recv()
            value = value + inbox[d, k_in].astype(f32)
        ret_out[piece_rows(p), :] = value.astype(bf16)
        for i in range(per):
            r = p * per + i

            @pl.when(r > 0)
            def _():
                give_back(r).start()

        return carry

    lax.fori_loop(0, pieces, finish, 0)
    for g in range(rs_total - h_p, n_z):
        gradients(g)
    for k in range(3):
        stored[k].start()
    ret[slot_rows(0), :] = ret_out[slot_rows(0), :]

    others = ret.at[cap:, :]
    remote(others, others, back_s, back_r, partner).wait_recv()
    mixed = (out_cot[...].astype(f32) + dot_nn(sel_t[...], ret[...])).astype(bf16)
    full_cot[tp] = mixed

    tok_pieces = 4 if pieces == 4 else 2
    tok_rows = toks // tok_pieces
    mixer_cot[...] = jnp.zeros_like(mixer_cot)

    wide = 2 * n_z // n_sp

    def proj_copy(j):
        return remote(
            pj_out.at[j],
            pj_in.at[sp, lax.rem(j, wide)],
            pj_s,
            pj_r,
            (j // wide, tp),
        )

    def proj_send(j):
        @pl.when(j // wide != sp)
        def _():
            proj_copy(j).start()

    def project(b, p):
        @pl.when(p == tok_pieces - 1)
        def _():
            whole = jnp.concatenate([full_cot[2 * b], full_cot[2 * b + 1]], axis=1)
            mixer_cot[...] += dot_nn(whole, out_w[feats(b), :])
            found = dot_nn(mix_t[...], whole).astype(bf16)
            for i in range(2):
                j = 2 * b + i
                pj_out[j] = found[:, i * cols : (i + 1) * cols]

                @pl.when(j // wide == sp)
                def _():
                    pj_in[sp, lax.rem(j, wide)] = pj_out[j]

                away = lax.rem(b - z + n_z, n_z)

                @pl.when(away != half)
                def _():
                    proj_send(j)

    ring(
        tok_pieces,
        lambda block, p: full_cot.at[block, pl.ds(pl.multiple_of(p * tok_rows, tok_rows), tok_rows), :],
        tk_s,
        tk_r,
        tkd_s,
        tkd_r,
        lambda p: None,
        project,
        lambda: None,
        0,
        half == 4,
    )

    cot = mixer_cot[...]
    fut = fine(dot_tn, q_dec[...], cot)
    fut_out[...] = fut.astype(bf16)
    lax.fori_loop(1, n_sp, to_earlier, 0)
    for i in range(2):
        proj_send(2 * zpos(half) + i)
    cot_values = jnp.where(causal, fine(dot_nt, cot, value[...]), 0.0)
    cum = cumul[...]
    q_grad = jnp.exp(cum) * (fine(dot_nt, cot, entry[...]) + fine(dot_nn, cot_values, k_back[...]))
    query_g[...] = (q_grad * DK ** (-0.5)).T
    key_part = jnp.exp(-cum) * fine(dot_tn, cot_values, q_dec[...])
    value_g[...] = fine(dot_tn, scores[...], cot)

    def fut_arrived(s, carry):
        @pl.when(s > sp)
        def _():
            remote(fut_out, fut_in.at[s], bw_s.at[0], bw_r.at[s], partner).wait_recv()

        return carry

    lax.fori_loop(0, n_sp, fut_arrived, 0)

    def pass_back(i, state):
        s = n_sp - 1 - i
        later_on = span_in[s, DK : 2 * DK, :] * state + fut_in[s].astype(f32)
        return jnp.where(s > sp, later_on, state)

    future = lax.fori_loop(0, n_sp, pass_back, jnp.zeros((DK, DV), f32))
    k_grad = key_part + jnp.exp(cum[toks - 1 : toks, :] - cum) * fine(dot_nt, value[...], future)
    k_grad_t = k_grad.T
    key_g[...] = k_grad_t
    value_g[...] += fine(dot_nn, k_end[...], future)
    span_end = span_out[DK : 2 * DK, :] * entry[...] + span_out[0:DK, :]
    beyond = jnp.sum(future * span_end, axis=1, keepdims=True)
    terms = query[...].astype(f32) * query_g[...] - key_in[...].astype(f32) * k_grad_t
    since = jnp.where(t_row >= t_col, 1.0, 0.0).astype(bf16)
    tail = fine(dot_nn, terms, since, 3) + beyond
    logit_g[...] = tail * jax.nn.sigmoid(-logit[...].astype(f32)) / decay_temp

    came = pj_in.at[1:]
    remote(came, came, pj_s, pj_r, partner).wait_recv()
    for i in range(wide):
        sums = jnp.zeros((128, cols), f32)
        for s in range(n_sp):
            sums = sums + pj_in[s, i].astype(f32)
        proj_g[i * cols : (i + 1) * cols, :] = sums.T

    for k in range(3, 8):
        stored[k].start()

    for copy in give_w:
        copy.wait_send()

    def fut_sent(r, carry):
        @pl.when(there(r) < sp)
        def _():
            future_copy(r).wait_send()

        return carry

    lax.fori_loop(1, n_sp, fut_sent, 0)
    for sent, sem in (
        (send.at[:, cap:, :], a2a_s),
        (ret.at[cap:, :], back_s),
        (span_in.at[1:], fw_s),
        (pj_in.at[1:], pj_s),
        (rows.at[: n_z - 1], ag_s),
        (rows.at[:n_z], agd_s),
        (full_cot.at[: n_z - 1], tk_s),
        (full_cot.at[:n_z], tkd_s),
        (stage, rs_s),
        (gu, gu_s),
    ):
        remote(sent, sent, sem, back_r, partner).wait_send()
    for copy in stored:
        copy.wait()


def store_kernel(*refs):
    taken = [
        pltpu.make_async_copy(source, target, refs[24].at[k])
        for k, (source, target) in enumerate(zip(refs[:8], refs[16:24]))
    ]
    stored = [
        pltpu.make_async_copy(source, target, refs[25].at[k])
        for k, (source, target) in enumerate(zip(refs[16:24], refs[8:16]))
    ]
    for copy in taken:
        copy.start()
    for first, second in zip(taken, stored):
        first.wait()
        second.start()
    for copy in stored:
        copy.wait()


def local(
    layer_in,
    out_cot,
    route_ids,
    route_probs,
    group_prob,
    gate_weight,
    up_weight,
    down_weight,
    out_weight,
    query,
    key_in,
    value,
    decay_logit,
):
    toks, cols = layer_in.shape
    n_sp, n_tp = lax.axis_size("sp"), lax.axis_size("tp")
    n_x = 4 if n_sp == 16 else n_sp
    n_z = n_tp // 2
    half = n_z // 2
    pieces = 4 if n_sp % 4 == 0 else 2
    width = gate_weight.shape[2]
    n_rows = 4 * toks
    total = (half - 1) * pieces + pieces // 2
    tk_pieces = 4 if pieces == 4 else 2
    tk_total = (half - 1) * tk_pieces + tk_pieces // 2
    chunk = n_rows // pieces
    wide = n_tp // n_sp
    dma = pltpu.SemaphoreType.DMA
    vmem = pl.BlockSpec(memory_space=pltpu.VMEM)
    hbm = pl.BlockSpec(memory_space=pltpu.HBM)
    small = (DK, toks)
    shapes = ((128, width),) * 3 + ((wide * cols, DV), small, small, (toks, DV), small)
    grads = pl.pallas_call(
        functools.partial(moe_kernel, (n_sp, n_x, n_z, pieces)),
        out_shape=tuple(jax.ShapeDtypeStruct(shape, f32) for shape in shapes),
        in_specs=[vmem] * 3 + [hbm] * 10,
        out_specs=[hbm] * 8,
        scratch_shapes=[
            pltpu.VMEM((toks, cols), bf16),
            pltpu.VMEM((toks, cols), bf16),
            pltpu.VMEM((128, width), bf16),
            pltpu.VMEM((128, width), bf16),
            pltpu.VMEM((128, width), bf16),
            pltpu.VMEM((width, DV), bf16),
            pltpu.VMEM((DK, toks), bf16),
            pltpu.VMEM((DK, toks), bf16),
            pltpu.VMEM((toks, DV), bf16),
            pltpu.VMEM((DK, toks), bf16),
            *(pltpu.VMEM(shape, f32) for shape in shapes),
            pltpu.VMEM((n_tp, toks, cols), bf16),
            pltpu.VMEM((toks, DV), f32),
            pltpu.VMEM((toks, DK), f32),
            pltpu.VMEM((toks, DK), f32),
            pltpu.VMEM((toks, DK), f32),
            pltpu.VMEM((toks, DK), f32),
            pltpu.VMEM((toks, toks), f32),
            pltpu.VMEM((toks, DV), f32),
            pltpu.VMEM((DV, toks), bf16),
            pltpu.VMEM((2 * DK, DV), f32),
            pltpu.VMEM((n_sp, 2 * DK, DV), f32),
            pltpu.VMEM((DK, DV), f32),
            pltpu.VMEM((DK, DV), bf16),
            pltpu.VMEM((n_sp, DK, DV), bf16),
            pltpu.VMEM((n_tp, DV, cols), bf16),
            pltpu.VMEM((n_sp, wide, DV, cols), bf16),
            pltpu.VMEM((2, n_rows, cols), bf16),
            pltpu.VMEM((toks, n_rows), bf16),
            pltpu.VMEM((n_tp, 2, n_rows, cols), bf16),
            pltpu.VMEM((n_rows, 384), f32),
            pltpu.VMEM((2, 128, width), bf16),
            pltpu.VMEM((n_rows, 256), bf16),
            pltpu.VMEM((n_rows, 256), bf16),
            pltpu.VMEM((256, n_rows), bf16),
            pltpu.VMEM((128, n_rows), bf16),
            pltpu.VMEM((2, total, chunk, cols), bf16),
            pltpu.VMEM((2, total, chunk, cols), bf16),
            pltpu.VMEM((n_rows, cols), bf16),
            pltpu.VMEM((n_rows, cols), bf16),
            dma(()),
            dma((pieces,)),
            dma(()),
            dma(()),
            dma(()),
            dma((2, total)),
            dma(()),
            dma((pieces + 2 * total,)),
            dma(()),
            dma((2, total)),
            dma(()),
            dma((2, tk_total)),
            dma(()),
            dma((tk_pieces + 2 * tk_total,)),
            dma((2,)),
            dma((2,)),
            dma(()),
            dma((pieces,)),
            dma(()),
            dma(()),
            dma((n_sp,)),
            dma((n_sp,)),
            dma(()),
            dma(()),
            dma((10,)),
            dma((8,)),
        ],
        compiler_params=pltpu.CompilerParams(
            collective_id=0, has_side_effects=True, vmem_limit_bytes=60 * 1024 * 1024
        ),
    )(
        route_ids.T,
        route_probs.T,
        group_prob,
        layer_in,
        out_cot,
        gate_weight[0],
        up_weight[0],
        down_weight[0],
        out_weight,
        query.T,
        key_in.T,
        value,
        decay_logit.T,
    )
    gate_g, up_g, down_g, proj_g, query_g, key_g, value_g, logit_g = pl.pallas_call(
        store_kernel,
        out_shape=tuple(jax.ShapeDtypeStruct(g.shape, g.dtype) for g in grads),
        in_specs=[hbm] * 8,
        out_specs=[hbm] * 8,
        scratch_shapes=[*(pltpu.VMEM(g.shape, g.dtype) for g in grads), dma((8,)), dma((8,))],
        compiler_params=pltpu.CompilerParams(vmem_limit_bytes=60 * 1024 * 1024),
    )(*grads)
    return (
        gate_g[None],
        up_g[None],
        down_g[None],
        proj_g,
        query_g.T,
        key_g.T,
        value_g,
        logit_g.T,
    )


def solution(mesh):
    in_specs = (
        P("sp", "tp"),
        P("sp", "tp"),
        P("sp", None),
        P("sp", None),
        P("sp"),
        P("sp", "tp", None),
        P("sp", "tp", None),
        P("sp", "tp", None),
        P(None, "tp"),
        P("sp", "tp"),
        P("sp", "tp"),
        P("sp", "tp"),
        P("sp", "tp"),
    )
    out_specs = (
        P("sp", "tp", None),
        P("sp", "tp", None),
        P("sp", "tp", None),
        P("sp", "tp"),
        P("sp", "tp"),
        P("sp", "tp"),
        P("sp", "tp"),
        P("sp", "tp"),
    )
    return jax.shard_map(local, mesh=mesh, in_specs=in_specs, out_specs=out_specs, check_vma=False)
```

```python
import functools

import jax
import jax.numpy as jnp
from jax import lax
from jax.experimental import pallas as pl
from jax.experimental.pallas import tpu as pltpu
from jax.sharding import PartitionSpec as P

DK = 64
DV = 128


decay_temp = 16.0
f32, bf16 = jnp.float32, jnp.bfloat16
MESH = pl.DeviceIdType.MESH


def dot_nt(a, b):
    return lax.dot_general(a, b, (((1,), (1,)), ((), ())), preferred_element_type=f32)


def dot_nn(a, b):
    return lax.dot_general(a, b, (((1,), (0,)), ((), ())), preferred_element_type=f32)


def dot_tn(a, b):
    return lax.dot_general(a, b, (((0,), (0,)), ((), ())), preferred_element_type=f32)


def parts_of(x, n):
    if x.dtype == bf16:
        return [x]
    found = []
    for _ in range(n):
        top = x.astype(bf16)
        found.append(top)
        x = x - top.astype(f32)
    return found


def fine(dot, a, b, n=2):
    a, b = parts_of(a, n), parts_of(b, n)
    terms = [dot(p, q) for i, p in enumerate(a) for j, q in enumerate(b) if i + j < n]
    total = terms[-1]
    for term in terms[-2::-1]:
        total = total + term
    return total


def moe_kernel(
    sizes,
    ids,
    probs,
    group,
    *refs,
):
    held, given, kept = refs[:10], refs[10:18], refs[18:]
    expert_kernel(sizes, ids, probs, group, held, given, *kept)


def expert_kernel(
    sizes,
    ids,
    probs,
    group,
    held,
    given,
    layer_in,
    out_cot,
    gate,
    up,
    down,
    out_w,
    query,
    key_in,
    value,
    logit,
    gate_g,
    up_g,
    down_g,
    proj_g,
    query_g,
    key_g,
    value_g,
    logit_g,
    full_cot,
    mixer_cot,
    q_dec,
    k_back,
    k_end,
    cumul,
    scores,
    within,
    mix_t,
    span_out,
    span_in,
    entry,
    fut_out,
    fut_in,
    pj_out,
    pj_in,
    send,
    sel_t,
    rows,
    pre,
    part_w,
    gu,
    gu_part,
    gu_t,
    hid_t,
    stage,
    inbox,
    ret_out,
    ret,
    a2a_s,
    a2a_r,
    back_s,
    back_r,
    ag_s,
    ag_r,
    agd_s,
    agd_r,
    rs_s,
    rs_r,
    tk_s,
    tk_r,
    tkd_s,
    tkd_r,
    misc_s,
    misc_r,
    gu_s,
    gu_r,
    fw_s,
    fw_r,
    bw_s,
    bw_r,
    pj_s,
    pj_r,
    load_s,
    give_s,
):
    n_sp, n_x, n_z, pieces = sizes
    n_y = n_sp // n_x
    half = n_z // 2
    targets = (layer_in, out_cot, gate, up, down, out_w, query, key_in, value, logit)
    loaded = [
        pltpu.make_async_copy(source, target, load_s.at[k])
        for k, (source, target) in enumerate(zip(held, targets))
    ]
    for k in (0, 1, 2, 3, 6, 7, 8, 9, 4, 5):
        loaded[k].start()
    results = (gate_g, up_g, down_g, proj_g, query_g, key_g, value_g, logit_g)
    stored = [
        pltpu.make_async_copy(source, target, give_s.at[k])
        for k, (source, target) in enumerate(zip(results, given))
    ]
    toks, cols = layer_in.shape
    cap = 4 * toks // n_sp
    n_rows = n_sp * cap
    per = n_sp // pieces
    chunk = n_rows // pieces
    sp = lax.axis_index("sp")
    tp = lax.axis_index("tp")
    core = lax.rem(tp, 2)
    z = tp // 2
    z_up = lax.rem(z + 1, n_z)
    z_dn = lax.rem(z + n_z - 1, n_z)
    partner = (sp, 2 * z + 1 - core)
    above, below = (sp, 2 * z_up + core), (sp, 2 * z_dn + core)
    two_up = (sp, 2 * lax.rem(z + 2, n_z) + core)
    two_dn = (sp, 2 * lax.rem(z + n_z - 2, n_z) + core)
    my_y, my_x = sp // n_x, lax.rem(sp, n_x)

    def there(r):
        ry, rx = r // n_x, lax.rem(r, n_x)
        return lax.rem(my_y + ry, n_y) * n_x + lax.rem(my_x + rx, n_x)

    def back_to(r):
        ry, rx = r // n_x, lax.rem(r, n_x)
        return lax.rem(my_y + n_y - ry, n_y) * n_x + lax.rem(my_x + n_x - rx, n_x)

    def zpos(d):
        return lax.rem(z + d + n_z, n_z)

    def remote(src, dst, s, r, dev):
        return pltpu.make_async_remote_copy(
            src_ref=src, dst_ref=dst, send_sem=s, recv_sem=r, device_id=dev, device_id_type=MESH
        )

    barrier = pltpu.get_barrier_semaphore()
    for r in range(1, n_sp):
        pl.semaphore_signal(barrier, inc=1, device_id=(there(r), tp), device_id_type=MESH)
    greeted = (partner, above, below) + ((two_up, two_dn) if half == 4 else ())
    for dev in greeted:
        pl.semaphore_signal(barrier, inc=1, device_id=dev, device_id_type=MESH)

    t_row = lax.broadcasted_iota(jnp.int32, (toks, toks), 0)
    t_col = lax.broadcasted_iota(jnp.int32, (toks, toks), 1)
    diagonal = t_row == t_col

    def as_row(column):
        return jnp.sum(jnp.where(diagonal, column, 0.0), axis=0, keepdims=True)

    def as_column(row):
        return jnp.sum(jnp.where(diagonal, row, 0.0), axis=1, keepdims=True)

    experts = lax.broadcasted_iota(jnp.int32, (toks, 128), 1)
    id0 = as_column(ids[0:1, :].astype(f32)).astype(jnp.int32)
    id1 = as_column(ids[1:2, :].astype(f32)).astype(jnp.int32)
    hit0, hit1 = experts == id0, experts == id1
    chosen = (jnp.where(hit0, 1.0, 0.0) + jnp.where(hit1, 1.0, 0.0)).astype(bf16)
    earlier = jnp.where(t_col < t_row, 1.0, 0.0).astype(bf16)
    count = dot_nn(earlier, chosen)
    pos0 = jnp.sum(jnp.where(hit0, count, 0.0), axis=1, keepdims=True)
    pos1 = jnp.sum(jnp.where(hit1, count, 0.0), axis=1, keepdims=True)

    def offset_of(expert):
        ey, ex = expert // n_x, lax.rem(expert, n_x)
        return lax.rem(ey + n_y - my_y, n_y) * n_x + lax.rem(ex + n_x - my_x, n_x)

    slot0 = offset_of(id0) * cap + pos0.astype(jnp.int32)
    slot1 = offset_of(id1) * cap + pos1.astype(jnp.int32)
    p0, p1 = probs[0:1, :], probs[1:2, :]
    group_row = group[...].reshape(1, toks)
    w0 = group_row * p0 / (p0 + p1)
    w1 = group_row * p1 / (p0 + p1)
    slot0_row, slot1_row = as_row(slot0.astype(f32)), as_row(slot1.astype(f32))
    loaded[0].wait()
    loaded[1].wait()
    both = jnp.concatenate([layer_in[...], out_cot[...]], axis=1)

    def select(p, carry):
        base = pl.multiple_of(p * chunk, chunk)
        here = (lax.broadcasted_iota(jnp.int32, (chunk, toks), 0) + p * chunk).astype(f32)
        m0, m1 = here == slot0_row, here == slot1_row
        pick = (jnp.where(m0, 1.0, 0.0) + jnp.where(m1, 1.0, 0.0)).astype(bf16)
        weight = jnp.sum(jnp.where(m0, w0, 0.0) + jnp.where(m1, w1, 0.0), axis=1, keepdims=True)
        picked = dot_nn(pick, both)
        send[0, pl.ds(base, chunk), :] = picked[:, :cols].astype(bf16)
        send[1, pl.ds(base, chunk), :] = (picked[:, cols:] * weight).astype(bf16)
        return carry

    select(0, 0)
    pl.semaphore_wait(barrier, n_sp - 1 + len(greeted))

    def slot_rows(r):
        return pl.ds(pl.multiple_of(r * cap, cap), cap)

    def dispatch(r):
        return remote(
            send.at[:, slot_rows(r), :],
            rows.at[tp, :, slot_rows(r), :],
            a2a_s,
            a2a_r.at[r // per],
            (there(r), tp),
        )

    def start_dispatch(p):
        for i in range(per):
            r = p * per + i

            @pl.when(r > 0)
            def _():
                dispatch(r).start()

    start_dispatch(0)

    def select_next(p, carry):
        select(p, 0)
        start_dispatch(p)
        return carry

    lax.fori_loop(1, pieces, select_next, 0)
    rows[tp, :, slot_rows(0), :] = send[:, slot_rows(0), :]

    give_w = [
        remote(w, part_w.at[k], misc_s.at[k], misc_r.at[k], partner)
        for k, w in enumerate((gate, up))
    ]
    loaded[2].wait()
    loaded[3].wait()
    for copy in give_w:
        copy.start()

    last = (half - 1) * pieces

    def ring(n_pieces, where, sems_s, sems_r, sems_ds, sems_dr, own_ready, compute, beside, stop, leap):
        h_p = n_pieces // 2
        total = (half - 1) * n_pieces + h_p

        def along(block, p, d, k, far=False):
            ref = where(block, p)
            return remote(ref, ref, sems_s, sems_r.at[d, k], (two_up, two_dn)[d] if far else (above, below)[d])

        def across(block, p, k):
            ref = where(block, p)
            return remote(ref, ref, sems_ds, sems_dr.at[k], partner)

        def own(p, carry):
            own_ready(p)
            if leap:
                along(tp, p, 0, n_pieces + p, True).start()
                along(tp, p, 1, n_pieces + p, True).start()
            along(tp, p, 0, p).start()
            along(tp, p, 1, p).start()
            across(tp, p, p).start()
            return carry

        lax.fori_loop(0, n_pieces, own, 0)
        beside()

        def own_compute(p, carry):
            across(tp, p, p).wait_recv()
            compute(z, p)
            return carry

        lax.fori_loop(0, n_pieces, own_compute, 0)

        def at(t):
            in_half = t >= (half - 1) * n_pieces
            p_up = lax.rem(t, n_pieces)
            p_dn = jnp.where(in_half, p_up + h_p, p_up)
            hop = t // n_pieces
            return hop, p_up, p_dn

        def move(t):
            hop, p_up, p_dn = at(t)
            b_up, b_dn = zpos(-1 - hop), zpos(1 + hop)
            along(2 * b_up + core, p_up, 0, t).wait_recv()
            pass_up = (hop < half - 2) | ((hop == half - 2) & (p_up < h_p))

            @pl.when((hop == 1) if leap else pass_up)
            def _():
                along(2 * b_up + core, p_up, 0, t + n_pieces).start()

            if leap:
                @pl.when((hop == 1) & (p_up < h_p))
                def _():
                    along(2 * b_up + core, p_up, 0, t + 2 * n_pieces, True).start()

            across(2 * b_up + core, p_up, n_pieces + 2 * t).start()
            along(2 * b_dn + core, p_dn, 1, t).wait_recv()

            @pl.when((hop == 1) if leap else (hop < half - 2))
            def _():
                along(2 * b_dn + core, p_dn, 1, t + n_pieces).start()

            if leap:
                @pl.when((hop == 1) & (p_dn >= h_p))
                def _():
                    along(2 * b_dn + core, p_dn, 1, t + 2 * n_pieces - h_p, True).start()
            else:
                @pl.when((hop == half - 2) & (p_dn >= h_p))
                def _():
                    along(2 * b_dn + core, p_dn, 1, t + n_pieces - h_p).start()

            across(2 * b_dn + core, p_dn, n_pieces + 2 * t + 1).start()

        def turn(u):
            if not leap:
                return u
            return jnp.where(u < n_pieces, u + n_pieces, jnp.where(u < 2 * n_pieces, u - n_pieces, u))

        def step(u, carry):
            move(turn(u))

            @pl.when(u > 0)
            def _():
                use(turn(u - 1))

            return carry

        def use(t):
            hop, p_up, p_dn = at(t)
            b_up, b_dn = zpos(-1 - hop), zpos(1 + hop)
            across(2 * b_up + 1 - core, p_up, n_pieces + 2 * t).wait_recv()
            compute(b_up, p_up)
            across(2 * b_dn + 1 - core, p_dn, n_pieces + 2 * t + 1).wait_recv()
            compute(b_dn, p_dn)

        lax.fori_loop(0, total - stop, step, 0)
        use(total - stop - 1)
        return move, use


    def piece_rows(p):
        return pl.ds(pl.multiple_of(p * chunk, chunk), chunk)

    def rows_ready(p):
        @pl.when((p == 0) & (per > 1))
        def _():
            came = rows.at[tp, :, cap:chunk, :]
            remote(came, came, a2a_s, a2a_r.at[0], partner).wait_recv()

        @pl.when(p > 0)
        def _():
            came = rows.at[tp, :, piece_rows(p), :]
            remote(came, came, a2a_s, a2a_r.at[p], partner).wait_recv()

    def feats(b):
        return pl.ds(pl.multiple_of(b * 2 * cols, 2 * cols), 2 * cols)

    causal = t_col <= t_row

    def to_peers(copy_of):
        def one(r, carry):
            copy_of(r).start()
            return carry

        lax.fori_loop(1, n_sp, one, 0)

    def span_copy(r):
        return remote(span_out, span_in.at[sp], fw_s, fw_r, (there(r), tp))

    def future_copy(r):
        return remote(fut_out, fut_in.at[sp], bw_s.at[r], bw_r.at[sp], (there(r), tp))

    def to_earlier(r, carry):
        @pl.when(there(r) < sp)
        def _():
            future_copy(r).start()

        return carry

    def attend():
        slots = lax.broadcasted_iota(jnp.int32, (toks, n_rows), 1)
        sel_t[...] = (
            jnp.where(slots == slot0, 1.0, 0.0) + jnp.where(slots == slot1, 1.0, 0.0)
        ).astype(bf16)
        for k in (6, 7, 8, 9, 4, 5):
            loaded[k].wait()
        log_decay = jax.nn.log_sigmoid(logit[...].astype(f32).T) / decay_temp
        upto = jnp.where(causal, 1.0, 0.0).astype(bf16)
        cum = fine(dot_nn, upto, log_decay, 3)
        total = cum[toks - 1 : toks, :]
        cumul[...] = cum
        k = key_in[...].astype(f32).T
        q_dec[...] = query[...].astype(f32).T * DK ** (-0.5) * jnp.exp(cum)
        k_back[...] = k * jnp.exp(-cum)
        k_end[...] = k * jnp.exp(total - cum)
        span_out[0:DK, :] = fine(dot_tn, k_end[...], value[...])
        span_out[DK : 2 * DK, :] = jnp.exp(fine(dot_tn, log_decay, jnp.ones((toks, DV), bf16), 3))
        to_peers(span_copy)
        span_in[sp] = span_out[...]
        found = jnp.where(causal, fine(dot_nt, q_dec[...], k_back[...]), 0.0)
        scores[...] = found
        within[...] = fine(dot_nn, found, value[...])
        pre[...] = jnp.zeros_like(pre)

    def enter():
        came = span_in.at[1:]
        remote(came, came, fw_s, fw_r, partner).wait_recv()

        def pass_on(s, state):
            return jnp.where(s < sp, span_in[s, DK : 2 * DK, :] * state + span_in[s, 0:DK, :], state)

        entry[...] = lax.fori_loop(0, n_sp, pass_on, jnp.zeros((DK, DV), f32))
        mixed_out = within[...] + fine(dot_nn, q_dec[...], entry[...])
        mix_t[...] = mixed_out.T.astype(bf16)


    def expert_in(b, p):
        w_gu = jnp.concatenate([gate[:, feats(b)], up[:, feats(b)]], axis=0)
        at = piece_rows(p)
        x = jnp.concatenate([rows[2 * b, 0, at, :], rows[2 * b + 1, 0, at, :]], axis=1)
        c = jnp.concatenate([rows[2 * b, 1, at, :], rows[2 * b + 1, 1, at, :]], axis=1)
        pre[at, 0:256] += dot_nt(x, w_gu)
        pre[at, 256:384] += dot_nt(c, down[:, feats(b)])

    early = 1 if pieces == 4 else 0
    move, use = ring(
        pieces,
        lambda block, p: rows.at[block, :, piece_rows(p), :],
        ag_s,
        ag_r,
        agd_s,
        agd_r,
        rows_ready,
        expert_in,
        attend,
        early,
        False,
    )

    h_p = pieces // 2

    def give_gu(p):
        at = piece_rows(p)
        return remote(gu.at[at, :], gu_part.at[at, :], gu_s, gu_r.at[p], partner)

    def middle(i, carry):
        p = i // 2 + lax.rem(i, 2) * h_p
        at = piece_rows(p)
        gate_pre, up_pre, hidden_cot = pre[at, 0:128], pre[at, 128:256], pre[at, 256:384]
        sig = jax.nn.sigmoid(gate_pre)
        active = gate_pre * sig
        gu[at, 0:128] = (hidden_cot * up_pre * sig * (1.0 + gate_pre * (1.0 - sig))).astype(bf16)
        gu[at, 128:256] = (hidden_cot * active).astype(bf16)
        give_gu(p).start()
        pre[at, 0:128] = active * up_pre
        return carry

    rs_total = h_p + (half - 1) * pieces

    def partial(b, p):
        cols_at = pl.ds(pl.multiple_of((2 * b + core) * cols, cols), cols)
        mine = jnp.concatenate([gate[:, cols_at], up[:, cols_at]], axis=0)
        theirs = jnp.concatenate([part_w[0, :, cols_at], part_w[1, :, cols_at]], axis=0)
        at = piece_rows(p)
        return dot_nn(gu[at, :], mine) + dot_nn(gu_part[at, :], theirs)

    def hop_sum(d, k):
        return remote(
            stage.at[d, k],
            inbox.at[d, k],
            rs_s,
            rs_r.at[d, k],
            above if d == 0 else below,
        )

    def first(t, carry):
        for d in range(2):
            give_gu(t + d * h_p).wait_recv()
            stage[d, t] = partial(zpos(half), t + d * h_p).astype(bf16)
            hop_sum(d, t).start()
        return carry

    if early:
        lax.fori_loop(0, 2, middle, 0)
        for copy in give_w:
            copy.wait_recv()
        move(rs_total - 1)
        first(0, 0)
        use(rs_total - 1)
        lax.fori_loop(2, pieces, middle, 0)
        lax.fori_loop(1, h_p, first, 0)
    else:
        lax.fori_loop(0, pieces, middle, 0)
        for copy in give_w:
            copy.wait_recv()
        lax.fori_loop(0, h_p, first, 0)
    gu_t[...] = gu[...].T
    hid_t[...] = pre[:, 0:128].astype(bf16).T
    enter()

    def gradients(b):
        x = jnp.concatenate([rows[2 * b, 0], rows[2 * b + 1, 0]], axis=1)
        c = jnp.concatenate([rows[2 * b, 1], rows[2 * b + 1, 1]], axis=1)
        both_g = dot_nn(gu_t[...], x)
        gate_g[:, feats(b)] = both_g[0:128]
        up_g[:, feats(b)] = both_g[128:256]
        down_g[:, feats(b)] = dot_nn(hid_t[...], c)

    def later(u, carry):
        t = u + h_p
        hop, p = 1 + u // pieces, lax.rem(u, pieces)
        for d in range(2):
            dest = zpos(half - hop) if d == 0 else zpos(hop - half)
            value = partial(dest, p)
            mine_first = (p >= h_p) if d == 0 else (p < h_p)
            alone = (hop == 1) & mine_first
            k_in = jnp.where(hop == 1, p - d * h_p, t - pieces)

            @pl.when(alone)
            def _():
                stage[d, t] = value.astype(bf16)

            @pl.when(jnp.logical_not(alone))
            def _():
                hop_sum(d, k_in).wait_recv()
                stage[d, t] = (value + inbox[d, k_in].astype(f32)).astype(bf16)

            hop_sum(d, t).start()

        @pl.when(u < n_z)
        def _():
            gradients(u)

        return carry

    lax.fori_loop(0, rs_total - h_p, later, 0)

    def give_back(r):
        return remote(
            ret_out.at[slot_rows(r), :],
            ret.at[slot_rows(r), :],
            back_s,
            back_r,
            (back_to(r), tp),
        )

    def finish(p, carry):
        k_in = rs_total - pieces + p
        value = partial(z, p)
        for d in range(2):
            hop_sum(d, k_in).wait_recv()
            value = value + inbox[d, k_in].astype(f32)
        ret_out[piece_rows(p), :] = value.astype(bf16)
        for i in range(per):
            r = p * per + i

            @pl.when(r > 0)
            def _():
                give_back(r).start()

        return carry

    lax.fori_loop(0, pieces, finish, 0)
    for g in range(rs_total - h_p, n_z):
        gradients(g)
    for k in range(3):
        stored[k].start()
    ret[slot_rows(0), :] = ret_out[slot_rows(0), :]

    others = ret.at[cap:, :]
    remote(others, others, back_s, back_r, partner).wait_recv()

    tok_pieces = 4 if pieces == 4 else 2
    tok_rows = toks // tok_pieces

    def tok_at(p):
        return pl.ds(pl.multiple_of(p * tok_rows, tok_rows), tok_rows)

    def mix(p):
        at = tok_at(p)
        routed = dot_nn(sel_t[at, :], ret[...])
        full_cot[tp, at, :] = (out_cot[at, :].astype(f32) + routed).astype(bf16)

    mixer_cot[...] = jnp.zeros_like(mixer_cot)

    wide = 2 * n_z // n_sp

    def proj_copy(j):
        return remote(
            pj_out.at[j],
            pj_in.at[sp, lax.rem(j, wide)],
            pj_s,
            pj_r,
            (j // wide, tp),
        )

    def proj_send(j):
        @pl.when(j // wide != sp)
        def _():
            proj_copy(j).start()

    def project(b, p):
        @pl.when(p == tok_pieces - 1)
        def _():
            whole = jnp.concatenate([full_cot[2 * b], full_cot[2 * b + 1]], axis=1)
            mixer_cot[...] += dot_nn(whole, out_w[feats(b), :])
            found = dot_nn(mix_t[...], whole).astype(bf16)
            for i in range(2):
                j = 2 * b + i
                pj_out[j] = found[:, i * cols : (i + 1) * cols]

                @pl.when(j // wide == sp)
                def _():
                    pj_in[sp, lax.rem(j, wide)] = pj_out[j]

                away = lax.rem(b - z + n_z, n_z)

                @pl.when(away != half)
                def _():
                    proj_send(j)

    ring(
        tok_pieces,
        lambda block, p: full_cot.at[block, tok_at(p), :],
        tk_s,
        tk_r,
        tkd_s,
        tkd_r,
        mix,
        project,
        lambda: None,
        0,
        half == 4,
    )

    cot = mixer_cot[...]
    fut = fine(dot_tn, q_dec[...], cot)
    fut_out[...] = fut.astype(bf16)
    lax.fori_loop(1, n_sp, to_earlier, 0)
    for i in range(2):
        proj_send(2 * zpos(half) + i)
    cot_values = jnp.where(causal, fine(dot_nt, cot, value[...]), 0.0)
    cum = cumul[...]
    q_grad = jnp.exp(cum) * (fine(dot_nt, cot, entry[...]) + fine(dot_nn, cot_values, k_back[...]))
    query_g[...] = (q_grad * DK ** (-0.5)).T
    key_part = jnp.exp(-cum) * fine(dot_tn, cot_values, q_dec[...])
    value_g[...] = fine(dot_tn, scores[...], cot)

    def fut_arrived(s, carry):
        @pl.when(s > sp)
        def _():
            remote(fut_out, fut_in.at[s], bw_s.at[0], bw_r.at[s], partner).wait_recv()

        return carry

    lax.fori_loop(0, n_sp, fut_arrived, 0)

    def pass_back(i, state):
        s = n_sp - 1 - i
        later_on = span_in[s, DK : 2 * DK, :] * state + fut_in[s].astype(f32)
        return jnp.where(s > sp, later_on, state)

    future = lax.fori_loop(0, n_sp, pass_back, jnp.zeros((DK, DV), f32))
    k_grad = key_part + jnp.exp(cum[toks - 1 : toks, :] - cum) * fine(dot_nt, value[...], future)
    k_grad_t = k_grad.T
    key_g[...] = k_grad_t
    value_g[...] += fine(dot_nn, k_end[...], future)
    span_end = span_out[DK : 2 * DK, :] * entry[...] + span_out[0:DK, :]
    beyond = jnp.sum(future * span_end, axis=1, keepdims=True)
    terms = query[...].astype(f32) * query_g[...] - key_in[...].astype(f32) * k_grad_t
    since = jnp.where(t_row >= t_col, 1.0, 0.0).astype(bf16)
    tail = fine(dot_nn, terms, since, 3) + beyond
    logit_g[...] = tail * jax.nn.sigmoid(-logit[...].astype(f32)) / decay_temp

    came = pj_in.at[1:]
    remote(came, came, pj_s, pj_r, partner).wait_recv()
    for i in range(wide):
        sums = jnp.zeros((128, cols), f32)
        for s in range(n_sp):
            sums = sums + pj_in[s, i].astype(f32)
        proj_g[i * cols : (i + 1) * cols, :] = sums.T

    for k in range(3, 8):
        stored[k].start()

    for copy in give_w:
        copy.wait_send()

    def fut_sent(r, carry):
        @pl.when(there(r) < sp)
        def _():
            future_copy(r).wait_send()

        return carry

    lax.fori_loop(1, n_sp, fut_sent, 0)
    for sent, sem in (
        (send.at[:, cap:, :], a2a_s),
        (ret.at[cap:, :], back_s),
        (span_in.at[1:], fw_s),
        (pj_in.at[1:], pj_s),
        (rows.at[: n_z - 1], ag_s),
        (rows.at[:n_z], agd_s),
        (full_cot.at[: n_z - 1], tk_s),
        (full_cot.at[:n_z], tkd_s),
        (stage, rs_s),
        (gu, gu_s),
    ):
        remote(sent, sent, sem, back_r, partner).wait_send()
    for copy in stored:
        copy.wait()


def store_kernel(*refs):
    taken = [
        pltpu.make_async_copy(source, target, refs[24].at[k])
        for k, (source, target) in enumerate(zip(refs[:8], refs[16:24]))
    ]
    stored = [
        pltpu.make_async_copy(source, target, refs[25].at[k])
        for k, (source, target) in enumerate(zip(refs[16:24], refs[8:16]))
    ]
    for copy in taken:
        copy.start()
    for first, second in zip(taken, stored):
        first.wait()
        second.start()
    for copy in stored:
        copy.wait()


def local(
    layer_in,
    out_cot,
    route_ids,
    route_probs,
    group_prob,
    gate_weight,
    up_weight,
    down_weight,
    out_weight,
    query,
    key_in,
    value,
    decay_logit,
):
    toks, cols = layer_in.shape
    n_sp, n_tp = lax.axis_size("sp"), lax.axis_size("tp")
    n_x = 4 if n_sp == 16 else n_sp
    n_z = n_tp // 2
    half = n_z // 2
    pieces = 4 if n_sp % 4 == 0 else 2
    width = gate_weight.shape[2]
    n_rows = 4 * toks
    total = (half - 1) * pieces + pieces // 2
    tk_pieces = 4 if pieces == 4 else 2
    tk_total = (half - 1) * tk_pieces + tk_pieces // 2
    chunk = n_rows // pieces
    wide = n_tp // n_sp
    dma = pltpu.SemaphoreType.DMA
    vmem = pl.BlockSpec(memory_space=pltpu.VMEM)
    hbm = pl.BlockSpec(memory_space=pltpu.HBM)
    small = (DK, toks)
    shapes = ((128, width),) * 3 + ((wide * cols, DV), small, small, (toks, DV), small)
    grads = pl.pallas_call(
        functools.partial(moe_kernel, (n_sp, n_x, n_z, pieces)),
        out_shape=tuple(jax.ShapeDtypeStruct(shape, f32) for shape in shapes),
        in_specs=[vmem] * 3 + [hbm] * 10,
        out_specs=[hbm] * 8,
        scratch_shapes=[
            pltpu.VMEM((toks, cols), bf16),
            pltpu.VMEM((toks, cols), bf16),
            pltpu.VMEM((128, width), bf16),
            pltpu.VMEM((128, width), bf16),
            pltpu.VMEM((128, width), bf16),
            pltpu.VMEM((width, DV), bf16),
            pltpu.VMEM((DK, toks), bf16),
            pltpu.VMEM((DK, toks), bf16),
            pltpu.VMEM((toks, DV), bf16),
            pltpu.VMEM((DK, toks), bf16),
            *(pltpu.VMEM(shape, f32) for shape in shapes),
            pltpu.VMEM((n_tp, toks, cols), bf16),
            pltpu.VMEM((toks, DV), f32),
            pltpu.VMEM((toks, DK), f32),
            pltpu.VMEM((toks, DK), f32),
            pltpu.VMEM((toks, DK), f32),
            pltpu.VMEM((toks, DK), f32),
            pltpu.VMEM((toks, toks), f32),
            pltpu.VMEM((toks, DV), f32),
            pltpu.VMEM((DV, toks), bf16),
            pltpu.VMEM((2 * DK, DV), f32),
            pltpu.VMEM((n_sp, 2 * DK, DV), f32),
            pltpu.VMEM((DK, DV), f32),
            pltpu.VMEM((DK, DV), bf16),
            pltpu.VMEM((n_sp, DK, DV), bf16),
            pltpu.VMEM((n_tp, DV, cols), bf16),
            pltpu.VMEM((n_sp, wide, DV, cols), bf16),
            pltpu.VMEM((2, n_rows, cols), bf16),
            pltpu.VMEM((toks, n_rows), bf16),
            pltpu.VMEM((n_tp, 2, n_rows, cols), bf16),
            pltpu.VMEM((n_rows, 384), f32),
            pltpu.VMEM((2, 128, width), bf16),
            pltpu.VMEM((n_rows, 256), bf16),
            pltpu.VMEM((n_rows, 256), bf16),
            pltpu.VMEM((256, n_rows), bf16),
            pltpu.VMEM((128, n_rows), bf16),
            pltpu.VMEM((2, total, chunk, cols), bf16),
            pltpu.VMEM((2, total, chunk, cols), bf16),
            pltpu.VMEM((n_rows, cols), bf16),
            pltpu.VMEM((n_rows, cols), bf16),
            dma(()),
            dma((pieces,)),
            dma(()),
            dma(()),
            dma(()),
            dma((2, total)),
            dma(()),
            dma((pieces + 2 * total,)),
            dma(()),
            dma((2, total)),
            dma(()),
            dma((2, tk_total)),
            dma(()),
            dma((tk_pieces + 2 * tk_total,)),
            dma((2,)),
            dma((2,)),
            dma(()),
            dma((pieces,)),
            dma(()),
            dma(()),
            dma((n_sp,)),
            dma((n_sp,)),
            dma(()),
            dma(()),
            dma((10,)),
            dma((8,)),
        ],
        compiler_params=pltpu.CompilerParams(
            collective_id=0, has_side_effects=True, vmem_limit_bytes=60 * 1024 * 1024
        ),
    )(
        route_ids.T,
        route_probs.T,
        group_prob,
        layer_in,
        out_cot,
        gate_weight[0],
        up_weight[0],
        down_weight[0],
        out_weight,
        query.T,
        key_in.T,
        value,
        decay_logit.T,
    )
    gate_g, up_g, down_g, proj_g, query_g, key_g, value_g, logit_g = pl.pallas_call(
        store_kernel,
        out_shape=tuple(jax.ShapeDtypeStruct(g.shape, g.dtype) for g in grads),
        in_specs=[hbm] * 8,
        out_specs=[hbm] * 8,
        scratch_shapes=[*(pltpu.VMEM(g.shape, g.dtype) for g in grads), dma((8,)), dma((8,))],
        compiler_params=pltpu.CompilerParams(vmem_limit_bytes=60 * 1024 * 1024),
    )(*grads)
    return (
        gate_g[None],
        up_g[None],
        down_g[None],
        proj_g,
        query_g.T,
        key_g.T,
        value_g,
        logit_g.T,
    )


def solution(mesh):
    in_specs = (
        P("sp", "tp"),
        P("sp", "tp"),
        P("sp", None),
        P("sp", None),
        P("sp"),
        P("sp", "tp", None),
        P("sp", "tp", None),
        P("sp", "tp", None),
        P(None, "tp"),
        P("sp", "tp"),
        P("sp", "tp"),
        P("sp", "tp"),
        P("sp", "tp"),
    )
    out_specs = (
        P("sp", "tp", None),
        P("sp", "tp", None),
        P("sp", "tp", None),
        P("sp", "tp"),
        P("sp", "tp"),
        P("sp", "tp"),
        P("sp", "tp"),
        P("sp", "tp"),
    )
    return jax.shard_map(local, mesh=mesh, in_specs=in_specs, out_specs=out_specs, check_vma=False)
```

```python
import functools

import jax
import jax.numpy as jnp
from jax import lax
from jax.experimental import pallas as pl
from jax.experimental.pallas import tpu as pltpu
from jax.sharding import PartitionSpec as P

DK = 64
DV = 128


decay_temp = 16.0
f32, bf16 = jnp.float32, jnp.bfloat16
MESH = pl.DeviceIdType.MESH


def dot_nt(a, b):
    return lax.dot_general(a, b, (((1,), (1,)), ((), ())), preferred_element_type=f32)


def dot_nn(a, b):
    return lax.dot_general(a, b, (((1,), (0,)), ((), ())), preferred_element_type=f32)


def dot_tn(a, b):
    return lax.dot_general(a, b, (((0,), (0,)), ((), ())), preferred_element_type=f32)


def parts_of(x, n):
    if x.dtype == bf16:
        return [x]
    found = []
    for _ in range(n):
        top = x.astype(bf16)
        found.append(top)
        x = x - top.astype(f32)
    return found


def fine(dot, a, b, n=2):
    a, b = parts_of(a, n), parts_of(b, n)
    terms = [dot(p, q) for i, p in enumerate(a) for j, q in enumerate(b) if i + j < n]
    total = terms[-1]
    for term in terms[-2::-1]:
        total = total + term
    return total


def moe_kernel(
    sizes,
    ids,
    probs,
    group,
    *refs,
):
    held, given, kept = refs[:10], refs[10:18], refs[18:]
    expert_kernel(sizes, ids, probs, group, held, given, *kept)


def expert_kernel(
    sizes,
    ids,
    probs,
    group,
    held,
    given,
    layer_in,
    out_cot,
    gate,
    up,
    down,
    out_w,
    query,
    key_in,
    value,
    logit,
    gate_g,
    up_g,
    down_g,
    proj_g,
    query_g,
    key_g,
    value_g,
    logit_g,
    full_cot,
    mixer_cot,
    q_dec,
    k_back,
    k_end,
    cumul,
    scores,
    within,
    mix_t,
    span_out,
    span_in,
    entry,
    fut_out,
    fut_in,
    pj_out,
    pj_in,
    send,
    near,
    send_near,
    sel_t,
    rows,
    pre,
    part_w,
    gu,
    gu_part,
    gu_t,
    hid_t,
    stage,
    inbox,
    ret_out,
    ret,
    a2a_s,
    a2a_r,
    back_s,
    back_r,
    ag_s,
    ag_r,
    agd_s,
    agd_r,
    rs_s,
    rs_r,
    tk_s,
    tk_r,
    tkd_s,
    tkd_r,
    misc_s,
    misc_r,
    gu_s,
    gu_r,
    tok_s,
    tok_r,
    nb_s,
    nb_r,
    fw_s,
    fw_r,
    bw_s,
    bw_r,
    pj_s,
    pj_r,
    load_s,
    give_s,
):
    n_sp, n_x, n_z, pieces = sizes
    n_y = n_sp // n_x
    half = n_z // 2
    targets = (layer_in, out_cot, gate, up, down, out_w, query, key_in, value, logit)
    loaded = [
        pltpu.make_async_copy(source, target, load_s.at[k])
        for k, (source, target) in enumerate(zip(held, targets))
    ]
    for k in (0, 1, 2, 3, 6, 7, 8, 9, 4, 5):
        loaded[k].start()
    results = (gate_g, up_g, down_g, proj_g, query_g, key_g, value_g, logit_g)
    stored = [
        pltpu.make_async_copy(source, target, give_s.at[k])
        for k, (source, target) in enumerate(zip(results, given))
    ]
    toks, cols = layer_in.shape
    cap = 4 * toks // n_sp
    n_rows = n_sp * cap
    per = n_sp // pieces
    chunk = n_rows // pieces
    sp = lax.axis_index("sp")
    tp = lax.axis_index("tp")
    core = lax.rem(tp, 2)
    z = tp // 2
    z_up = lax.rem(z + 1, n_z)
    z_dn = lax.rem(z + n_z - 1, n_z)
    partner = (sp, 2 * z + 1 - core)
    above, below = (sp, 2 * z_up + core), (sp, 2 * z_dn + core)
    two_up = (sp, 2 * lax.rem(z + 2, n_z) + core)
    two_dn = (sp, 2 * lax.rem(z + n_z - 2, n_z) + core)
    my_y, my_x = sp // n_x, lax.rem(sp, n_x)

    def row_of(k):
        return jnp.where(k == 1, 2, jnp.where(k == 2, 1, k)) if n_y == 4 else k

    def there(r):
        ry, rx = row_of(r // n_x), lax.rem(r, n_x)
        return lax.rem(my_y + ry, n_y) * n_x + lax.rem(my_x + rx, n_x)

    def back_to(r):
        ry, rx = row_of(r // n_x), lax.rem(r, n_x)
        return lax.rem(my_y + n_y - ry, n_y) * n_x + lax.rem(my_x + n_x - rx, n_x)

    def zpos(d):
        return lax.rem(z + d + n_z, n_z)

    def remote(src, dst, s, r, dev):
        return pltpu.make_async_remote_copy(
            src_ref=src, dst_ref=dst, send_sem=s, recv_sem=r, device_id=dev, device_id_type=MESH
        )

    barrier = pltpu.get_barrier_semaphore()
    for r in range(1, n_sp):
        pl.semaphore_signal(barrier, inc=1, device_id=(there(r), tp), device_id_type=MESH)
    greeted = (partner, above, below) + ((two_up, two_dn) if half == 4 else ())
    for dev in greeted:
        pl.semaphore_signal(barrier, inc=1, device_id=dev, device_id_type=MESH)

    def piece_rows(p):
        return pl.ds(pl.multiple_of(p * chunk, chunk), chunk)

    t_row = lax.broadcasted_iota(jnp.int32, (toks, toks), 0)
    t_col = lax.broadcasted_iota(jnp.int32, (toks, toks), 1)
    diagonal = t_row == t_col

    def as_row(column):
        return jnp.sum(jnp.where(diagonal, column, 0.0), axis=0, keepdims=True)

    def as_column(row):
        return jnp.sum(jnp.where(diagonal, row, 0.0), axis=1, keepdims=True)

    experts = lax.broadcasted_iota(jnp.int32, (toks, 128), 1)
    id0 = as_column(ids[0:1, :].astype(f32)).astype(jnp.int32)
    id1 = as_column(ids[1:2, :].astype(f32)).astype(jnp.int32)
    hit0, hit1 = experts == id0, experts == id1
    chosen = (jnp.where(hit0, 1.0, 0.0) + jnp.where(hit1, 1.0, 0.0)).astype(bf16)
    earlier = jnp.where(t_col < t_row, 1.0, 0.0).astype(bf16)
    count = dot_nn(earlier, chosen)
    pos0 = jnp.sum(jnp.where(hit0, count, 0.0), axis=1, keepdims=True)
    pos1 = jnp.sum(jnp.where(hit1, count, 0.0), axis=1, keepdims=True)

    def offset_of(expert):
        ey, ex = expert // n_x, lax.rem(expert, n_x)
        return row_of(lax.rem(ey + n_y - my_y, n_y)) * n_x + lax.rem(ex + n_x - my_x, n_x)

    slot0 = offset_of(id0) * cap + pos0.astype(jnp.int32)
    slot1 = offset_of(id1) * cap + pos1.astype(jnp.int32)
    p0, p1 = probs[0:1, :], probs[1:2, :]
    group_row = group[...].reshape(1, toks)
    w0 = group_row * p0 / (p0 + p1)
    w1 = group_row * p1 / (p0 + p1)
    slot0_row, slot1_row = as_row(slot0.astype(f32)), as_row(slot1.astype(f32))
    loaded[0].wait()
    loaded[1].wait()
    both = jnp.concatenate([layer_in[...], out_cot[...]], axis=1)

    def picking(p):
        here = (lax.broadcasted_iota(jnp.int32, (chunk, toks), 0) + p * chunk).astype(f32)
        m0, m1 = here == slot0_row, here == slot1_row
        pick = (jnp.where(m0, 1.0, 0.0) + jnp.where(m1, 1.0, 0.0)).astype(bf16)
        weight = jnp.sum(jnp.where(m0, w0, 0.0) + jnp.where(m1, w1, 0.0), axis=1, keepdims=True)
        return pick, weight

    def select(p, carry):
        pick, weight = picking(p)
        picked = dot_nn(pick, both)
        send[0, piece_rows(p), :] = picked[:, :cols].astype(bf16)
        send[1, piece_rows(p), :] = (picked[:, cols:] * weight).astype(bf16)
        return carry

    select(0, 0)
    pl.semaphore_wait(barrier, n_sp - 1 + len(greeted))

    def give_tok(d):
        return [
            remote(source, near.at[1 - d, k], tok_s, tok_r.at[1 - d], below if d == 0 else above)
            for k, source in enumerate((layer_in, out_cot))
        ]

    for d in range(2):
        for copy in give_tok(d):
            copy.start()

    def slot_rows(r):
        return pl.ds(pl.multiple_of(r * cap, cap), cap)

    def dispatch(r):
        return remote(
            send.at[:, slot_rows(r), :],
            rows.at[tp, :, slot_rows(r), :],
            a2a_s,
            a2a_r.at[r // per],
            (there(r), tp),
        )

    def start_dispatch(p):
        for i in range(per):
            r = p * per + i

            @pl.when(r > 0)
            def _():
                dispatch(r).start()

    start_dispatch(0)

    def select_next(p, carry):
        select(p, 0)
        start_dispatch(p)
        return carry

    lax.fori_loop(1, pieces, select_next, 0)
    rows[tp, :, slot_rows(0), :] = send[:, slot_rows(0), :]

    through = pieces // 2
    nb_tp = (2 * z_dn + core, 2 * z_up + core)

    def dispatch_near(r, d):
        return remote(
            send_near.at[d, :, slot_rows(r), :],
            rows.at[nb_tp[d], :, slot_rows(r), :],
            nb_s,
            nb_r.at[d, r // per],
            (there(r), tp),
        )

    def near_rows():
        for d in range(2):
            remote(near.at[d], near.at[d], tok_s, tok_r.at[d], partner).wait_recv()
        tokens = jnp.concatenate([near[0, 0], near[0, 1], near[1, 0], near[1, 1]], axis=1)

        def one(p, carry):
            pick, weight = picking(p)
            picked = dot_nn(pick, tokens)
            for d in range(2):
                x = picked[:, 2 * d * cols : (2 * d + 1) * cols]
                c = picked[:, (2 * d + 1) * cols : (2 * d + 2) * cols]
                send_near[d, 0, piece_rows(p), :] = x.astype(bf16)
                send_near[d, 1, piece_rows(p), :] = (c * weight).astype(bf16)

            for i in range(per):
                for d in range(2):
                    dispatch_near(p * per + i, d).start()

            return carry

        lax.fori_loop(through, pieces, one, 0)

    def near_ready(d, p):
        came = rows.at[nb_tp[d], :, piece_rows(p), :]
        remote(came, came, nb_s, nb_r.at[d, p], partner).wait_recv()

    give_w = [
        remote(w, part_w.at[k], misc_s.at[k], misc_r.at[k], partner)
        for k, w in enumerate((gate, up))
    ]
    loaded[2].wait()
    loaded[3].wait()
    for copy in give_w:
        copy.start()

    last = (half - 1) * pieces

    def ring(n_pieces, where, sems_s, sems_r, sems_ds, sems_dr, own_ready, compute, beside, stop, leap, side):
        h_p = n_pieces // 2
        total = (half - 1) * n_pieces + h_p

        def along(block, p, d, k, far=False):
            ref = where(block, p)
            return remote(ref, ref, sems_s, sems_r.at[d, k], (two_up, two_dn)[d] if far else (above, below)[d])

        def across(block, p, k):
            ref = where(block, p)
            return remote(ref, ref, sems_ds, sems_dr.at[k], partner)

        def own(p, carry):
            own_ready(p)
            if leap:
                along(tp, p, 0, n_pieces + p, True).start()
                along(tp, p, 1, n_pieces + p, True).start()
            @pl.when((p < through) if side else (p >= 0))
            def _():
                along(tp, p, 0, p).start()
                along(tp, p, 1, p).start()

            across(tp, p, p).start()
            return carry

        lax.fori_loop(0, 1, own, 0)
        beside()
        lax.fori_loop(1, n_pieces, own, 0)

        def own_compute(p, carry):
            across(tp, p, p).wait_recv()
            compute(z, p)
            return carry

        lax.fori_loop(0, n_pieces, own_compute, 0)

        def at(t):
            in_half = t >= (half - 1) * n_pieces
            p_up = lax.rem(t, n_pieces)
            p_dn = jnp.where(in_half, p_up + h_p, p_up)
            hop = t // n_pieces
            return hop, p_up, p_dn

        def arrive(t, d, block, p):
            if side is None:
                along(block, p, d, t).wait_recv()
                return

            beyond = (t >= through) & (t < n_pieces)

            @pl.when(jnp.logical_not(beyond))
            def _():
                along(block, p, d, t).wait_recv()

            @pl.when(beyond)
            def _():
                side(d, p)

        def move(t):
            hop, p_up, p_dn = at(t)
            b_up, b_dn = zpos(-1 - hop), zpos(1 + hop)
            arrive(t, 0, 2 * b_up + core, p_up)
            pass_up = (hop < half - 2) | ((hop == half - 2) & (p_up < h_p))

            @pl.when((hop == 1) if leap else pass_up)
            def _():
                along(2 * b_up + core, p_up, 0, t + n_pieces).start()

            if leap:
                @pl.when((hop == 1) & (p_up < h_p))
                def _():
                    along(2 * b_up + core, p_up, 0, t + 2 * n_pieces, True).start()

            across(2 * b_up + core, p_up, n_pieces + 2 * t).start()
            arrive(t, 1, 2 * b_dn + core, p_dn)

            @pl.when((hop == 1) if leap else (hop < half - 2))
            def _():
                along(2 * b_dn + core, p_dn, 1, t + n_pieces).start()

            if leap:
                @pl.when((hop == 1) & (p_dn >= h_p))
                def _():
                    along(2 * b_dn + core, p_dn, 1, t + 2 * n_pieces - h_p, True).start()
            else:
                @pl.when((hop == half - 2) & (p_dn >= h_p))
                def _():
                    along(2 * b_dn + core, p_dn, 1, t + n_pieces - h_p).start()

            across(2 * b_dn + core, p_dn, n_pieces + 2 * t + 1).start()

        def turn(u):
            if side:
                full = half - 1
                v = u - full * through
                rest = n_pieces - through
                ringed = (u // through) * n_pieces + lax.rem(u, through)
                sided = (v // rest) * n_pieces + through + lax.rem(jnp.maximum(v, 0), rest)
                return jnp.where(v < 0, ringed, jnp.where(u < full * n_pieces, sided, u))
            if not leap:
                return u
            return jnp.where(u < n_pieces, u + n_pieces, jnp.where(u < 2 * n_pieces, u - n_pieces, u))

        def step(u, carry):
            move(turn(u))

            @pl.when(u > 0)
            def _():
                use(turn(u - 1))

            return carry

        def use(t):
            hop, p_up, p_dn = at(t)
            b_up, b_dn = zpos(-1 - hop), zpos(1 + hop)
            across(2 * b_up + 1 - core, p_up, n_pieces + 2 * t).wait_recv()
            compute(b_up, p_up)
            across(2 * b_dn + 1 - core, p_dn, n_pieces + 2 * t + 1).wait_recv()
            compute(b_dn, p_dn)

        lax.fori_loop(0, total - stop, step, 0)
        use(total - stop - 1)
        return move, use


    def rows_ready(p):
        @pl.when((p == 0) & (per > 1))
        def _():
            came = rows.at[tp, :, cap:chunk, :]
            remote(came, came, a2a_s, a2a_r.at[0], partner).wait_recv()

        @pl.when(p > 0)
        def _():
            came = rows.at[tp, :, piece_rows(p), :]
            remote(came, came, a2a_s, a2a_r.at[p], partner).wait_recv()

    def feats(b):
        return pl.ds(pl.multiple_of(b * 2 * cols, 2 * cols), 2 * cols)

    causal = t_col <= t_row

    def to_peers(copy_of):
        def one(r, carry):
            copy_of(r).start()
            return carry

        lax.fori_loop(1, n_sp, one, 0)

    def span_copy(r):
        return remote(span_out, span_in.at[sp], fw_s, fw_r, (there(r), tp))

    def future_copy(r):
        return remote(fut_out, fut_in.at[sp], bw_s.at[r], bw_r.at[sp], (there(r), tp))

    def to_earlier(r, carry):
        @pl.when(there(r) < sp)
        def _():
            future_copy(r).start()

        return carry

    def attend():
        slots = lax.broadcasted_iota(jnp.int32, (toks, n_rows), 1)
        sel_t[...] = (
            jnp.where(slots == slot0, 1.0, 0.0) + jnp.where(slots == slot1, 1.0, 0.0)
        ).astype(bf16)
        for k in (6, 7, 8, 9, 4, 5):
            loaded[k].wait()
        log_decay = jax.nn.log_sigmoid(logit[...].astype(f32).T) / decay_temp
        upto = jnp.where(causal, 1.0, 0.0).astype(bf16)
        cum = fine(dot_nn, upto, log_decay, 3)
        total = cum[toks - 1 : toks, :]
        cumul[...] = cum
        k = key_in[...].astype(f32).T
        q_dec[...] = query[...].astype(f32).T * DK ** (-0.5) * jnp.exp(cum)
        k_back[...] = k * jnp.exp(-cum)
        k_end[...] = k * jnp.exp(total - cum)
        span_out[0:DK, :] = fine(dot_tn, k_end[...], value[...])
        span_out[DK : 2 * DK, :] = jnp.exp(fine(dot_tn, log_decay, jnp.ones((toks, DV), bf16), 3))
        to_peers(span_copy)
        span_in[sp] = span_out[...]
        found = jnp.where(causal, fine(dot_nt, q_dec[...], k_back[...]), 0.0)
        scores[...] = found
        within[...] = fine(dot_nn, found, value[...])
        pre[...] = jnp.zeros_like(pre)

    def enter():
        came = span_in.at[1:]
        remote(came, came, fw_s, fw_r, partner).wait_recv()

        def pass_on(s, state):
            return jnp.where(s < sp, span_in[s, DK : 2 * DK, :] * state + span_in[s, 0:DK, :], state)

        entry[...] = lax.fori_loop(0, n_sp, pass_on, jnp.zeros((DK, DV), f32))
        mixed_out = within[...] + fine(dot_nn, q_dec[...], entry[...])
        mix_t[...] = mixed_out.T.astype(bf16)


    def expert_in(b, p):
        w_gu = jnp.concatenate([gate[:, feats(b)], up[:, feats(b)]], axis=0)
        at = piece_rows(p)
        x = jnp.concatenate([rows[2 * b, 0, at, :], rows[2 * b + 1, 0, at, :]], axis=1)
        c = jnp.concatenate([rows[2 * b, 1, at, :], rows[2 * b + 1, 1, at, :]], axis=1)
        pre[at, 0:256] += dot_nt(x, w_gu)
        pre[at, 256:384] += dot_nt(c, down[:, feats(b)])

    early = 1 if pieces == 4 else 0
    attend()
    move, use = ring(
        pieces,
        lambda block, p: rows.at[block, :, piece_rows(p), :],
        ag_s,
        ag_r,
        agd_s,
        agd_r,
        rows_ready,
        expert_in,
        near_rows,
        early,
        False,
        near_ready,
    )

    h_p = pieces // 2

    def give_gu(p):
        at = piece_rows(p)
        return remote(gu.at[at, :], gu_part.at[at, :], gu_s, gu_r.at[p], partner)

    def middle(i, carry):
        p = i // 2 + lax.rem(i, 2) * h_p
        at = piece_rows(p)
        gate_pre, up_pre, hidden_cot = pre[at, 0:128], pre[at, 128:256], pre[at, 256:384]
        sig = jax.nn.sigmoid(gate_pre)
        active = gate_pre * sig
        gu[at, 0:128] = (hidden_cot * up_pre * sig * (1.0 + gate_pre * (1.0 - sig))).astype(bf16)
        gu[at, 128:256] = (hidden_cot * active).astype(bf16)
        give_gu(p).start()
        pre[at, 0:128] = active * up_pre
        return carry

    rs_total = h_p + (half - 1) * pieces

    def partial(b, p):
        cols_at = pl.ds(pl.multiple_of((2 * b + core) * cols, cols), cols)
        mine = jnp.concatenate([gate[:, cols_at], up[:, cols_at]], axis=0)
        theirs = jnp.concatenate([part_w[0, :, cols_at], part_w[1, :, cols_at]], axis=0)
        at = piece_rows(p)
        return dot_nn(gu[at, :], mine) + dot_nn(gu_part[at, :], theirs)

    def hop_sum(d, k):
        return remote(
            stage.at[d, k],
            inbox.at[d, k],
            rs_s,
            rs_r.at[d, k],
            above if d == 0 else below,
        )

    def first(t, carry):
        for d in range(2):
            give_gu(t + d * h_p).wait_recv()
            stage[d, t] = partial(zpos(half), t + d * h_p).astype(bf16)
            hop_sum(d, t).start()
        return carry

    if early:
        lax.fori_loop(0, 2, middle, 0)
        for copy in give_w:
            copy.wait_recv()
        move(rs_total - 1)
        first(0, 0)
        use(rs_total - 1)
        lax.fori_loop(2, pieces, middle, 0)
        lax.fori_loop(1, h_p, first, 0)
    else:
        lax.fori_loop(0, pieces, middle, 0)
        for copy in give_w:
            copy.wait_recv()
        lax.fori_loop(0, h_p, first, 0)
    gu_t[...] = gu[...].T
    hid_t[...] = pre[:, 0:128].astype(bf16).T
    enter()

    def gradients(b):
        x = jnp.concatenate([rows[2 * b, 0], rows[2 * b + 1, 0]], axis=1)
        c = jnp.concatenate([rows[2 * b, 1], rows[2 * b + 1, 1]], axis=1)
        both_g = dot_nn(gu_t[...], x)
        gate_g[:, feats(b)] = both_g[0:128]
        up_g[:, feats(b)] = both_g[128:256]
        down_g[:, feats(b)] = dot_nn(hid_t[...], c)

    def later(u, carry):
        t = u + h_p
        hop, p = 1 + u // pieces, lax.rem(u, pieces)
        for d in range(2):
            dest = zpos(half - hop) if d == 0 else zpos(hop - half)
            value = partial(dest, p)
            mine_first = (p >= h_p) if d == 0 else (p < h_p)
            alone = (hop == 1) & mine_first
            k_in = jnp.where(hop == 1, p - d * h_p, t - pieces)

            @pl.when(alone)
            def _():
                stage[d, t] = value.astype(bf16)

            @pl.when(jnp.logical_not(alone))
            def _():
                hop_sum(d, k_in).wait_recv()
                stage[d, t] = (value + inbox[d, k_in].astype(f32)).astype(bf16)

            hop_sum(d, t).start()

        @pl.when(u < n_z)
        def _():
            gradients(u)

        return carry

    lax.fori_loop(0, rs_total - h_p, later, 0)

    def give_back(r):
        return remote(
            ret_out.at[slot_rows(r), :],
            ret.at[slot_rows(r), :],
            back_s,
            back_r,
            (back_to(r), tp),
        )

    def finish(p, carry):
        k_in = rs_total - pieces + p
        value = partial(z, p)
        for d in range(2):
            hop_sum(d, k_in).wait_recv()
            value = value + inbox[d, k_in].astype(f32)
        ret_out[piece_rows(p), :] = value.astype(bf16)
        for i in range(per):
            r = p * per + i

            @pl.when(r > 0)
            def _():
                give_back(r).start()

        return carry

    lax.fori_loop(0, pieces, finish, 0)
    for g in range(rs_total - h_p, n_z):
        gradients(g)
    for k in range(3):
        stored[k].start()
    ret[slot_rows(0), :] = ret_out[slot_rows(0), :]

    others = ret.at[cap:, :]
    remote(others, others, back_s, back_r, partner).wait_recv()

    tok_pieces = 4 if pieces == 4 else 2
    tok_rows = toks // tok_pieces

    def tok_at(p):
        return pl.ds(pl.multiple_of(p * tok_rows, tok_rows), tok_rows)

    def mix(p):
        at = tok_at(p)
        routed = dot_nn(sel_t[at, :], ret[...])
        full_cot[tp, at, :] = (out_cot[at, :].astype(f32) + routed).astype(bf16)

    mixer_cot[...] = jnp.zeros_like(mixer_cot)

    wide = 2 * n_z // n_sp

    def proj_copy(j):
        return remote(
            pj_out.at[j],
            pj_in.at[sp, lax.rem(j, wide)],
            pj_s,
            pj_r,
            (j // wide, tp),
        )

    def proj_send(j):
        @pl.when(j // wide != sp)
        def _():
            proj_copy(j).start()

    def project(b, p):
        @pl.when(p == tok_pieces - 1)
        def _():
            whole = jnp.concatenate([full_cot[2 * b], full_cot[2 * b + 1]], axis=1)
            mixer_cot[...] += dot_nn(whole, out_w[feats(b), :])
            found = dot_nn(mix_t[...], whole).astype(bf16)
            for i in range(2):
                j = 2 * b + i
                pj_out[j] = found[:, i * cols : (i + 1) * cols]

                @pl.when(j // wide == sp)
                def _():
                    pj_in[sp, lax.rem(j, wide)] = pj_out[j]

                away = lax.rem(b - z + n_z, n_z)

                @pl.when(away != half)
                def _():
                    proj_send(j)

    ring(
        tok_pieces,
        lambda block, p: full_cot.at[block, tok_at(p), :],
        tk_s,
        tk_r,
        tkd_s,
        tkd_r,
        mix,
        project,
        lambda: None,
        0,
        half == 4,
        None,
    )

    cot = mixer_cot[...]
    fut = fine(dot_tn, q_dec[...], cot)
    fut_out[...] = fut.astype(bf16)
    lax.fori_loop(1, n_sp, to_earlier, 0)
    for i in range(2):
        proj_send(2 * zpos(half) + i)
    cot_values = jnp.where(causal, fine(dot_nt, cot, value[...]), 0.0)
    cum = cumul[...]
    q_grad = jnp.exp(cum) * (fine(dot_nt, cot, entry[...]) + fine(dot_nn, cot_values, k_back[...]))
    query_g[...] = (q_grad * DK ** (-0.5)).T
    key_part = jnp.exp(-cum) * fine(dot_tn, cot_values, q_dec[...])
    value_g[...] = fine(dot_tn, scores[...], cot)

    def fut_arrived(s, carry):
        @pl.when(s > sp)
        def _():
            remote(fut_out, fut_in.at[s], bw_s.at[0], bw_r.at[s], partner).wait_recv()

        return carry

    lax.fori_loop(0, n_sp, fut_arrived, 0)

    def pass_back(i, state):
        s = n_sp - 1 - i
        later_on = span_in[s, DK : 2 * DK, :] * state + fut_in[s].astype(f32)
        return jnp.where(s > sp, later_on, state)

    future = lax.fori_loop(0, n_sp, pass_back, jnp.zeros((DK, DV), f32))
    k_grad = key_part + jnp.exp(cum[toks - 1 : toks, :] - cum) * fine(dot_nt, value[...], future)
    k_grad_t = k_grad.T
    key_g[...] = k_grad_t
    value_g[...] += fine(dot_nn, k_end[...], future)
    span_end = span_out[DK : 2 * DK, :] * entry[...] + span_out[0:DK, :]
    beyond = jnp.sum(future * span_end, axis=1, keepdims=True)
    terms = query[...].astype(f32) * query_g[...] - key_in[...].astype(f32) * k_grad_t
    since = jnp.where(t_row >= t_col, 1.0, 0.0).astype(bf16)
    tail = fine(dot_nn, terms, since, 3) + beyond
    logit_g[...] = tail * jax.nn.sigmoid(-logit[...].astype(f32)) / decay_temp

    came = pj_in.at[1:]
    remote(came, came, pj_s, pj_r, partner).wait_recv()
    for i in range(wide):
        sums = jnp.zeros((128, cols), f32)
        for s in range(n_sp):
            sums = sums + pj_in[s, i].astype(f32)
        proj_g[i * cols : (i + 1) * cols, :] = sums.T

    for k in range(3, 8):
        stored[k].start()

    for copy in give_w:
        copy.wait_send()

    def fut_sent(r, carry):
        @pl.when(there(r) < sp)
        def _():
            future_copy(r).wait_send()

        return carry

    lax.fori_loop(1, n_sp, fut_sent, 0)
    for sent, sem in (
        (send.at[:, cap:, :], a2a_s),
        (ret.at[cap:, :], back_s),
        (span_in.at[1:], fw_s),
        (pj_in.at[1:], pj_s),
        (near, tok_s),
        (send_near.at[:, :, through * chunk :, :], nb_s),
        (rows.at[: 4 * (rs_total - pieces + through) // pieces, 0], ag_s),
        (rows.at[:n_z], agd_s),
        (full_cot.at[: n_z - 1], tk_s),
        (full_cot.at[:n_z], tkd_s),
        (stage, rs_s),
        (gu, gu_s),
    ):
        remote(sent, sent, sem, back_r, partner).wait_send()
    for copy in stored:
        copy.wait()


def store_kernel(*refs):
    taken = [
        pltpu.make_async_copy(source, target, refs[24].at[k])
        for k, (source, target) in enumerate(zip(refs[:8], refs[16:24]))
    ]
    stored = [
        pltpu.make_async_copy(source, target, refs[25].at[k])
        for k, (source, target) in enumerate(zip(refs[16:24], refs[8:16]))
    ]
    for copy in taken:
        copy.start()
    for first, second in zip(taken, stored):
        first.wait()
        second.start()
    for copy in stored:
        copy.wait()


def local(
    layer_in,
    out_cot,
    route_ids,
    route_probs,
    group_prob,
    gate_weight,
    up_weight,
    down_weight,
    out_weight,
    query,
    key_in,
    value,
    decay_logit,
):
    toks, cols = layer_in.shape
    n_sp, n_tp = lax.axis_size("sp"), lax.axis_size("tp")
    n_x = 4 if n_sp == 16 else n_sp
    n_z = n_tp // 2
    half = n_z // 2
    pieces = 4 if n_sp % 4 == 0 else 2
    width = gate_weight.shape[2]
    n_rows = 4 * toks
    total = (half - 1) * pieces + pieces // 2
    tk_pieces = 4 if pieces == 4 else 2
    tk_total = (half - 1) * tk_pieces + tk_pieces // 2
    chunk = n_rows // pieces
    wide = n_tp // n_sp
    dma = pltpu.SemaphoreType.DMA
    vmem = pl.BlockSpec(memory_space=pltpu.VMEM)
    hbm = pl.BlockSpec(memory_space=pltpu.HBM)
    small = (DK, toks)
    shapes = ((128, width),) * 3 + ((wide * cols, DV), small, small, (toks, DV), small)
    grads = pl.pallas_call(
        functools.partial(moe_kernel, (n_sp, n_x, n_z, pieces)),
        out_shape=tuple(jax.ShapeDtypeStruct(shape, f32) for shape in shapes),
        in_specs=[vmem] * 3 + [hbm] * 10,
        out_specs=[hbm] * 8,
        scratch_shapes=[
            pltpu.VMEM((toks, cols), bf16),
            pltpu.VMEM((toks, cols), bf16),
            pltpu.VMEM((128, width), bf16),
            pltpu.VMEM((128, width), bf16),
            pltpu.VMEM((128, width), bf16),
            pltpu.VMEM((width, DV), bf16),
            pltpu.VMEM((DK, toks), bf16),
            pltpu.VMEM((DK, toks), bf16),
            pltpu.VMEM((toks, DV), bf16),
            pltpu.VMEM((DK, toks), bf16),
            *(pltpu.VMEM(shape, f32) for shape in shapes),
            pltpu.VMEM((n_tp, toks, cols), bf16),
            pltpu.VMEM((toks, DV), f32),
            pltpu.VMEM((toks, DK), f32),
            pltpu.VMEM((toks, DK), f32),
            pltpu.VMEM((toks, DK), f32),
            pltpu.VMEM((toks, DK), f32),
            pltpu.VMEM((toks, toks), f32),
            pltpu.VMEM((toks, DV), f32),
            pltpu.VMEM((DV, toks), bf16),
            pltpu.VMEM((2 * DK, DV), f32),
            pltpu.VMEM((n_sp, 2 * DK, DV), f32),
            pltpu.VMEM((DK, DV), f32),
            pltpu.VMEM((DK, DV), bf16),
            pltpu.VMEM((n_sp, DK, DV), bf16),
            pltpu.VMEM((n_tp, DV, cols), bf16),
            pltpu.VMEM((n_sp, wide, DV, cols), bf16),
            pltpu.VMEM((2, n_rows, cols), bf16),
            pltpu.VMEM((2, 2, toks, cols), bf16),
            pltpu.VMEM((2, 2, n_rows, cols), bf16),
            pltpu.VMEM((toks, n_rows), bf16),
            pltpu.VMEM((n_tp, 2, n_rows, cols), bf16),
            pltpu.VMEM((n_rows, 384), f32),
            pltpu.VMEM((2, 128, width), bf16),
            pltpu.VMEM((n_rows, 256), bf16),
            pltpu.VMEM((n_rows, 256), bf16),
            pltpu.VMEM((256, n_rows), bf16),
            pltpu.VMEM((128, n_rows), bf16),
            pltpu.VMEM((2, total, chunk, cols), bf16),
            pltpu.VMEM((2, total, chunk, cols), bf16),
            pltpu.VMEM((n_rows, cols), bf16),
            pltpu.VMEM((n_rows, cols), bf16),
            dma(()),
            dma((pieces,)),
            dma(()),
            dma(()),
            dma(()),
            dma((2, total)),
            dma(()),
            dma((pieces + 2 * total,)),
            dma(()),
            dma((2, total)),
            dma(()),
            dma((2, tk_total)),
            dma(()),
            dma((tk_pieces + 2 * tk_total,)),
            dma((2,)),
            dma((2,)),
            dma(()),
            dma((pieces,)),
            dma(()),
            dma((2,)),
            dma(()),
            dma((2, pieces)),
            dma(()),
            dma(()),
            dma((n_sp,)),
            dma((n_sp,)),
            dma(()),
            dma(()),
            dma((10,)),
            dma((8,)),
        ],
        compiler_params=pltpu.CompilerParams(
            collective_id=0, has_side_effects=True, vmem_limit_bytes=60 * 1024 * 1024
        ),
    )(
        route_ids.T,
        route_probs.T,
        group_prob,
        layer_in,
        out_cot,
        gate_weight[0],
        up_weight[0],
        down_weight[0],
        out_weight,
        query.T,
        key_in.T,
        value,
        decay_logit.T,
    )
    gate_g, up_g, down_g, proj_g, query_g, key_g, value_g, logit_g = pl.pallas_call(
        store_kernel,
        out_shape=tuple(jax.ShapeDtypeStruct(g.shape, g.dtype) for g in grads),
        in_specs=[hbm] * 8,
        out_specs=[hbm] * 8,
        scratch_shapes=[*(pltpu.VMEM(g.shape, g.dtype) for g in grads), dma((8,)), dma((8,))],
        compiler_params=pltpu.CompilerParams(vmem_limit_bytes=60 * 1024 * 1024),
    )(*grads)
    return (
        gate_g[None],
        up_g[None],
        down_g[None],
        proj_g,
        query_g.T,
        key_g.T,
        value_g,
        logit_g.T,
    )


def solution(mesh):
    in_specs = (
        P("sp", "tp"),
        P("sp", "tp"),
        P("sp", None),
        P("sp", None),
        P("sp"),
        P("sp", "tp", None),
        P("sp", "tp", None),
        P("sp", "tp", None),
        P(None, "tp"),
        P("sp", "tp"),
        P("sp", "tp"),
        P("sp", "tp"),
        P("sp", "tp"),
    )
    out_specs = (
        P("sp", "tp", None),
        P("sp", "tp", None),
        P("sp", "tp", None),
        P("sp", "tp"),
        P("sp", "tp"),
        P("sp", "tp"),
        P("sp", "tp"),
        P("sp", "tp"),
    )
    return jax.shard_map(local, mesh=mesh, in_specs=in_specs, out_specs=out_specs, check_vma=False)
```
